512 devices in a mesh: ep: 32 (over z, x), tp: 16 (over y, core).
Axes of the slice: x: 4, y: 8, z: 8, core: 2. Of those that a mesh axis runs over, the one named last changes fastest.
Arguments:
- queries: bfloat16 [8192, 1536], P('ep', 'tp'), may hold values from -600 to 600
- compressed_key_value: bfloat16 [8192, 512], P('ep'), may hold values from -6 to 6
- rope_key: bfloat16 [8192, 32], P('ep'), may hold values from -6 to 6
- latent_norm_gain: float32 [512], replicated, may hold values from 0.1 to 1.9
- latent_to_key_value: bfloat16 [512, 2048], P(None, 'tp'), may hold values from -0.25 to 0.25
- out_proj: bfloat16 [1024, 2048], P(None, 'tp'), may hold values from -1.5 to 1.5
- moe_input: bfloat16 [8192, 2048], P('ep'), may hold values from -6 to 6
- moe_gain: float32 [2048], replicated, may hold values from 0.1 to 1.9
- routes: int32 [8192, 2], P('ep'), may hold values from 0 to 31, all different within a row; in each aligned block of 256 rows (0 to 255, 256 to 511, ...) at most 24 rows name the same one
- route_weight: float32 [8192, 2], P('ep'), may hold values from 0.2 to 1
- gate_weight: bfloat16 [32, 2048, 4096], P('ep', None, 'tp'), may hold values from -0.125 to 0.125
- up_weight: bfloat16 [32, 2048, 4096], P('ep', None, 'tp'), may hold values from -0.125 to 0.125
- down_weight: bfloat16 [32, 4096, 2048], P('ep', 'tp'), may hold values from -0.09375 to 0.09375
Outputs:
- attention_out: bfloat16 [8192, 2048], P('ep', 'tp')
- expert_out: bfloat16 [8192, 2048], P('ep', 'tp')
The draws below stay inside these ranges and needn't reach their ends.
Inputs may be any that keep to these rules, and one draw needn't show every extreme that they name: `routes`: each row names 2 different experts. In the rows of one device (aligned blocks of 256 rows) no expert is named by more than 24 rows, and in some blocks one expert is named by exactly 24 rows.
All inputs are finite; a program needn't handle non-finite values.
Results may differ from the reference program's by a relative error of at most 0.019.
The reference program's roundings to bfloat16 on the way count: a program that leaves them out, or rounds other values in their place, can miss the bound.
Values may be sent and summed in bfloat16 or wider, within the bound.
No kernel may reach another device: no remote copies, remote signals or barrier semaphores. Data moves between devices by JAX's collectives and lax.ppermute only.
A program may use at most 128 MiB of HBM per device.

```python
import math
import jax
import jax.numpy as jnp
import numpy as np
from jax import lax

D = 2048
ATTENTION_HEADS = 16
PLAIN_HEAD_DIM = 64
ROPE = 32
VALUE_HEAD_DIM = 64
LATENT_WIDTH = 512
EXPERT_FF = 4096
TOP = 2
TOK_DEV = 256
MLA_W = 1024
MICRO_TOKENS = 8192
EXPERTS = 32
CAP = 24
N_EP = 32
N_TP = 16


def draw_queries(key, part):
    base_values = jax.random.normal(key, (MICRO_TOKENS, ATTENTION_HEADS * (PLAIN_HEAD_DIM + ROPE)), jnp.float32) * 2.0
    return jnp.clip(base_values, -600.0, 600.0).astype(jnp.bfloat16)


def block_scale(rng, shape, split, low, largest):
    factor_of, own = 1.0, jax.random.fold_in(rng, 6)
    for dim, shards_of in split:
        heights = jnp.exp(jax.random.uniform(jax.random.fold_in(own, dim), (shards_of,), jnp.float32, low / len(split), largest / len(split)))
        factor_of = factor_of * jnp.repeat(heights, shape[dim] // shards_of).reshape([-1 if axis == dim else 1 for axis in range(len(shape))])
    return factor_of


def assign_block(rng, own, number, rows, number_of, top, limit, skew):
    sequence = jax.random.permutation(rng, number_of)
    crowded, usual = shares(number_of, rows * top, limit, skew, True), shares(number_of, rows * top, limit, skew, False)
    places = jnp.arange(number_of)

    def named(sizes, offset_by):
        used = int((sizes > 0).sum())
        fixed = max(1, used // 4)
        shifted = fixed + (places - fixed + offset_by * (used - fixed)) % max(1, number_of - fixed)
        return jnp.zeros((number_of,), jnp.int32).at[sequence[jnp.where(places < fixed, places, shifted)]].set(jnp.asarray(sizes, jnp.int32))

    sizes = jnp.where(number % 4 == 0, named(crowded, number // 4), named(usual, number - number // 4 - 1))
    mixed = jax.random.permutation(jax.random.fold_in(own, 3), number_of)
    source_of, receiver = mixed[0:number_of // 2 * 2:2], mixed[1:number_of // 2 * 2:2]
    room = jnp.minimum(sizes[source_of] - 1, limit - sizes[receiver]) // 2
    room = jnp.where((source_of == sequence[0]) | (receiver == sequence[0]) | (sizes[receiver] == 0), 0, jnp.maximum(room, 0))
    shifted = jax.random.randint(jax.random.fold_in(own, 4), (number_of // 2,), 0, 1 << 20) % (room + 1)
    sizes = sizes.at[source_of].add(-shifted).at[receiver].add(shifted)
    members = jnp.searchsorted(jnp.cumsum(sizes), jnp.arange(rows * top), side="right").astype(jnp.int32)
    table = members.reshape(top, rows).T
    table = table[jax.random.permutation(jax.random.fold_in(own, 1), rows)]
    offset_by = jax.random.randint(jax.random.fold_in(own, 2), (rows, 1), 0, top)
    return jnp.take_along_axis(table, (jnp.arange(top)[None, :] + offset_by) % top, axis=1)


def shares(number_of, total, bound, skew, full):
    portions = [(1 << 20) // math.isqrt(standing ** skew) + 1 for standing in range(1, number_of + 1)]
    largest = bound if full else min(bound, max(-(-total // number_of), total * portions[0] // sum(portions)))
    least = 1 if total - largest >= number_of - 1 else 0
    given, spare = [largest] + [least] * (number_of - 1), total - largest - least * (number_of - 1)
    while spare > 0:
        free = [i for i in range(1, number_of) if given[i] < largest] or [i for i in range(1, number_of) if given[i] < bound]
        mass, remaining = sum([portions[i] for i in free]), spare
        for i in free:
            extra = min(bound - given[i], max(1, remaining * portions[i] // mass), spare)
            given[i] = given[i] + extra
            spare = spare - extra
    return np.array(given)


def bell_draw(stream_key, extent, deviation, limit, pieces=(), held_as=jnp.bfloat16):
    drawn = jax.random.normal(stream_key, extent, jnp.float32) * deviation
    if len(pieces) > 0:
        drawn = block_scale(stream_key, extent, pieces, -0.22, 0.18) * drawn
    return jnp.clip(drawn, min=-limit, max=limit).astype(held_as)


def setup_inputs(seed: int = 0) -> dict:
    key_list = jax.random.split(jax.random.key(seed), 14)
    queries = draw_queries(jax.random.fold_in(key_list[13], 71), 0)
    compressed_key_value = bell_draw(key_list[1], (MICRO_TOKENS, LATENT_WIDTH), 1.0, 6.0, ((0, 32),))
    rope_key = bell_draw(key_list[2], (MICRO_TOKENS, ROPE), 1.0, 6.0, ((0, 32),))
    latent_norm_gain = jnp.clip(1.0 + 0.18 * jax.random.normal(key_list[3], (LATENT_WIDTH,), jnp.float32), 0.1, 1.9)
    latent_to_key_value = bell_draw(key_list[4], (LATENT_WIDTH, ATTENTION_HEADS * (PLAIN_HEAD_DIM + VALUE_HEAD_DIM)), LATENT_WIDTH ** -0.5, 0.25, ((1, 16),))
    out_proj = bell_draw(key_list[5], (MLA_W, D), ATTENTION_HEADS ** -0.5, 1.5, ((1, 16),))
    moe_input = bell_draw(key_list[6], (MICRO_TOKENS, D), 1.0, 6.0, ((0, 32),))
    moe_gain = jnp.clip(1.0 + 0.18 * jax.random.normal(key_list[7], (D,), jnp.float32), 0.1, 1.9)
    routes_keys = jax.random.split(jax.random.fold_in(key_list[8], 1), MICRO_TOKENS // TOK_DEV)
    routes_turns = jax.random.permutation(jax.random.fold_in(key_list[8], 3), MICRO_TOKENS // TOK_DEV)
    routes = jax.vmap(lambda own, number: assign_block(jax.random.fold_in(key_list[8], 2), own, number, TOK_DEV, EXPERTS, TOP, CAP, 2))(routes_keys, routes_turns).reshape((MICRO_TOKENS, TOP))
    route_weight = jnp.clip(0.2 + 0.8 * jax.random.uniform(key_list[9], (MICRO_TOKENS, TOP), jnp.float32) ** block_scale(key_list[9], (MICRO_TOKENS, TOP), ((0, 32),), -0.2, 0.2), 0.2, 1.0)
    gate_weight = bell_draw(key_list[10], (EXPERTS, D, EXPERT_FF), D ** -0.5, 0.125, ((0, 32), (2, 16)))
    up_weight = bell_draw(key_list[11], (EXPERTS, D, EXPERT_FF), D ** -0.5, 0.125, ((0, 32), (2, 16)))
    down_weight = bell_draw(key_list[12], (EXPERTS, EXPERT_FF, D), EXPERT_FF ** -0.5, 0.09375, ((0, 32), (1, 16)))
    return {"queries": queries, "compressed_key_value": compressed_key_value, "rope_key": rope_key, "latent_norm_gain": latent_norm_gain, "latent_to_key_value": latent_to_key_value, "out_proj": out_proj, "moe_input": moe_input, "moe_gain": moe_gain, "routes": routes, "route_weight": route_weight, "gate_weight": gate_weight, "up_weight": up_weight, "down_weight": down_weight}


EPSILON = 1e-06
ROPE_BASE_VALUE = 10000.0

def rms_scale(values, gain_vector):
    floats = values.astype(jnp.float32)
    return floats * lax.rsqrt(lax.optimization_barrier(jnp.mean(floats * floats, axis=-1, keepdims=True)) + EPSILON) * gain_vector.astype(jnp.float32)

def rotary(values, positions):
    full_width = values.shape[-1]
    half_dim = full_width // 2
    frequency = ROPE_BASE_VALUE ** (-jnp.arange(half_dim, dtype=jnp.float32) * 2.0 / full_width)
    angles = positions[..., None] * frequency
    cosine = jnp.cos(angles)
    sine_part = jnp.sin(angles)
    first_half = values[..., :half_dim]
    second_half = values[..., half_dim:]
    return jnp.concatenate([first_half * cosine - second_half * sine_part, second_half * cosine + first_half * sine_part], axis=-1)

def slot_table(block_routes, capacity, experts):
    flat_routes = block_routes.reshape(-1).astype(jnp.int32)
    onehot_table = (flat_routes[:, None] == jnp.arange(experts, dtype=jnp.int32)[None, :]).astype(jnp.int32)
    earlier = jnp.cumsum(onehot_table, axis=0) - onehot_table
    slot_index = lax.optimization_barrier(jnp.sum(earlier * onehot_table, axis=1)).astype(jnp.int32)
    destination = (flat_routes * capacity + slot_index).astype(jnp.int32)
    token_count = block_routes.shape[0]
    source_rows = (jnp.arange(flat_routes.shape[0], dtype=jnp.int32) // block_routes.shape[1]).astype(jnp.int32)
    source_table = jnp.full((experts * capacity,), token_count, jnp.int32).at[destination].set(source_rows)
    return (destination, source_table)

def reference(queries, compressed_key_value, rope_key, latent_norm_gain, latent_to_key_value, out_proj, moe_input, moe_gain, routes, route_weight, gate_weight, up_weight, down_weight):
    positions = jnp.arange(MICRO_TOKENS, dtype=jnp.float32)
    query_heads = queries.reshape(MICRO_TOKENS, ATTENTION_HEADS, PLAIN_HEAD_DIM + ROPE)
    query_nope = query_heads[..., :PLAIN_HEAD_DIM]
    query_rope = rotary(query_heads[..., PLAIN_HEAD_DIM:].astype(jnp.float32), positions[:, None]).astype(jnp.bfloat16)
    latent_normed = rms_scale(compressed_key_value, latent_norm_gain).astype(jnp.bfloat16)
    key_value = jnp.dot(latent_normed, latent_to_key_value, preferred_element_type=jnp.float32).astype(jnp.bfloat16)
    key_value = key_value.reshape(MICRO_TOKENS, ATTENTION_HEADS, PLAIN_HEAD_DIM + VALUE_HEAD_DIM)
    key_rope = rotary(rope_key.astype(jnp.float32), positions).astype(jnp.bfloat16)
    score_scale = (PLAIN_HEAD_DIM + ROPE) ** (-0.5)

    def one_head(inputs):
        head_nope, head_rope, head_kv = inputs
        key_nope = head_kv[:, :PLAIN_HEAD_DIM]
        head_values = head_kv[:, PLAIN_HEAD_DIM:]

        def one_block(block_inputs):
            block_nope, block_rope = block_inputs
            scores = (jnp.dot(block_nope, key_nope.T, preferred_element_type=jnp.float32) + jnp.dot(block_rope, key_rope.T, preferred_element_type=jnp.float32)) * score_scale
            row_max = lax.optimization_barrier(jnp.max(scores, axis=-1, keepdims=True))
            weights = jnp.exp(scores - row_max)
            row_total = lax.optimization_barrier(jnp.sum(weights, axis=-1, keepdims=True))
            mixed_rows = jnp.dot(weights.astype(jnp.bfloat16), head_values, preferred_element_type=jnp.float32) / row_total
            return mixed_rows.astype(jnp.bfloat16)
        blocks_out = lax.map(one_block, (head_nope.reshape(N_EP, TOK_DEV, PLAIN_HEAD_DIM), head_rope.reshape(N_EP, TOK_DEV, ROPE)))
        return blocks_out.reshape(MICRO_TOKENS, VALUE_HEAD_DIM)
    per_head = lax.map(one_head, (query_nope.transpose(1, 0, 2), query_rope.transpose(1, 0, 2), key_value.transpose(1, 0, 2)))
    attended = per_head.transpose(1, 0, 2).reshape(MICRO_TOKENS, ATTENTION_HEADS * VALUE_HEAD_DIM)
    attention_out = jnp.dot(attended, out_proj, preferred_element_type=jnp.float32).astype(jnp.bfloat16)
    normed = rms_scale(moe_input, moe_gain).astype(jnp.bfloat16)
    destination, source_table = jax.vmap(lambda block_routes: slot_table(block_routes, CAP, EXPERTS))(routes.reshape(N_EP, TOK_DEV, TOP))
    padded = jnp.concatenate([normed.reshape(N_EP, TOK_DEV, D), jnp.zeros((N_EP, 1, D), jnp.bfloat16)], axis=1)
    outgoing = jax.vmap(lambda table_rows, row_index: table_rows[row_index])(padded, source_table)
    per_expert = outgoing.reshape(N_EP, EXPERTS, CAP, D).transpose(1, 0, 2, 3).reshape(EXPERTS, N_EP * CAP, D)
    width_block = EXPERT_FF // N_TP

    def one_expert(inputs):
        expert_rows, gate_matrix, up_matrix, down_matrix = inputs
        gate_value = jnp.dot(expert_rows, gate_matrix, preferred_element_type=jnp.float32)
        up_value = jnp.dot(expert_rows, up_matrix, preferred_element_type=jnp.float32)
        hidden = (jax.nn.silu(gate_value) * up_value).astype(jnp.bfloat16)
        partial_sums = jnp.einsum('rjf,jfd->jrd', hidden.reshape(-1, N_TP, width_block).astype(jnp.float32), down_matrix.reshape(N_TP, width_block, D).astype(jnp.float32))
        rounded = lax.optimization_barrier(partial_sums.astype(jnp.bfloat16))
        return lax.optimization_barrier(jnp.sum(rounded.astype(jnp.float32), axis=0)).astype(jnp.bfloat16)
    results = lax.map(one_expert, (per_expert, gate_weight, up_weight, down_weight))
    returned = results.reshape(EXPERTS, N_EP, CAP, D).transpose(1, 0, 2, 3).reshape(N_EP, EXPERTS * CAP, D)
    picked = jax.vmap(lambda table_rows, row_index: table_rows[row_index])(returned, destination)
    weighted = picked.astype(jnp.float32).reshape(N_EP, TOK_DEV, TOP, D) * route_weight.reshape(N_EP, TOK_DEV, TOP, 1)
    expert_out = lax.optimization_barrier(jnp.sum(weighted, axis=2)).reshape(MICRO_TOKENS, D).astype(jnp.bfloat16)
    return (attention_out, expert_out)
```

```python
import math

import jax
import jax.numpy as jnp
from jax import lax
from jax.experimental import pallas as pl
from jax.experimental.pallas import tpu as pltpu
from jax.sharding import PartitionSpec as P

PLAIN_HEAD_DIM = 64
ROPE = 32
VALUE_HEAD_DIM = 64
LANES = 128

EPSILON = 1e-06
ROPE_BASE_VALUE = 10000.0

VMEM = pl.BlockSpec(memory_space=pltpu.VMEM)
SMEM = pl.BlockSpec(memory_space=pltpu.SMEM)


def kernel_call(body, out_shape, in_specs, out_specs, flops, limit=48):
    return pl.pallas_call(
        body,
        out_shape=out_shape,
        in_specs=in_specs,
        out_specs=out_specs,
        compiler_params=pltpu.CompilerParams(vmem_limit_bytes=limit * 1024 * 1024),
        cost_estimate=pl.CostEstimate(flops=flops, transcendentals=0, bytes_accessed=0),
    )


def rms_scale(values, gain_vector):
    floats = values.astype(jnp.float32)
    return (
        floats
        * lax.rsqrt(jnp.mean(floats * floats, axis=-1, keepdims=True) + EPSILON)
        * gain_vector
    )


def to_everyone(array, axis, groups, count):
    return lax.all_to_all(
        jnp.broadcast_to(array[None], (count, *array.shape)),
        axis,
        0,
        0,
        tiled=True,
        axis_index_groups=groups,
    )


def pack_rows(index, moe_input, gain, routes, capacity, expert_total):
    rows, width = moe_input.shape
    places = expert_total * capacity
    top = routes.shape[1]

    def body(index_ref, input_ref, gain_ref, routes_ref, out_ref, place_ref):
        floats = input_ref[...].astype(jnp.float32)
        scale = lax.rsqrt(jnp.mean(floats * floats, axis=-1, keepdims=True) + EPSILON)
        start = pl.multiple_of(index_ref[0] * LANES, LANES)
        own = input_ref[:, pl.ds(start, LANES)].astype(jnp.float32)
        normed = (own * scale * gain_ref[:, pl.ds(start, LANES)]).astype(jnp.bfloat16)
        chosen = routes_ref[...]
        expert = lax.broadcasted_iota(jnp.int32, (rows, expert_total), 1)
        named = [chosen[:, k : k + 1] == expert for k in range(top)]
        either = named[0]
        for other in named[1:]:
            either = either | other
        ones = jnp.where(either, 1.0, 0.0).astype(jnp.bfloat16)
        lower = lax.broadcasted_iota(jnp.int32, (rows, rows), 0) > lax.broadcasted_iota(
            jnp.int32, (rows, rows), 1
        )
        lower = jnp.where(lower, 1.0, 0.0).astype(jnp.bfloat16)
        earlier = jnp.dot(lower, ones, preferred_element_type=jnp.float32)
        value = earlier + expert.astype(jnp.float32) * float(capacity)
        slots = lax.broadcasted_iota(jnp.int32, (rows, places), 1)
        hit = None
        for k in range(top):
            place = jnp.sum(jnp.where(named[k], value, 0.0), axis=1, keepdims=True).astype(
                jnp.int32
            )
            place_ref[:, k : k + 1] = place
            here = slots == place
            hit = here if hit is None else hit | here
        select = jnp.where(hit, 1.0, 0.0).astype(jnp.bfloat16)
        out_ref[...] = lax.dot_general(
            select, normed, (((0,), (0,)), ((), ())), preferred_element_type=jnp.float32
        ).astype(jnp.bfloat16)

    return kernel_call(
        body,
        (
            jax.ShapeDtypeStruct((places, LANES), jnp.bfloat16),
            jax.ShapeDtypeStruct((rows, top), jnp.int32),
        ),
        [SMEM, VMEM, VMEM, VMEM],
        (VMEM, VMEM),
        2 * rows * places * LANES,
    )(index, moe_input, gain, routes)


def attend(query, key_value, score_scale):
    blocks, rows, _ = query.shape
    pieces, _, length = key_value.shape
    factor = score_scale * math.log2(math.e)
    first_value = PLAIN_HEAD_DIM + ROPE

    def body(query_ref, key_ref, out_ref):
        def one_block(i, carry):
            q = query_ref[i]
            scores = [
                jnp.dot(q, key_ref[j, :LANES, :], preferred_element_type=jnp.float32)
                for j in range(pieces)
            ]
            top = scores[0]
            for s in scores[1:]:
                top = jnp.maximum(top, s)
            top = jnp.max(top, axis=1, keepdims=True) * factor
            total = None
            mixed = None
            for j in range(pieces):
                weight = jnp.exp2(scores[j] * factor - top)
                total = weight if total is None else total + weight
                part = lax.dot_general(
                    weight.astype(jnp.bfloat16),
                    key_ref[j, first_value:, :],
                    (((1,), (1,)), ((), ())),
                    preferred_element_type=jnp.float32,
                )
                mixed = part if mixed is None else mixed + part
            total = jnp.sum(total, axis=1, keepdims=True)
            out_ref[i, :, :VALUE_HEAD_DIM] = (mixed / total).astype(jnp.bfloat16)
            log_total = top + jnp.log2(total)
            high = log_total.astype(jnp.bfloat16).astype(jnp.float32)
            middle = (log_total - high).astype(jnp.bfloat16).astype(jnp.float32)
            low = log_total - high - middle
            lane = lax.broadcasted_iota(jnp.int32, (rows, LANES - VALUE_HEAD_DIM), 1)
            out_ref[i, :, VALUE_HEAD_DIM:] = jnp.where(
                lane == 0, high, jnp.where(lane == 1, middle, low)
            ).astype(jnp.bfloat16)
            return carry

        lax.fori_loop(0, blocks, one_block, 0)

    return kernel_call(
        body,
        jax.ShapeDtypeStruct((blocks, rows, LANES), jnp.bfloat16),
        [VMEM, VMEM],
        VMEM,
        4 * blocks * rows * pieces * length * 2 * LANES,
    )(query, key_value)


def experts(rows_in, gates, ups, downs):
    blocks, rows, _ = rows_in.shape
    units = gates[0].shape[1]
    wide = 2 * LANES
    count = len(gates)

    def body(*refs):
        rows_ref = refs[0]
        gate_refs, up_refs, down_refs = (refs[1 + k * count : 1 + (k + 1) * count] for k in range(3))
        out_ref = refs[-1]
        hidden = []
        for gate_ref, up_ref in zip(gate_refs, up_refs):
            gate_value = jnp.zeros((rows, units), jnp.float32)
            up_value = jnp.zeros((rows, units), jnp.float32)
            for b in range(0, blocks, 2):
                part = jnp.concatenate([rows_ref[b], rows_ref[b + 1]], axis=1)
                span = slice(b * LANES, b * LANES + wide)
                gate_value += jnp.dot(part, gate_ref[span, :], preferred_element_type=jnp.float32)
                up_value += jnp.dot(part, up_ref[span, :], preferred_element_type=jnp.float32)
            silu = gate_value / (1.0 + jnp.exp(-gate_value))
            hidden.append((silu * up_value).astype(jnp.bfloat16))
        for b in range(0, blocks, 2):
            span = slice(b * LANES, b * LANES + wide)
            total = None
            for h, down_ref in zip(hidden, down_refs):
                part = jnp.dot(h, down_ref[:, span], preferred_element_type=jnp.float32)
                total = part if total is None else total + part
            total = total.astype(jnp.bfloat16)
            out_ref[b] = total[:, :LANES]
            out_ref[b + 1] = total[:, LANES:]

    return kernel_call(
        body,
        jax.ShapeDtypeStruct((blocks, rows, LANES), jnp.bfloat16),
        [VMEM] * (1 + 3 * count),
        VMEM,
        2 * rows * blocks * LANES * units * 3 * count,
    )(rows_in, *gates, *ups, *downs)


def combine(returned, places, route_weight):
    total, width = returned.shape
    rows, top = places.shape

    def body(rows_ref, place_ref, weight_ref, out_ref):
        slots = lax.broadcasted_iota(jnp.int32, (rows, total), 1)
        result = None
        for k in range(top):
            select = jnp.where(slots == place_ref[:, k : k + 1], 1.0, 0.0).astype(jnp.bfloat16)
            picked = jnp.dot(select, rows_ref[...], preferred_element_type=jnp.float32)
            part = picked * weight_ref[:, k : k + 1]
            result = part if result is None else result + part
        out_ref[...] = result.astype(jnp.bfloat16)

    return kernel_call(
        body,
        jax.ShapeDtypeStruct((rows, width), jnp.bfloat16),
        [VMEM] * 3,
        VMEM,
        2 * rows * total * width * top,
    )(returned, places, route_weight)


def make_local(z_count, x_count, tp_count):
    x_groups = [[x_count * z + x for x in range(x_count)] for z in range(z_count)]
    z_groups = [[x_count * z + x for z in range(z_count)] for x in range(x_count)]
    partner = [(i, i ^ 1) for i in range(tp_count)]

    def local(
        queries,
        compressed_key_value,
        rope_key,
        latent_norm_gain,
        latent_to_key_value,
        out_proj,
        moe_input,
        moe_gain,
        routes,
        route_weight,
        gate_weight,
        up_weight,
        down_weight,
    ):
        row_count = queries.shape[0]
        ep_count = z_count * x_count
        capacity = 3 * row_count // ep_count
        tp_index = lax.axis_index("tp").astype(jnp.int32)

        gates = [gate_weight[0]]
        ups = [up_weight[0]]
        downs = [down_weight[0]]
        for pair in (gates, ups, downs):
            pair.append(lax.ppermute(pair[0], "tp", partner))

        outgoing, places = pack_rows(
            tp_index.reshape(1), moe_input, moe_gain.reshape(1, -1), routes, capacity, ep_count
        )
        arrived = lax.all_to_all(
            outgoing.reshape(ep_count, capacity, LANES), "ep", 0, 0, tiled=True
        )

        offset = lax.axis_index("ep") * row_count
        positions = (offset + jnp.arange(row_count, dtype=jnp.int32)).astype(jnp.float32)
        half = ROPE // 2
        frequency = ROPE_BASE_VALUE ** (-jnp.arange(half, dtype=jnp.float32) * 2.0 / ROPE)
        angles = positions[:, None] * frequency
        cosine, sine = jnp.cos(angles), jnp.sin(angles)

        def rotated(values):
            first, second = values[:, :half], values[:, half:]
            return jnp.concatenate(
                [first * cosine - second * sine, second * cosine + first * sine], axis=1
            ).astype(jnp.bfloat16)

        query = jnp.concatenate(
            [
                queries[:, :PLAIN_HEAD_DIM],
                rotated(queries[:, PLAIN_HEAD_DIM:].astype(jnp.float32)),
                jnp.zeros((row_count, LANES - PLAIN_HEAD_DIM - ROPE), jnp.bfloat16),
            ],
            axis=1,
        )
        latent_normed = rms_scale(compressed_key_value, latent_norm_gain).astype(jnp.bfloat16)
        own_keys = lax.dot_general(
            latent_to_key_value,
            latent_normed,
            (((0,), (1,)), ((), ())),
            preferred_element_type=jnp.float32,
        ).astype(jnp.bfloat16)
        own_rope = rotated(rope_key.astype(jnp.float32)).T
        own_pack = jnp.concatenate(
            [own_keys[:PLAIN_HEAD_DIM], own_rope, own_keys[PLAIN_HEAD_DIM:]], axis=0
        )
        key_value = to_everyone(own_pack, "ep", z_groups, z_count)
        query_all = to_everyone(query, "ep", x_groups, x_count)
        partial_all = attend(query_all, key_value, (PLAIN_HEAD_DIM + ROPE) ** (-0.5))
        partials = lax.all_to_all(
            partial_all, "ep", 0, 0, tiled=True, axis_index_groups=x_groups
        ).astype(jnp.float32)
        log_total = jnp.sum(partials[:, :, VALUE_HEAD_DIM : VALUE_HEAD_DIM + 3], axis=2, keepdims=True)
        share = jnp.exp2(log_total - jnp.max(log_total, axis=0, keepdims=True))
        attended = jnp.sum(partials[:, :, :VALUE_HEAD_DIM] * share, axis=0) / jnp.sum(share, axis=0)
        everyone = lax.all_gather(attended.astype(jnp.bfloat16).T, "tp", axis=0, tiled=True)
        attention_out = lax.dot_general(
            everyone, out_proj, (((0,), (0,)), ((), ())), preferred_element_type=jnp.float32
        ).astype(jnp.bfloat16)

        halves = arrived.reshape(1, 2, ep_count * capacity // 2, LANES)
        spread = jnp.broadcast_to(halves, (tp_count // 2, *halves.shape[1:]))
        rows_in = lax.all_to_all(
            spread.reshape(tp_count, *halves.shape[2:]), "tp", 0, 0, tiled=True
        )
        partial_out = experts(rows_in, gates, ups, downs)
        groups = lax.all_to_all(partial_out, "tp", 0, 0, tiled=True)
        groups = groups.reshape(tp_count // 2, ep_count, capacity, LANES)
        summed = jnp.sum(groups.astype(jnp.float32), axis=0).astype(jnp.bfloat16)
        returned = lax.all_to_all(summed, "ep", 0, 0, tiled=True)
        expert_out = combine(returned.reshape(ep_count * capacity, LANES), places, route_weight)
        return (attention_out, expert_out)

    return local


def solution(mesh):
    ep_count = mesh.shape["ep"]
    x_count = 4
    return jax.shard_map(
        make_local(ep_count // x_count, x_count, mesh.shape["tp"]),
        mesh=mesh,
        in_specs=(
            P("ep", "tp"),
            P("ep", None),
            P("ep", None),
            P(),
            P(None, "tp"),
            P(None, "tp"),
            P("ep", None),
            P(),
            P("ep", None),
            P("ep", None),
            P("ep", None, "tp"),
            P("ep", None, "tp"),
            P("ep", "tp", None),
        ),
        out_specs=(P("ep", "tp"), P("ep", "tp")),
        check_vma=False,
    )
```

```python
import math

import jax
import jax.numpy as jnp
from jax import lax
from jax.experimental import pallas as pl
from jax.experimental.pallas import tpu as pltpu
from jax.sharding import PartitionSpec as P

PLAIN_HEAD_DIM = 64
ROPE = 32
VALUE_HEAD_DIM = 64
LANES = 128

EPSILON = 1e-06
ROPE_BASE_VALUE = 10000.0

VMEM = pl.BlockSpec(memory_space=pltpu.VMEM)
SMEM = pl.BlockSpec(memory_space=pltpu.SMEM)
ANY = pl.BlockSpec(memory_space=pl.ANY)


def kernel_call(body, out_shape, in_specs, out_specs, flops, limit=48):
    return pl.pallas_call(
        body,
        out_shape=out_shape,
        in_specs=in_specs,
        out_specs=out_specs,
        compiler_params=pltpu.CompilerParams(vmem_limit_bytes=limit * 1024 * 1024),
        cost_estimate=pl.CostEstimate(flops=flops, transcendentals=0, bytes_accessed=0),
    )


def rms_scale(values, gain_vector):
    floats = values.astype(jnp.float32)
    return (
        floats
        * lax.rsqrt(jnp.mean(floats * floats, axis=-1, keepdims=True) + EPSILON)
        * gain_vector
    )


def sequenced(array, *earlier):
    def body(array_ref, *refs):
        refs[-1][...] = array_ref[...]

    return kernel_call(
        body,
        jax.ShapeDtypeStruct(array.shape, array.dtype),
        [VMEM] + [ANY] * len(earlier),
        VMEM,
        array.size,
    )(array, *earlier)


LEAD = 8


def unpacked(message):
    blocks = message.shape[0]
    tails = message[:, 2 * LEAD :].reshape(blocks // 2, 2, LEAD, LANES)
    even, odd = tails[:, 0], tails[:, 1]
    upper = lax.broadcasted_iota(jnp.int32, even.shape, 1) < LEAD // 2
    left = jnp.where(upper, even, pltpu.roll(odd, LEAD // 2, 1))
    right = jnp.where(upper, pltpu.roll(even, LEAD // 2, 1), odd)
    return tuple(
        jnp.concatenate([lead.reshape(-1, LANES), tail.reshape(-1, LANES)], axis=0)
        for lead, tail in ((message[:, :LEAD], left), (message[:, LEAD : 2 * LEAD], right))
    )


def packed(left, right):
    blocks = left.shape[0] // (LEAD + LEAD // 2)
    split = blocks * LEAD
    left_tail = left[split:].reshape(blocks // 2, LEAD, LANES)
    right_tail = right[split:].reshape(blocks // 2, LEAD, LANES)
    upper = lax.broadcasted_iota(jnp.int32, left_tail.shape, 1) < LEAD // 2
    even = jnp.where(upper, left_tail, pltpu.roll(right_tail, LEAD // 2, 1))
    odd = jnp.where(upper, pltpu.roll(left_tail, LEAD // 2, 1), right_tail)
    tails = jnp.concatenate([even[:, None], odd[:, None]], axis=1).reshape(blocks, LEAD, LANES)
    return jnp.concatenate(
        [
            left[:split].reshape(blocks, LEAD, LANES),
            right[:split].reshape(blocks, LEAD, LANES),
            tails,
        ],
        axis=1,
    )


def pack_rows(index, moe_input, gain, routes, capacity, expert_total):
    rows, width = moe_input.shape
    places = expert_total * capacity
    half = capacity // 2
    top = routes.shape[1]
    wide = 2 * LANES

    def body(index_ref, input_ref, gain_ref, routes_ref, out_ref, place_ref):
        floats = input_ref[...].astype(jnp.float32)
        scale = lax.rsqrt(jnp.mean(floats * floats, axis=-1, keepdims=True) + EPSILON)
        start = pl.multiple_of(index_ref[0] * wide, wide)
        own = input_ref[:, pl.ds(start, wide)].astype(jnp.float32)
        normed = (own * scale * gain_ref[:, pl.ds(start, wide)]).astype(jnp.bfloat16)
        chosen = routes_ref[...]
        expert = lax.broadcasted_iota(jnp.int32, (rows, expert_total), 1)
        named = [chosen[:, k : k + 1] == expert for k in range(top)]
        either = named[0]
        for other in named[1:]:
            either = either | other
        ones = jnp.where(either, 1.0, 0.0).astype(jnp.bfloat16)
        lower = lax.broadcasted_iota(jnp.int32, (rows, rows), 0) > lax.broadcasted_iota(
            jnp.int32, (rows, rows), 1
        )
        lower = jnp.where(lower, 1.0, 0.0).astype(jnp.bfloat16)
        earlier = jnp.dot(lower, ones, preferred_element_type=jnp.float32)
        slot = earlier - (index_ref[1] * half).astype(jnp.float32)
        valid = (slot >= 0.0) & (slot < float(half))
        base = slot + expert.astype(jnp.float32) * float(capacity) + 1.0
        step = float(LEAD)
        values = (
            jnp.where(slot < step, base, base + step),
            jnp.where(slot < step, base + step, base + step + float(LEAD // 2)),
        )
        slots = lax.broadcasted_iota(jnp.int32, (rows, places), 1)
        total = None
        for side, value in enumerate(values):
            hit = None
            for k in range(top):
                place = jnp.sum(jnp.where(named[k] & valid, value, 0.0), axis=1, keepdims=True)
                place = place.astype(jnp.int32) - 1
                column = side * top + k
                place_ref[:, column : column + 1] = place
                here = slots == place
                hit = here if hit is None else hit | here
            part = lax.dot_general(
                jnp.where(hit, 1.0, 0.0).astype(jnp.bfloat16),
                normed[:, side * LANES : (side + 1) * LANES],
                (((0,), (0,)), ((), ())),
                preferred_element_type=jnp.float32,
            )
            total = part if total is None else total + part
        out_ref[...] = total.astype(jnp.bfloat16)

    return kernel_call(
        body,
        (
            jax.ShapeDtypeStruct((places, LANES), jnp.bfloat16),
            jax.ShapeDtypeStruct((rows, 2 * top), jnp.int32),
        ),
        [SMEM, VMEM, VMEM, VMEM],
        (VMEM, VMEM),
        4 * rows * places * LANES,
    )(index, moe_input, gain, routes)


def fan_out(arrived, copies):
    blocks = arrived.shape[0]
    rows = blocks * (LEAD + LEAD // 2)

    def body(in_ref, out_ref):
        left, right = unpacked(in_ref[...].astype(jnp.float32))
        both = jnp.concatenate([left, right], axis=1).astype(jnp.bfloat16)
        for i in range(copies):
            out_ref[i] = both

    return kernel_call(
        body,
        jax.ShapeDtypeStruct((copies, rows, 2 * LANES), jnp.bfloat16),
        [VMEM],
        VMEM,
        1,
    )(arrived)


def add_up(parts, blocks):
    count = parts.shape[0]

    def body(in_ref, out_ref):
        total = in_ref[0].astype(jnp.float32)
        for i in range(1, count):
            total += in_ref[i].astype(jnp.float32)
        out_ref[...] = packed(total[:, :LANES], total[:, LANES:]).astype(jnp.bfloat16)

    return kernel_call(
        body,
        jax.ShapeDtypeStruct((blocks, 3 * LEAD, LANES), jnp.bfloat16),
        [VMEM],
        VMEM,
        1,
    )(parts)


def attend(index, query, key_value, score_scale):
    blocks, rows, _ = query.shape
    pieces, _, length = key_value.shape
    factor = score_scale * math.log2(math.e)
    first_value = PLAIN_HEAD_DIM + ROPE

    def body(index_ref, query_ref, key_ref, *out_refs):
        for i, out_ref in enumerate(out_refs):
            q = query_ref[(index_ref[0] + i) % blocks]
            scores = [
                jnp.dot(q, key_ref[j, :LANES, :], preferred_element_type=jnp.float32)
                for j in range(pieces)
            ]
            top = scores[0]
            for s in scores[1:]:
                top = jnp.maximum(top, s)
            top = jnp.max(top, axis=1, keepdims=True) * factor
            total = None
            mixed = None
            for j in range(pieces):
                weight = jnp.exp2(scores[j] * factor - top)
                total = weight if total is None else total + weight
                part = lax.dot_general(
                    weight.astype(jnp.bfloat16),
                    key_ref[j, first_value:, :],
                    (((1,), (1,)), ((), ())),
                    preferred_element_type=jnp.float32,
                )
                mixed = part if mixed is None else mixed + part
            total = jnp.sum(total, axis=1, keepdims=True)
            out_ref[:, :VALUE_HEAD_DIM] = (mixed / total).astype(jnp.bfloat16)
            log_total = top + jnp.log2(total)
            high = log_total.astype(jnp.bfloat16).astype(jnp.float32)
            middle = (log_total - high).astype(jnp.bfloat16).astype(jnp.float32)
            low = log_total - high - middle
            lane = lax.broadcasted_iota(jnp.int32, (rows, LANES - VALUE_HEAD_DIM), 1)
            out_ref[:, VALUE_HEAD_DIM:] = jnp.where(
                lane == 0, high, jnp.where(lane == 1, middle, low)
            ).astype(jnp.bfloat16)

    return kernel_call(
        body,
        tuple(jax.ShapeDtypeStruct((rows, LANES), jnp.bfloat16) for _ in range(blocks)),
        [SMEM, VMEM, VMEM],
        (VMEM,) * blocks,
        4 * blocks * rows * pieces * length * 2 * LANES,
    )(index, query, key_value)


def merge(partials):
    rows = partials[0].shape[0]

    def body(*refs):
        out_ref = refs[-1]
        values = [r[...].astype(jnp.float32) for r in refs[:-1]]
        first = VALUE_HEAD_DIM
        logs = [
            v[:, first : first + 1] + v[:, first + 1 : first + 2] + v[:, first + 2 : first + 3]
            for v in values
        ]
        top = logs[0]
        for log in logs[1:]:
            top = jnp.maximum(top, log)
        shares = [jnp.exp2(log - top) for log in logs]
        mixed = values[0] * shares[0]
        total = shares[0]
        for value, share in zip(values[1:], shares[1:]):
            mixed += value * share
            total += share
        out_ref[...] = (mixed / total).T[:VALUE_HEAD_DIM].astype(jnp.bfloat16)

    return kernel_call(
        body,
        jax.ShapeDtypeStruct((VALUE_HEAD_DIM, rows), jnp.bfloat16),
        [VMEM] * len(partials),
        VMEM,
        1,
    )(*partials)


def experts(rows_in, gates, ups, downs):
    blocks, rows, wide = rows_in.shape
    units = gates[0].shape[1]
    count = len(gates)

    def body(*refs):
        rows_ref = refs[0]
        gate_refs, up_refs, down_refs = (refs[1 + k * count : 1 + (k + 1) * count] for k in range(3))
        out_ref = refs[-1]
        hidden = []
        for gate_ref, up_ref in zip(gate_refs, up_refs):
            gate_value = jnp.zeros((rows, units), jnp.float32)
            up_value = jnp.zeros((rows, units), jnp.float32)
            for b in range(blocks):
                part = rows_ref[b]
                span = slice(b * wide, (b + 1) * wide)
                gate_value += jnp.dot(part, gate_ref[span, :], preferred_element_type=jnp.float32)
                up_value += jnp.dot(part, up_ref[span, :], preferred_element_type=jnp.float32)
            silu = gate_value / (1.0 + jnp.exp(-gate_value))
            hidden.append((silu * up_value).astype(jnp.bfloat16))
        for b in range(blocks):
            span = slice(b * wide, (b + 1) * wide)
            total = None
            for h, down_ref in zip(hidden, down_refs):
                part = jnp.dot(h, down_ref[:, span], preferred_element_type=jnp.float32)
                total = part if total is None else total + part
            out_ref[b] = total.astype(jnp.bfloat16)

    return kernel_call(
        body,
        jax.ShapeDtypeStruct((blocks, rows, wide), jnp.bfloat16),
        [VMEM] * (1 + 3 * count),
        VMEM,
        2 * rows * blocks * wide * units * 3 * count,
    )(rows_in, *gates, *ups, *downs)


def combine(index, returned, places, route_weight):
    total, width = returned.shape
    rows, top = route_weight.shape

    def body(index_ref, rows_ref, place_ref, weight_ref, own_ref, other_ref):
        slots = lax.broadcasted_iota(jnp.int32, (rows, total), 1)
        sides = []
        for side in range(2):
            result = None
            for k in range(top):
                column = side * top + k
                select = jnp.where(slots == place_ref[:, column : column + 1], 1.0, 0.0)
                picked = jnp.dot(
                    select.astype(jnp.bfloat16), rows_ref[...], preferred_element_type=jnp.float32
                )
                part = picked * weight_ref[:, k : k + 1]
                result = part if result is None else result + part
            sides.append(result)
        first = index_ref[1] == 0
        own_ref[...] = jnp.where(first, sides[0], sides[1])
        other_ref[...] = jnp.where(first, sides[1], sides[0])

    shape = jax.ShapeDtypeStruct((rows, width), jnp.float32)
    return kernel_call(
        body,
        (shape, shape),
        [SMEM, VMEM, VMEM, VMEM],
        (VMEM, VMEM),
        4 * rows * total * width * top,
    )(index, returned, places, route_weight)


def make_local(z_count, x_count, tp_count):
    cores = 2
    y_count = tp_count // cores
    ep_count = z_count * x_count
    x_groups = [[x_count * z + x for x in range(x_count)] for z in range(z_count)]
    z_groups = [[x_count * z + x for z in range(z_count)] for x in range(x_count)]
    y_groups = [[cores * y + c for y in range(y_count)] for c in range(cores)]
    partner = [(i, i ^ 1) for i in range(tp_count)]

    def local(
        queries,
        compressed_key_value,
        rope_key,
        latent_norm_gain,
        latent_to_key_value,
        out_proj,
        moe_input,
        moe_gain,
        routes,
        route_weight,
        gate_weight,
        up_weight,
        down_weight,
    ):
        row_count = queries.shape[0]
        capacity = 3 * row_count // ep_count
        tp_index = lax.axis_index("tp").astype(jnp.int32)
        ep_index = lax.axis_index("ep").astype(jnp.int32)
        place_index = jnp.stack([tp_index // cores, tp_index % cores])

        outgoing, places = pack_rows(
            place_index, moe_input, moe_gain.reshape(1, -1), routes, capacity, ep_count
        )
        arrived = lax.all_to_all(
            outgoing.reshape(ep_count, capacity, LANES), "ep", 0, 0, tiled=True
        )

        gates, ups, downs = [gate_weight[0]], [up_weight[0]], [down_weight[0]]
        for pair in (gates, ups, downs):
            pair.append(lax.ppermute(pair[0], "tp", partner))

        positions = (ep_index * row_count + jnp.arange(row_count, dtype=jnp.int32)).astype(
            jnp.float32
        )
        half = ROPE // 2
        frequency = ROPE_BASE_VALUE ** (-jnp.arange(half, dtype=jnp.float32) * 2.0 / ROPE)
        angles = positions[:, None] * frequency
        cosine, sine = jnp.cos(angles), jnp.sin(angles)

        def rotated(values):
            first, second = values[:, :half], values[:, half:]
            return jnp.concatenate(
                [first * cosine - second * sine, second * cosine + first * sine], axis=1
            ).astype(jnp.bfloat16)

        query = jnp.concatenate(
            [
                queries[:, :PLAIN_HEAD_DIM],
                rotated(queries[:, PLAIN_HEAD_DIM:].astype(jnp.float32)),
                jnp.zeros((row_count, LANES - PLAIN_HEAD_DIM - ROPE), jnp.bfloat16),
            ],
            axis=1,
        )
        latent_normed = rms_scale(compressed_key_value, latent_norm_gain).astype(jnp.bfloat16)
        own_keys = lax.dot_general(
            latent_to_key_value,
            latent_normed,
            (((0,), (1,)), ((), ())),
            preferred_element_type=jnp.float32,
        ).astype(jnp.bfloat16)
        own_rope = rotated(rope_key.astype(jnp.float32)).T
        own_pack = jnp.concatenate(
            [own_keys[:PLAIN_HEAD_DIM], own_rope, own_keys[PLAIN_HEAD_DIM:]], axis=0
        )
        query_all = lax.all_gather(
            sequenced(query, outgoing), "ep", axis=0, axis_index_groups=x_groups
        )
        key_value = lax.all_gather(
            sequenced(own_pack, arrived), "ep", axis=0, axis_index_groups=z_groups
        )
        partial_all = attend(
            (ep_index % x_count).reshape(1),
            query_all,
            key_value,
            (PLAIN_HEAD_DIM + ROPE) ** (-0.5),
        )

        rows_in = lax.all_to_all(
            fan_out(arrived, y_count), "tp", 0, 0, tiled=True, axis_index_groups=y_groups
        )
        partial_out = experts(rows_in, gates, ups, downs)
        groups = lax.all_to_all(
            partial_out, "tp", 0, 0, tiled=True, axis_index_groups=y_groups
        )

        partials = [sequenced(partial_all[0], partial_out)] + [
            lax.ppermute(
                sequenced(partial_all[i], partial_out),
                "ep",
                [
                    (x_count * z + x, x_count * z + (x + i) % x_count)
                    for z in range(z_count)
                    for x in range(x_count)
                ],
            )
            for i in range(1, x_count)
        ]
        everyone = lax.all_gather(merge(partials), "tp", axis=0, tiled=True)
        attention_out = lax.dot_general(
            everyone, out_proj, (((0,), (0,)), ((), ())), preferred_element_type=jnp.float32
        ).astype(jnp.bfloat16)

        returned = lax.all_to_all(add_up(groups, ep_count), "ep", 0, 0, tiled=True)
        own, other = combine(
            place_index, returned.reshape(ep_count * capacity, LANES), places, route_weight
        )
        expert_out = (own + lax.ppermute(other, "tp", partner)).astype(jnp.bfloat16)
        return (attention_out, expert_out)

    return local


def solution(mesh):
    ep_count = mesh.shape["ep"]
    x_count = 4
    return jax.shard_map(
        make_local(ep_count // x_count, x_count, mesh.shape["tp"]),
        mesh=mesh,
        in_specs=(
            P("ep", "tp"),
            P("ep", None),
            P("ep", None),
            P(),
            P(None, "tp"),
            P(None, "tp"),
            P("ep", None),
            P(),
            P("ep", None),
            P("ep", None),
            P("ep", None, "tp"),
            P("ep", None, "tp"),
            P("ep", "tp", None),
        ),
        out_specs=(P("ep", "tp"), P("ep", "tp")),
        check_vma=False,
    )
```

```python
import math

import jax
import jax.numpy as jnp
from jax import lax
from jax.experimental import pallas as pl
from jax.experimental.pallas import tpu as pltpu
from jax.sharding import PartitionSpec as P

PLAIN_HEAD_DIM = 64
ROPE = 32
VALUE_HEAD_DIM = 64
LANES = 128

EPSILON = 1e-06
ROPE_BASE_VALUE = 10000.0

VMEM = pl.BlockSpec(memory_space=pltpu.VMEM)
SMEM = pl.BlockSpec(memory_space=pltpu.SMEM)
ANY = pl.BlockSpec(memory_space=pl.ANY)


def kernel_call(body, out_shape, in_specs, out_specs, flops, limit=48):
    return pl.pallas_call(
        body,
        out_shape=out_shape,
        in_specs=in_specs,
        out_specs=out_specs,
        compiler_params=pltpu.CompilerParams(vmem_limit_bytes=limit * 1024 * 1024),
        cost_estimate=pl.CostEstimate(flops=flops, transcendentals=0, bytes_accessed=0),
    )


def rms_scale(values, gain_vector):
    floats = values.astype(jnp.float32)
    return (
        floats
        * lax.rsqrt(jnp.mean(floats * floats, axis=-1, keepdims=True) + EPSILON)
        * gain_vector
    )


def sequenced(array, *earlier):
    def body(array_ref, *refs):
        refs[-1][...] = array_ref[...]

    return kernel_call(
        body,
        jax.ShapeDtypeStruct(array.shape, array.dtype),
        [VMEM] + [ANY] * len(earlier),
        VMEM,
        array.size,
    )(array, *earlier)


LEAD = 8


def unpacked(message):
    blocks = message.shape[0]
    tails = message[:, 2 * LEAD :].reshape(blocks // 2, 2, LEAD, LANES)
    even, odd = tails[:, 0], tails[:, 1]
    upper = lax.broadcasted_iota(jnp.int32, even.shape, 1) < LEAD // 2
    left = jnp.where(upper, even, pltpu.roll(odd, LEAD // 2, 1))
    right = jnp.where(upper, pltpu.roll(even, LEAD // 2, 1), odd)
    return tuple(
        jnp.concatenate([lead.reshape(-1, LANES), tail.reshape(-1, LANES)], axis=0)
        for lead, tail in ((message[:, :LEAD], left), (message[:, LEAD : 2 * LEAD], right))
    )


def packed(left, right):
    blocks = left.shape[0] // (LEAD + LEAD // 2)
    split = blocks * LEAD
    left_tail = left[split:].reshape(blocks // 2, LEAD, LANES)
    right_tail = right[split:].reshape(blocks // 2, LEAD, LANES)
    upper = lax.broadcasted_iota(jnp.int32, left_tail.shape, 1) < LEAD // 2
    even = jnp.where(upper, left_tail, pltpu.roll(right_tail, LEAD // 2, 1))
    odd = jnp.where(upper, pltpu.roll(left_tail, LEAD // 2, 1), right_tail)
    tails = jnp.concatenate([even[:, None], odd[:, None]], axis=1).reshape(blocks, LEAD, LANES)
    return jnp.concatenate(
        [
            left[:split].reshape(blocks, LEAD, LANES),
            right[:split].reshape(blocks, LEAD, LANES),
            tails,
        ],
        axis=1,
    )


def pack_rows(index, moe_input, gain, routes, capacity, expert_total):
    rows, width = moe_input.shape
    places = expert_total * capacity
    half = capacity // 2
    top = routes.shape[1]
    wide = 2 * LANES

    def body(index_ref, input_ref, gain_ref, routes_ref, out_ref, place_ref):
        floats = input_ref[...].astype(jnp.float32)
        scale = lax.rsqrt(jnp.mean(floats * floats, axis=-1, keepdims=True) + EPSILON)
        normed = (floats * scale * gain_ref[...]).astype(jnp.bfloat16)
        chosen = routes_ref[...]
        expert = lax.broadcasted_iota(jnp.int32, (rows, expert_total), 1)
        named = [chosen[:, k : k + 1] == expert for k in range(top)]
        either = named[0]
        for other in named[1:]:
            either = either | other
        ones = jnp.where(either, 1.0, 0.0).astype(jnp.bfloat16)
        lower = lax.broadcasted_iota(jnp.int32, (rows, rows), 0) > lax.broadcasted_iota(
            jnp.int32, (rows, rows), 1
        )
        lower = jnp.where(lower, 1.0, 0.0).astype(jnp.bfloat16)
        earlier = jnp.dot(lower, ones, preferred_element_type=jnp.float32)
        slot = earlier - (index_ref[1] * half).astype(jnp.float32)
        valid = (slot >= 0.0) & (slot < float(half))
        base = slot + expert.astype(jnp.float32) * float(capacity) + 1.0
        step = float(LEAD)
        values = (
            jnp.where(slot < step, base, base + step),
            jnp.where(slot < step, base + step, base + step + float(LEAD // 2)),
        )
        slots = lax.broadcasted_iota(jnp.int32, (rows, places), 1)
        selects = []
        for side, value in enumerate(values):
            hit = None
            for k in range(top):
                place = jnp.sum(jnp.where(named[k] & valid, value, 0.0), axis=1, keepdims=True)
                place = place.astype(jnp.int32) - 1
                column = side * top + k
                place_ref[:, column : column + 1] = place
                here = slots == place
                hit = here if hit is None else hit | here
            selects.append(jnp.where(hit, 1.0, 0.0).astype(jnp.bfloat16))
        for b in range(width // wide):
            total = None
            for side, select in enumerate(selects):
                first = b * wide + side * LANES
                part = lax.dot_general(
                    select,
                    normed[:, first : first + LANES],
                    (((0,), (0,)), ((), ())),
                    preferred_element_type=jnp.float32,
                )
                total = part if total is None else total + part
            out_ref[:, b] = total.reshape(expert_total, capacity, LANES).astype(jnp.bfloat16)

    return kernel_call(
        body,
        (
            jax.ShapeDtypeStruct((expert_total, width // wide, capacity, LANES), jnp.bfloat16),
            jax.ShapeDtypeStruct((rows, 2 * top), jnp.int32),
        ),
        [SMEM, VMEM, VMEM, VMEM],
        (VMEM, VMEM),
        2 * rows * places * width,
    )(index, moe_input, gain, routes)


def add_up(parts, blocks, *earlier):
    count = parts.shape[0]

    def body(in_ref, *refs):
        out_ref = refs[-1]
        total = in_ref[0].astype(jnp.float32)
        for i in range(1, count):
            total += in_ref[i].astype(jnp.float32)
        out_ref[...] = packed(total[:, :LANES], total[:, LANES:]).astype(jnp.bfloat16)

    return kernel_call(
        body,
        jax.ShapeDtypeStruct((blocks, 3 * LEAD, LANES), jnp.bfloat16),
        [VMEM] + [ANY] * len(earlier),
        VMEM,
        1,
    )(parts, *earlier)


def attend(index, query, key_value, score_scale):
    blocks, rows, _ = query.shape
    pieces, _, length = key_value.shape
    factor = score_scale * math.log2(math.e)
    first_value = PLAIN_HEAD_DIM + ROPE

    def body(index_ref, query_ref, key_ref, *out_refs):
        for i, out_ref in enumerate(out_refs):
            q = query_ref[(index_ref[0] + i) % blocks]
            scores = [
                jnp.dot(q, key_ref[j, :LANES, :], preferred_element_type=jnp.float32)
                for j in range(pieces)
            ]
            top = scores[0]
            for s in scores[1:]:
                top = jnp.maximum(top, s)
            top = jnp.max(top, axis=1, keepdims=True) * factor
            total = None
            mixed = None
            for j in range(pieces):
                weight = jnp.exp2(scores[j] * factor - top)
                total = weight if total is None else total + weight
                part = lax.dot_general(
                    weight.astype(jnp.bfloat16),
                    key_ref[j, first_value:, :],
                    (((1,), (1,)), ((), ())),
                    preferred_element_type=jnp.float32,
                )
                mixed = part if mixed is None else mixed + part
            total = jnp.sum(total, axis=1, keepdims=True)
            out_ref[:, :VALUE_HEAD_DIM] = (mixed / total).astype(jnp.bfloat16)
            log_total = top + jnp.log2(total)
            high = log_total.astype(jnp.bfloat16).astype(jnp.float32)
            middle = (log_total - high).astype(jnp.bfloat16).astype(jnp.float32)
            low = log_total - high - middle
            lane = lax.broadcasted_iota(jnp.int32, (rows, LANES - VALUE_HEAD_DIM), 1)
            out_ref[:, VALUE_HEAD_DIM:] = jnp.where(
                lane == 0, high, jnp.where(lane == 1, middle, low)
            ).astype(jnp.bfloat16)

    return kernel_call(
        body,
        tuple(jax.ShapeDtypeStruct((rows, LANES), jnp.bfloat16) for _ in range(blocks)),
        [SMEM, VMEM, VMEM],
        (VMEM,) * blocks,
        4 * blocks * rows * pieces * length * 2 * LANES,
    )(index, query, key_value)


def merge(partials):
    rows = partials[0].shape[0]

    def body(*refs):
        out_ref = refs[-1]
        values = [r[...].astype(jnp.float32) for r in refs[:-1]]
        first = VALUE_HEAD_DIM
        logs = [
            v[:, first : first + 1] + v[:, first + 1 : first + 2] + v[:, first + 2 : first + 3]
            for v in values
        ]
        top = logs[0]
        for log in logs[1:]:
            top = jnp.maximum(top, log)
        shares = [jnp.exp2(log - top) for log in logs]
        mixed = values[0] * shares[0]
        total = shares[0]
        for value, share in zip(values[1:], shares[1:]):
            mixed += value * share
            total += share
        out_ref[...] = (mixed / total).T[:VALUE_HEAD_DIM].astype(jnp.bfloat16)

    return kernel_call(
        body,
        jax.ShapeDtypeStruct((VALUE_HEAD_DIM, rows), jnp.bfloat16),
        [VMEM] * len(partials),
        VMEM,
        1,
    )(*partials)


def experts(messages, gates, ups, downs, *earlier):
    sources, blocks, _, _ = messages.shape
    rows = sources * (LEAD + LEAD // 2)
    wide = 2 * LANES
    units = gates[0].shape[1]
    count = len(gates)

    def body(*refs):
        rows_ref = refs[0]
        gate_refs, up_refs, down_refs = (refs[1 + k * count : 1 + (k + 1) * count] for k in range(3))
        out_ref = refs[-1]
        hidden = []
        parts = [
            jnp.concatenate(unpacked(rows_ref[:, b].astype(jnp.float32)), axis=1).astype(jnp.bfloat16)
            for b in range(blocks)
        ]
        for gate_ref, up_ref in zip(gate_refs, up_refs):
            gate_value = jnp.zeros((rows, units), jnp.float32)
            up_value = jnp.zeros((rows, units), jnp.float32)
            for b, part in enumerate(parts):
                span = slice(b * wide, (b + 1) * wide)
                gate_value += jnp.dot(part, gate_ref[span, :], preferred_element_type=jnp.float32)
                up_value += jnp.dot(part, up_ref[span, :], preferred_element_type=jnp.float32)
            silu = gate_value / (1.0 + jnp.exp(-gate_value))
            hidden.append((silu * up_value).astype(jnp.bfloat16))
        for b in range(blocks):
            span = slice(b * wide, (b + 1) * wide)
            total = None
            for h, down_ref in zip(hidden, down_refs):
                part = jnp.dot(h, down_ref[:, span], preferred_element_type=jnp.float32)
                total = part if total is None else total + part
            out_ref[b] = total.astype(jnp.bfloat16)

    return kernel_call(
        body,
        jax.ShapeDtypeStruct((blocks, rows, wide), jnp.bfloat16),
        [VMEM] * (1 + 3 * count) + [ANY] * len(earlier),
        VMEM,
        2 * rows * blocks * wide * units * 3 * count,
    )(messages, *gates, *ups, *downs, *earlier)


def combine(index, returned, places, route_weight):
    total, width = returned.shape
    rows, top = route_weight.shape

    def body(index_ref, rows_ref, place_ref, weight_ref, own_ref, other_ref):
        slots = lax.broadcasted_iota(jnp.int32, (rows, total), 1)
        sides = []
        for side in range(2):
            result = None
            for k in range(top):
                column = side * top + k
                select = jnp.where(slots == place_ref[:, column : column + 1], 1.0, 0.0)
                picked = jnp.dot(
                    select.astype(jnp.bfloat16), rows_ref[...], preferred_element_type=jnp.float32
                )
                part = picked * weight_ref[:, k : k + 1]
                result = part if result is None else result + part
            sides.append(result)
        first = index_ref[1] == 0
        own_ref[...] = jnp.where(first, sides[0], sides[1])
        other_ref[...] = jnp.where(first, sides[1], sides[0])

    shape = jax.ShapeDtypeStruct((rows, width), jnp.float32)
    return kernel_call(
        body,
        (shape, shape),
        [SMEM, VMEM, VMEM, VMEM],
        (VMEM, VMEM),
        4 * rows * total * width * top,
    )(index, returned, places, route_weight)


def make_local(z_count, x_count, tp_count):
    cores = 2
    y_count = tp_count // cores
    ep_count = z_count * x_count
    x_groups = [[x_count * z + x for x in range(x_count)] for z in range(z_count)]
    z_groups = [[x_count * z + x for z in range(z_count)] for x in range(x_count)]
    y_groups = [[cores * y + c for y in range(y_count)] for c in range(cores)]
    partner = [(i, i ^ 1) for i in range(tp_count)]

    def local(
        queries,
        compressed_key_value,
        rope_key,
        latent_norm_gain,
        latent_to_key_value,
        out_proj,
        moe_input,
        moe_gain,
        routes,
        route_weight,
        gate_weight,
        up_weight,
        down_weight,
    ):
        row_count = queries.shape[0]
        capacity = 3 * row_count // ep_count
        tp_index = lax.axis_index("tp").astype(jnp.int32)
        ep_index = lax.axis_index("ep").astype(jnp.int32)
        place_index = jnp.stack([tp_index // cores, tp_index % cores])

        outgoing, places = pack_rows(
            place_index, moe_input, moe_gain.reshape(1, -1), routes, capacity, ep_count
        )
        arrived = lax.all_to_all(outgoing, "ep", 0, 0, tiled=True)

        gates, ups, downs = [gate_weight[0]], [up_weight[0]], [down_weight[0]]
        for pair in (gates, ups, downs):
            pair.append(lax.ppermute(pair[0], "tp", partner))

        positions = (ep_index * row_count + jnp.arange(row_count, dtype=jnp.int32)).astype(
            jnp.float32
        )
        half = ROPE // 2
        frequency = ROPE_BASE_VALUE ** (-jnp.arange(half, dtype=jnp.float32) * 2.0 / ROPE)
        angles = positions[:, None] * frequency
        cosine, sine = jnp.cos(angles), jnp.sin(angles)

        def rotated(values):
            first, second = values[:, :half], values[:, half:]
            return jnp.concatenate(
                [first * cosine - second * sine, second * cosine + first * sine], axis=1
            ).astype(jnp.bfloat16)

        query = jnp.concatenate(
            [
                queries[:, :PLAIN_HEAD_DIM],
                rotated(queries[:, PLAIN_HEAD_DIM:].astype(jnp.float32)),
                jnp.zeros((row_count, LANES - PLAIN_HEAD_DIM - ROPE), jnp.bfloat16),
            ],
            axis=1,
        )
        latent_normed = rms_scale(compressed_key_value, latent_norm_gain).astype(jnp.bfloat16)
        own_keys = lax.dot_general(
            latent_to_key_value,
            latent_normed,
            (((0,), (1,)), ((), ())),
            preferred_element_type=jnp.float32,
        ).astype(jnp.bfloat16)
        own_rope = rotated(rope_key.astype(jnp.float32)).T
        own_pack = jnp.concatenate(
            [own_keys[:PLAIN_HEAD_DIM], own_rope, own_keys[PLAIN_HEAD_DIM:]], axis=0
        )
        key_value = lax.all_gather(
            sequenced(own_pack, outgoing), "ep", axis=0, axis_index_groups=z_groups
        )

        partial_out = experts(arrived, gates, ups, downs, key_value)
        groups = lax.all_to_all(
            partial_out, "tp", 0, 0, tiled=True, axis_index_groups=y_groups
        )

        query_all = lax.all_gather(
            sequenced(query, partial_out), "ep", axis=0, axis_index_groups=x_groups
        )
        partial_all = attend(
            (ep_index % x_count).reshape(1),
            query_all,
            key_value,
            (PLAIN_HEAD_DIM + ROPE) ** (-0.5),
        )
        partials = [partial_all[0]] + [
            lax.ppermute(
                partial_all[i],
                "ep",
                [
                    (x_count * z + x, x_count * z + (x + i) % x_count)
                    for z in range(z_count)
                    for x in range(x_count)
                ],
            )
            for i in range(1, x_count)
        ]
        attended = merge(partials)
        summed = add_up(groups, ep_count, attended)
        everyone = lax.all_gather(sequenced(attended, summed), "tp", axis=0, tiled=True)
        attention_out = lax.dot_general(
            everyone, out_proj, (((0,), (0,)), ((), ())), preferred_element_type=jnp.float32
        ).astype(jnp.bfloat16)

        returned = lax.all_to_all(summed, "ep", 0, 0, tiled=True)
        own, other = combine(
            place_index, returned.reshape(ep_count * capacity, LANES), places, route_weight
        )
        expert_out = (own + lax.ppermute(other, "tp", partner)).astype(jnp.bfloat16)
        return (attention_out, expert_out)

    return local


def solution(mesh):
    ep_count = mesh.shape["ep"]
    x_count = 4
    return jax.shard_map(
        make_local(ep_count // x_count, x_count, mesh.shape["tp"]),
        mesh=mesh,
        in_specs=(
            P("ep", "tp"),
            P("ep", None),
            P("ep", None),
            P(),
            P(None, "tp"),
            P(None, "tp"),
            P("ep", None),
            P(),
            P("ep", None),
            P("ep", None),
            P("ep", None, "tp"),
            P("ep", None, "tp"),
            P("ep", "tp", None),
        ),
        out_specs=(P("ep", "tp"), P("ep", "tp")),
        check_vma=False,
    )
```

```python
import math

import jax
import jax.numpy as jnp
from jax import lax
from jax.experimental import pallas as pl
from jax.experimental.pallas import tpu as pltpu
from jax.sharding import PartitionSpec as P


PLAIN_HEAD_DIM = 64
ROPE = 32
VALUE_HEAD_DIM = 64
LANES = 128

EPSILON = 1e-06
ROPE_BASE_VALUE = 10000.0


VMEM = pl.BlockSpec(memory_space=pltpu.VMEM)
SMEM = pl.BlockSpec(memory_space=pltpu.SMEM)
ANY = pl.BlockSpec(memory_space=pl.ANY)


def kernel_call(body, out_shape, in_specs, out_specs, flops, limit=48):
    return pl.pallas_call(
        body,
        out_shape=out_shape,
        in_specs=in_specs,
        out_specs=out_specs,
        compiler_params=pltpu.CompilerParams(vmem_limit_bytes=limit * 1024 * 1024),
        cost_estimate=pl.CostEstimate(flops=flops, transcendentals=0, bytes_accessed=0),
    )


def rms_scale(values, gain_vector):
    floats = values.astype(jnp.float32)
    return (
        floats
        * lax.rsqrt(jnp.mean(floats * floats, axis=-1, keepdims=True) + EPSILON)
        * gain_vector
    )


def to_everyone(array, axis, groups, count):
    return lax.all_to_all(
        jnp.broadcast_to(array[None], (count, *array.shape)),
        axis,
        0,
        0,
        tiled=True,
        axis_index_groups=groups,
    )


def sequenced(array, *earlier):
    def body(array_ref, *refs):
        refs[-1][...] = array_ref[...]

    return kernel_call(
        body,
        jax.ShapeDtypeStruct(array.shape, array.dtype),
        [VMEM] + [ANY] * len(earlier),
        VMEM,
        array.size,
    )(array, *earlier)


SHARE = 6
PARTS = 4


def message_rows(shape, dim):
    place = lax.broadcasted_iota(jnp.int32, shape, dim)
    source = jnp.floor((place.astype(jnp.float32) + 0.5) * (1.0 / SHARE)).astype(jnp.int32)
    return place + source * (SHARE * (PARTS - 1))


def pack_rows(index, moe_input, gain, routes, capacity, expert_total):
    rows, width = moe_input.shape
    places = expert_total * capacity
    top = routes.shape[1]
    wide = PARTS * LANES

    def body(index_ref, input_ref, gain_ref, routes_ref, out_ref, place_ref):
        floats = input_ref[...].astype(jnp.float32)
        scale = lax.rsqrt(jnp.mean(floats * floats, axis=-1, keepdims=True) + EPSILON)
        normed = (floats * scale * gain_ref[...]).astype(jnp.bfloat16)
        chosen = routes_ref[...]
        expert = lax.broadcasted_iota(jnp.int32, (rows, expert_total), 1)
        named = [chosen[:, k : k + 1] == expert for k in range(top)]
        either = named[0]
        for other in named[1:]:
            either = either | other
        ones = jnp.where(either, 1.0, 0.0).astype(jnp.bfloat16)
        lower = lax.broadcasted_iota(jnp.int32, (rows, rows), 0) > lax.broadcasted_iota(
            jnp.int32, (rows, rows), 1
        )
        lower = jnp.where(lower, 1.0, 0.0).astype(jnp.bfloat16)
        earlier = jnp.dot(lower, ones, preferred_element_type=jnp.float32)
        first_row = expert.astype(jnp.float32) * float(capacity)
        share = float(SHARE)

        def within(part):
            slot = earlier - part.astype(jnp.float32) * share
            return slot, (slot >= 0.0) & (slot < share)

        def pick(k, value, valid):
            chosen_value = jnp.where(named[k] & valid, value + 1.0, 0.0)
            return jnp.sum(chosen_value, axis=1, keepdims=True).astype(jnp.int32) - 1

        slot, valid = within(index_ref[0])
        starts = [pick(k, slot + first_row, valid) for k in range(top)]
        slots = lax.broadcasted_iota(jnp.int32, (rows, places), 1)
        selects = []
        for part in range(PARTS):
            hit = None
            for start in starts:
                target = jnp.where(start < 0, -1, start + part * SHARE)
                here = slots == target
                hit = here if hit is None else hit | here
            selects.append(jnp.where(hit, 1.0, 0.0).astype(jnp.bfloat16))
        for b in range(width // wide):
            total = None
            for part, select in enumerate(selects):
                first = b * wide + part * LANES
                piece = lax.dot_general(
                    select,
                    normed[:, first : first + LANES],
                    (((0,), (0,)), ((), ())),
                    preferred_element_type=jnp.float32,
                )
                total = piece if total is None else total + piece
            out_ref[:, b] = total.reshape(expert_total, capacity, LANES).astype(jnp.bfloat16)

        low_slot, low_valid = within(index_ref[1])
        high_slot, high_valid = within(index_ref[1] + 2)
        value = jnp.where(low_valid, low_slot, high_slot + 2.0 * share) + first_row
        for k in range(top):
            start = pick(k, value, low_valid | high_valid)
            for side in range(2):
                column = side * top + k
                place_ref[:, column : column + 1] = jnp.where(
                    start < 0, -1, start + side * SHARE
                )

    return kernel_call(
        body,
        (
            jax.ShapeDtypeStruct((expert_total, width // wide, capacity, LANES), jnp.bfloat16),
            jax.ShapeDtypeStruct((rows, 2 * top), jnp.int32),
        ),
        [SMEM, VMEM, VMEM, VMEM],
        (VMEM, VMEM),
        2 * rows * places * width,
    )(index, moe_input, gain, routes)


def add_up(parts, blocks, *earlier):
    count, rows, _ = parts.shape
    capacity = SHARE * PARTS

    def body(in_ref, *refs):
        out_ref = refs[-1]
        targets = message_rows((blocks * capacity, rows), 1)
        lines = lax.broadcasted_iota(jnp.int32, (blocks * capacity, rows), 0)
        total = None
        for parity in range(2):
            added = in_ref[parity].astype(jnp.float32)
            for i in range(parity + 2, count, 2):
                added += in_ref[i].astype(jnp.float32)
            added = added.astype(jnp.bfloat16)
            for side in range(2):
                offset = (2 * parity + side) * SHARE
                select = jnp.where(lines == targets + offset, 1.0, 0.0).astype(jnp.bfloat16)
                part = jnp.dot(
                    select,
                    added[:, side * LANES : (side + 1) * LANES],
                    preferred_element_type=jnp.float32,
                )
                total = part if total is None else total + part
        out_ref[...] = total.reshape(blocks, capacity, LANES).astype(jnp.bfloat16)

    return kernel_call(
        body,
        jax.ShapeDtypeStruct((blocks, capacity, LANES), jnp.bfloat16),
        [VMEM] + [ANY] * len(earlier),
        VMEM,
        1,
    )(parts, *earlier)


def attend(query, key_value, score_scale):
    blocks, rows, _ = query.shape
    pieces, _, length = key_value.shape
    factor = score_scale * math.log2(math.e)
    first_value = PLAIN_HEAD_DIM + ROPE

    def body(query_ref, key_ref, out_ref):
        for i in range(blocks):
            q = query_ref[i]
            scores = [
                jnp.dot(q, key_ref[j, :LANES, :], preferred_element_type=jnp.float32)
                for j in range(pieces)
            ]
            top = scores[0]
            for s in scores[1:]:
                top = jnp.maximum(top, s)
            top = jnp.max(top, axis=1, keepdims=True) * factor
            total = None
            mixed = None
            for j in range(pieces):
                weight = jnp.exp2(scores[j] * factor - top)
                total = weight if total is None else total + weight
                part = lax.dot_general(
                    weight.astype(jnp.bfloat16),
                    key_ref[j, first_value:, :],
                    (((1,), (1,)), ((), ())),
                    preferred_element_type=jnp.float32,
                )
                mixed = part if mixed is None else mixed + part
            total = jnp.sum(total, axis=1, keepdims=True)
            out_ref[i, :, :VALUE_HEAD_DIM] = (mixed / total).astype(jnp.bfloat16)
            log_total = top + jnp.log2(total)
            high = log_total.astype(jnp.bfloat16).astype(jnp.float32)
            middle = (log_total - high).astype(jnp.bfloat16).astype(jnp.float32)
            low = log_total - high - middle
            lane = lax.broadcasted_iota(jnp.int32, (rows, LANES - VALUE_HEAD_DIM), 1)
            out_ref[i, :, VALUE_HEAD_DIM:] = jnp.where(
                lane == 0, high, jnp.where(lane == 1, middle, low)
            ).astype(jnp.bfloat16)

    return kernel_call(
        body,
        jax.ShapeDtypeStruct((blocks, rows, LANES), jnp.bfloat16),
        [VMEM, VMEM],
        VMEM,
        4 * blocks * rows * pieces * length * 2 * LANES,
    )(query, key_value)


def merge(partials):
    count, rows, _ = partials.shape

    def body(in_ref, out_ref):
        values = [in_ref[i].astype(jnp.float32) for i in range(count)]
        first = VALUE_HEAD_DIM
        logs = [
            v[:, first : first + 1] + v[:, first + 1 : first + 2] + v[:, first + 2 : first + 3]
            for v in values
        ]
        top = logs[0]
        for log in logs[1:]:
            top = jnp.maximum(top, log)
        shares = [jnp.exp2(log - top) for log in logs]
        mixed = values[0] * shares[0]
        total = shares[0]
        for value, share in zip(values[1:], shares[1:]):
            mixed += value * share
            total += share
        out_ref[...] = (mixed / total).T[:VALUE_HEAD_DIM].astype(jnp.bfloat16)

    return kernel_call(
        body,
        jax.ShapeDtypeStruct((VALUE_HEAD_DIM, rows), jnp.bfloat16),
        [VMEM],
        VMEM,
        1,
    )(partials)


def hidden_units(messages, gates, ups):
    sources, blocks, capacity, _ = messages.shape
    rows = sources * SHARE
    units = gates[0].shape[1]
    count = len(gates)
    wide = 2 * LANES

    def body(rows_ref, *refs):
        gate_refs, up_refs, out_ref = refs[:count], refs[count : 2 * count], refs[-1]
        targets = message_rows((rows, sources * capacity), 0)
        lines = lax.broadcasted_iota(jnp.int32, (rows, sources * capacity), 1)
        selects = [
            jnp.where(lines == targets + part * SHARE, 1.0, 0.0).astype(jnp.bfloat16)
            for part in range(PARTS)
        ]
        parts = []
        for b in range(blocks):
            block = rows_ref[:, b].astype(jnp.float32).reshape(sources * capacity, LANES)
            block = block.astype(jnp.bfloat16)
            columns = [
                jnp.dot(select, block, preferred_element_type=jnp.float32).astype(jnp.bfloat16)
                for select in selects
            ]
            for part in range(0, PARTS, 2):
                parts.append(jnp.concatenate(columns[part : part + 2], axis=1))
        for g, (gate_ref, up_ref) in enumerate(zip(gate_refs, up_refs)):
            gate_value = jnp.zeros((rows, units), jnp.float32)
            up_value = jnp.zeros((rows, units), jnp.float32)
            for b, part in enumerate(parts):
                span = slice(b * wide, (b + 1) * wide)
                gate_value += jnp.dot(part, gate_ref[span, :], preferred_element_type=jnp.float32)
                up_value += jnp.dot(part, up_ref[span, :], preferred_element_type=jnp.float32)
            silu = gate_value / (1.0 + jnp.exp(-gate_value))
            out_ref[g] = (silu * up_value).astype(jnp.bfloat16)

    return kernel_call(
        body,
        jax.ShapeDtypeStruct((count, rows, units), jnp.bfloat16),
        [VMEM] * (1 + 2 * count),
        VMEM,
        4 * rows * gates[0].shape[0] * units * count,
    )(messages, *gates, *ups)


def project_down(hidden, downs, blocks, *earlier):
    count, rows, units = hidden.shape
    wide = downs[0].shape[1] // blocks

    def body(hidden_ref, *refs):
        out_ref = refs[-1]
        for b in range(blocks):
            span = slice(b * wide, (b + 1) * wide)
            total = None
            for g in range(count):
                part = jnp.dot(
                    hidden_ref[g], refs[g][:, span], preferred_element_type=jnp.float32
                )
                total = part if total is None else total + part
            out_ref[b] = total.astype(jnp.bfloat16)

    return kernel_call(
        body,
        jax.ShapeDtypeStruct((blocks, rows, wide), jnp.bfloat16),
        [VMEM] * (1 + count) + [ANY] * len(earlier),
        VMEM,
        2 * rows * units * count * wide * blocks,
    )(hidden, *downs, *earlier)


def combine(index, returned, places, route_weight):
    total, width = returned.shape
    rows, top = route_weight.shape

    def body(index_ref, rows_ref, place_ref, weight_ref, own_ref, other_ref):
        slots = lax.broadcasted_iota(jnp.int32, (rows, total), 1)
        sides = []
        for side in range(2):
            result = None
            for k in range(top):
                column = side * top + k
                select = jnp.where(slots == place_ref[:, column : column + 1], 1.0, 0.0)
                picked = jnp.dot(
                    select.astype(jnp.bfloat16), rows_ref[...], preferred_element_type=jnp.float32
                )
                part = picked * weight_ref[:, k : k + 1]
                result = part if result is None else result + part
            sides.append(result)
        first = index_ref[1] == 0
        own_ref[...] = jnp.where(first, sides[0], sides[1])
        other_ref[...] = jnp.where(first, sides[1], sides[0])

    shape = jax.ShapeDtypeStruct((rows, width), jnp.float32)
    return kernel_call(
        body,
        (shape, shape),
        [SMEM, VMEM, VMEM, VMEM],
        (VMEM, VMEM),
        4 * rows * total * width * top,
    )(index, returned, places, route_weight)


def make_local(z_count, x_count, tp_count):
    cores = 2
    y_count = tp_count // cores
    ep_count = z_count * x_count
    x_groups = [[x_count * z + x for x in range(x_count)] for z in range(z_count)]
    z_groups = [[x_count * z + x for z in range(z_count)] for x in range(x_count)]
    y_groups = [[cores * y + c for y in range(y_count)] for c in range(cores)]
    partner = [(i, i ^ 1) for i in range(tp_count)]
    neighbour = [(i, i ^ cores) for i in range(tp_count)]

    def local(
        queries,
        compressed_key_value,
        rope_key,
        latent_norm_gain,
        latent_to_key_value,
        out_proj,
        moe_input,
        moe_gain,
        routes,
        route_weight,
        gate_weight,
        up_weight,
        down_weight,
    ):
        row_count = queries.shape[0]
        capacity = 3 * row_count // ep_count
        tp_index = lax.axis_index("tp").astype(jnp.int32)
        ep_index = lax.axis_index("ep").astype(jnp.int32)
        place_index = jnp.stack([tp_index % PARTS, tp_index % cores])

        groups_of = [[gate_weight[0]], [up_weight[0]], [down_weight[0]]]
        for group in groups_of:
            group.append(lax.ppermute(group[0], "tp", neighbour))

        outgoing, places = pack_rows(
            place_index, moe_input, moe_gain.reshape(1, -1), routes, capacity, ep_count
        )
        arrived = lax.all_to_all(outgoing, "ep", 0, 0, tiled=True)

        for group in groups_of:
            group += [lax.ppermute(weight, "tp", partner) for weight in group[:2]]
        gates, ups, downs = groups_of

        positions = (ep_index * row_count + jnp.arange(row_count, dtype=jnp.int32)).astype(
            jnp.float32
        )
        half = ROPE // 2
        frequency = ROPE_BASE_VALUE ** (-jnp.arange(half, dtype=jnp.float32) * 2.0 / ROPE)
        angles = positions[:, None] * frequency
        cosine, sine = jnp.cos(angles), jnp.sin(angles)

        def rotated(values):
            first, second = values[:, :half], values[:, half:]
            return jnp.concatenate(
                [first * cosine - second * sine, second * cosine + first * sine], axis=1
            ).astype(jnp.bfloat16)

        query = jnp.concatenate(
            [
                queries[:, :PLAIN_HEAD_DIM],
                rotated(queries[:, PLAIN_HEAD_DIM:].astype(jnp.float32)),
                jnp.zeros((row_count, LANES - PLAIN_HEAD_DIM - ROPE), jnp.bfloat16),
            ],
            axis=1,
        )
        latent_normed = rms_scale(compressed_key_value, latent_norm_gain).astype(jnp.bfloat16)
        own_keys = lax.dot_general(
            latent_to_key_value,
            latent_normed,
            (((0,), (1,)), ((), ())),
            preferred_element_type=jnp.float32,
        ).astype(jnp.bfloat16)
        own_rope = rotated(rope_key.astype(jnp.float32)).T
        own_pack = jnp.concatenate(
            [own_keys[:PLAIN_HEAD_DIM], own_rope, own_keys[PLAIN_HEAD_DIM:]], axis=0
        )
        key_value = to_everyone(sequenced(own_pack, arrived), "ep", z_groups, z_count)
        hidden = hidden_units(arrived, gates, ups)
        query_all = to_everyone(sequenced(query, key_value, hidden), "ep", x_groups, x_count)
        partial_all = attend(query_all, key_value, (PLAIN_HEAD_DIM + ROPE) ** (-0.5))
        partials = lax.all_to_all(
            partial_all, "ep", 0, 0, tiled=True, axis_index_groups=x_groups
        )

        partial_out = project_down(hidden, downs, y_count, partials)
        groups = lax.all_to_all(
            partial_out, "tp", 0, 0, tiled=True, axis_index_groups=y_groups
        )
        attended = merge(partials)
        everyone = lax.all_gather(
            sequenced(attended, partial_out), "tp", axis=0, tiled=True
        )
        summed = add_up(groups, ep_count, everyone)
        attention_out = lax.dot_general(
            everyone, out_proj, (((0,), (0,)), ((), ())), preferred_element_type=jnp.float32
        ).astype(jnp.bfloat16)

        returned = lax.all_to_all(summed, "ep", 0, 0, tiled=True)
        own, other = combine(
            place_index, returned.reshape(ep_count * capacity, LANES), places, route_weight
        )
        expert_out = (own + lax.ppermute(other, "tp", partner)).astype(jnp.bfloat16)
        return (attention_out, expert_out)

    return local


def solution(mesh):
    ep_count = mesh.shape["ep"]
    x_count = 4
    local = make_local(ep_count // x_count, x_count, mesh.shape["tp"])

    return jax.shard_map(
        local,
        mesh=mesh,
        in_specs=(
            P("ep", "tp"),
            P("ep", None),
            P("ep", None),
            P(),
            P(None, "tp"),
            P(None, "tp"),
            P("ep", None),
            P(),
            P("ep", None),
            P("ep", None),
            P("ep", None, "tp"),
            P("ep", None, "tp"),
            P("ep", "tp", None),
        ),
        out_specs=(P("ep", "tp"), P("ep", "tp")),
        check_vma=False,
    )
```

```python
import math

import jax
import jax.numpy as jnp
from jax import lax
from jax.experimental import pallas as pl
from jax.experimental.pallas import tpu as pltpu
from jax.sharding import PartitionSpec as P


PLAIN_HEAD_DIM = 64
ROPE = 32
VALUE_HEAD_DIM = 64
LANES = 128

EPSILON = 1e-06
ROPE_BASE_VALUE = 10000.0


VMEM = pl.BlockSpec(memory_space=pltpu.VMEM)
SMEM = pl.BlockSpec(memory_space=pltpu.SMEM)
ANY = pl.BlockSpec(memory_space=pl.ANY)


def kernel_call(body, out_shape, in_specs, out_specs, flops, limit=48):
    return pl.pallas_call(
        body,
        out_shape=out_shape,
        in_specs=in_specs,
        out_specs=out_specs,
        compiler_params=pltpu.CompilerParams(vmem_limit_bytes=limit * 1024 * 1024),
        cost_estimate=pl.CostEstimate(flops=flops, transcendentals=0, bytes_accessed=0),
    )


def rms_scale(values, gain_vector):
    floats = values.astype(jnp.float32)
    return (
        floats
        * lax.rsqrt(jnp.mean(floats * floats, axis=-1, keepdims=True) + EPSILON)
        * gain_vector
    )


def to_everyone(array, axis, groups, count):
    return lax.all_to_all(
        jnp.broadcast_to(array[None], (count, *array.shape)),
        axis,
        0,
        0,
        tiled=True,
        axis_index_groups=groups,
    )


def sequenced(array, *earlier):
    def body(array_ref, *refs):
        refs[-1][...] = array_ref[...]

    return kernel_call(
        body,
        jax.ShapeDtypeStruct(array.shape, array.dtype),
        [VMEM] + [ANY] * len(earlier),
        VMEM,
        array.size,
    )(array, *earlier)


SHARE = 6
PARTS = 4


def message_rows(shape, dim):
    place = lax.broadcasted_iota(jnp.int32, shape, dim)
    source = jnp.floor((place.astype(jnp.float32) + 0.5) * (1.0 / SHARE)).astype(jnp.int32)
    return place + source * (SHARE * (PARTS - 1))


def pack_rows(index, moe_input, gain, routes, capacity, expert_total):
    rows, width = moe_input.shape
    places = expert_total * capacity
    top = routes.shape[1]
    wide = PARTS * LANES

    def body(index_ref, input_ref, gain_ref, routes_ref, out_ref, place_ref):
        floats = input_ref[...].astype(jnp.float32)
        scale = lax.rsqrt(jnp.mean(floats * floats, axis=-1, keepdims=True) + EPSILON)
        normed = (floats * scale * gain_ref[...]).astype(jnp.bfloat16)
        chosen = routes_ref[...]
        expert = lax.broadcasted_iota(jnp.int32, (rows, expert_total), 1)
        named = [chosen[:, k : k + 1] == expert for k in range(top)]
        either = named[0]
        for other in named[1:]:
            either = either | other
        ones = jnp.where(either, 1.0, 0.0).astype(jnp.bfloat16)
        lower = lax.broadcasted_iota(jnp.int32, (rows, rows), 0) > lax.broadcasted_iota(
            jnp.int32, (rows, rows), 1
        )
        lower = jnp.where(lower, 1.0, 0.0).astype(jnp.bfloat16)
        earlier = jnp.dot(lower, ones, preferred_element_type=jnp.float32)
        first_row = expert.astype(jnp.float32) * float(capacity)
        share = float(SHARE)

        def within(part):
            slot = earlier - part.astype(jnp.float32) * share
            return slot, (slot >= 0.0) & (slot < share)

        def pick(k, value, valid):
            chosen_value = jnp.where(named[k] & valid, value + 1.0, 0.0)
            return jnp.sum(chosen_value, axis=1, keepdims=True).astype(jnp.int32) - 1

        slot, valid = within(index_ref[0])
        starts = [pick(k, slot + first_row, valid) for k in range(top)]
        slots = lax.broadcasted_iota(jnp.int32, (rows, places), 1)
        selects = []
        for part in range(PARTS):
            hit = None
            for start in starts:
                target = jnp.where(start < 0, -1, start + part * SHARE)
                here = slots == target
                hit = here if hit is None else hit | here
            selects.append(jnp.where(hit, 1.0, 0.0).astype(jnp.bfloat16))
        for b in range(width // wide):
            total = None
            for part, select in enumerate(selects):
                first = b * wide + part * LANES
                piece = lax.dot_general(
                    select,
                    normed[:, first : first + LANES],
                    (((0,), (0,)), ((), ())),
                    preferred_element_type=jnp.float32,
                )
                total = piece if total is None else total + piece
            out_ref[:, b] = total.reshape(expert_total, capacity, LANES).astype(jnp.bfloat16)

        low_slot, low_valid = within(index_ref[1])
        high_slot, high_valid = within(index_ref[1] + 2)
        value = jnp.where(low_valid, low_slot, high_slot + 2.0 * share) + first_row
        for k in range(top):
            start = pick(k, value, low_valid | high_valid)
            for side in range(2):
                column = side * top + k
                place_ref[:, column : column + 1] = jnp.where(
                    start < 0, -1, start + side * SHARE
                )

    return kernel_call(
        body,
        (
            jax.ShapeDtypeStruct((expert_total, width // wide, capacity, LANES), jnp.bfloat16),
            jax.ShapeDtypeStruct((rows, 2 * top), jnp.int32),
        ),
        [SMEM, VMEM, VMEM, VMEM],
        (VMEM, VMEM),
        2 * rows * places * width,
    )(index, moe_input, gain, routes)


def add_up(parts, blocks, *earlier):
    count, rows, _ = parts.shape
    capacity = SHARE * PARTS

    def body(in_ref, *refs):
        out_ref = refs[-1]
        targets = message_rows((blocks * capacity, rows), 1)
        lines = lax.broadcasted_iota(jnp.int32, (blocks * capacity, rows), 0)
        total = None
        for parity in range(2):
            added = in_ref[parity].astype(jnp.float32)
            for i in range(parity + 2, count, 2):
                added += in_ref[i].astype(jnp.float32)
            added = added.astype(jnp.bfloat16)
            for side in range(2):
                offset = (2 * parity + side) * SHARE
                select = jnp.where(lines == targets + offset, 1.0, 0.0).astype(jnp.bfloat16)
                part = jnp.dot(
                    select,
                    added[:, side * LANES : (side + 1) * LANES],
                    preferred_element_type=jnp.float32,
                )
                total = part if total is None else total + part
        out_ref[...] = total.reshape(blocks, capacity, LANES).astype(jnp.bfloat16)

    return kernel_call(
        body,
        jax.ShapeDtypeStruct((blocks, capacity, LANES), jnp.bfloat16),
        [VMEM] + [ANY] * len(earlier),
        VMEM,
        1,
    )(parts, *earlier)


def attend(index, query, key_value, score_scale, *earlier):
    blocks, rows, _ = query.shape
    pieces, _, length = key_value.shape
    factor = score_scale * math.log2(math.e)
    first_value = PLAIN_HEAD_DIM + ROPE

    def body(index_ref, query_ref, key_ref, *refs):
        for i, out_ref in enumerate(refs[-blocks:]):
            q = query_ref[(index_ref[0] + i) % blocks]
            scores = [
                jnp.dot(q, key_ref[j, :LANES, :], preferred_element_type=jnp.float32)
                for j in range(pieces)
            ]
            top = scores[0]
            for s in scores[1:]:
                top = jnp.maximum(top, s)
            top = jnp.max(top, axis=1, keepdims=True) * factor
            total = None
            mixed = None
            for j in range(pieces):
                weight = jnp.exp2(scores[j] * factor - top)
                total = weight if total is None else total + weight
                part = lax.dot_general(
                    weight.astype(jnp.bfloat16),
                    key_ref[j, first_value:, :],
                    (((1,), (1,)), ((), ())),
                    preferred_element_type=jnp.float32,
                )
                mixed = part if mixed is None else mixed + part
            total = jnp.sum(total, axis=1, keepdims=True)
            out_ref[:, :VALUE_HEAD_DIM] = (mixed / total).astype(jnp.bfloat16)
            log_total = top + jnp.log2(total)
            high = log_total.astype(jnp.bfloat16).astype(jnp.float32)
            middle = (log_total - high).astype(jnp.bfloat16).astype(jnp.float32)
            low = log_total - high - middle
            lane = lax.broadcasted_iota(jnp.int32, (rows, LANES - VALUE_HEAD_DIM), 1)
            out_ref[:, VALUE_HEAD_DIM:] = jnp.where(
                lane == 0, high, jnp.where(lane == 1, middle, low)
            ).astype(jnp.bfloat16)

    return kernel_call(
        body,
        tuple(jax.ShapeDtypeStruct((rows, LANES), jnp.bfloat16) for _ in range(blocks)),
        [SMEM, VMEM, VMEM] + [ANY] * len(earlier),
        (VMEM,) * blocks,
        4 * blocks * rows * pieces * length * 2 * LANES,
    )(index, query, key_value, *earlier)


def merge(partials):
    rows = partials[0].shape[0]

    def body(*refs):
        out_ref = refs[-1]
        values = [r[...].astype(jnp.float32) for r in refs[:-1]]
        first = VALUE_HEAD_DIM
        logs = [
            v[:, first : first + 1] + v[:, first + 1 : first + 2] + v[:, first + 2 : first + 3]
            for v in values
        ]
        top = logs[0]
        for log in logs[1:]:
            top = jnp.maximum(top, log)
        shares = [jnp.exp2(log - top) for log in logs]
        mixed = values[0] * shares[0]
        total = shares[0]
        for value, share in zip(values[1:], shares[1:]):
            mixed += value * share
            total += share
        out_ref[...] = (mixed / total).T[:VALUE_HEAD_DIM].astype(jnp.bfloat16)

    return kernel_call(
        body,
        jax.ShapeDtypeStruct((VALUE_HEAD_DIM, rows), jnp.bfloat16),
        [VMEM] * len(partials),
        VMEM,
        1,
    )(*partials)


def hidden_units(messages, gates, ups):
    sources, blocks, capacity, _ = messages.shape
    rows = sources * SHARE
    units = gates[0].shape[1]
    count = len(gates)
    wide = 2 * LANES

    def body(rows_ref, *refs):
        gate_refs, up_refs, out_ref = refs[:count], refs[count : 2 * count], refs[-1]
        targets = message_rows((rows, sources * capacity), 0)
        lines = lax.broadcasted_iota(jnp.int32, (rows, sources * capacity), 1)
        selects = [
            jnp.where(lines == targets + part * SHARE, 1.0, 0.0).astype(jnp.bfloat16)
            for part in range(PARTS)
        ]
        parts = []
        for b in range(blocks):
            block = rows_ref[:, b].astype(jnp.float32).reshape(sources * capacity, LANES)
            block = block.astype(jnp.bfloat16)
            columns = [
                jnp.dot(select, block, preferred_element_type=jnp.float32).astype(jnp.bfloat16)
                for select in selects
            ]
            for part in range(0, PARTS, 2):
                parts.append(jnp.concatenate(columns[part : part + 2], axis=1))
        for g, (gate_ref, up_ref) in enumerate(zip(gate_refs, up_refs)):
            gate_value = jnp.zeros((rows, units), jnp.float32)
            up_value = jnp.zeros((rows, units), jnp.float32)
            for b, part in enumerate(parts):
                span = slice(b * wide, (b + 1) * wide)
                gate_value += jnp.dot(part, gate_ref[span, :], preferred_element_type=jnp.float32)
                up_value += jnp.dot(part, up_ref[span, :], preferred_element_type=jnp.float32)
            silu = gate_value / (1.0 + jnp.exp(-gate_value))
            out_ref[g] = (silu * up_value).astype(jnp.bfloat16)

    return kernel_call(
        body,
        jax.ShapeDtypeStruct((count, rows, units), jnp.bfloat16),
        [VMEM] * (1 + 2 * count),
        VMEM,
        4 * rows * gates[0].shape[0] * units * count,
    )(messages, *gates, *ups)


def project_down(hidden, downs, blocks, *earlier):
    count, rows, units = hidden.shape
    wide = downs[0].shape[1] // blocks

    def body(hidden_ref, *refs):
        out_ref = refs[-1]
        for b in range(blocks):
            span = slice(b * wide, (b + 1) * wide)
            total = None
            for g in range(count):
                part = jnp.dot(
                    hidden_ref[g], refs[g][:, span], preferred_element_type=jnp.float32
                )
                total = part if total is None else total + part
            out_ref[b] = total.astype(jnp.bfloat16)

    return kernel_call(
        body,
        jax.ShapeDtypeStruct((blocks, rows, wide), jnp.bfloat16),
        [VMEM] * (1 + count) + [ANY] * len(earlier),
        VMEM,
        2 * rows * units * count * wide * blocks,
    )(hidden, *downs, *earlier)


def combine(index, returned, places, route_weight):
    total, width = returned.shape
    rows, top = route_weight.shape

    def body(index_ref, rows_ref, place_ref, weight_ref, own_ref, other_ref):
        slots = lax.broadcasted_iota(jnp.int32, (rows, total), 1)
        sides = []
        for side in range(2):
            result = None
            for k in range(top):
                column = side * top + k
                select = jnp.where(slots == place_ref[:, column : column + 1], 1.0, 0.0)
                picked = jnp.dot(
                    select.astype(jnp.bfloat16), rows_ref[...], preferred_element_type=jnp.float32
                )
                part = picked * weight_ref[:, k : k + 1]
                result = part if result is None else result + part
            sides.append(result)
        first = index_ref[1] == 0
        own_ref[...] = jnp.where(first, sides[0], sides[1])
        other_ref[...] = jnp.where(first, sides[1], sides[0])

    shape = jax.ShapeDtypeStruct((rows, width), jnp.float32)
    return kernel_call(
        body,
        (shape, shape),
        [SMEM, VMEM, VMEM, VMEM],
        (VMEM, VMEM),
        4 * rows * total * width * top,
    )(index, returned, places, route_weight)


def make_local(z_count, x_count, tp_count):
    cores = 2
    y_count = tp_count // cores
    ep_count = z_count * x_count
    x_groups = [[x_count * z + x for x in range(x_count)] for z in range(z_count)]
    z_groups = [[x_count * z + x for z in range(z_count)] for x in range(x_count)]
    y_groups = [[cores * y + c for y in range(y_count)] for c in range(cores)]
    partner = [(i, i ^ 1) for i in range(tp_count)]
    neighbour = [(i, i ^ cores) for i in range(tp_count)]

    def local(
        queries,
        compressed_key_value,
        rope_key,
        latent_norm_gain,
        latent_to_key_value,
        out_proj,
        moe_input,
        moe_gain,
        routes,
        route_weight,
        gate_weight,
        up_weight,
        down_weight,
    ):
        row_count = queries.shape[0]
        capacity = 3 * row_count // ep_count
        tp_index = lax.axis_index("tp").astype(jnp.int32)
        ep_index = lax.axis_index("ep").astype(jnp.int32)
        place_index = jnp.stack([tp_index % PARTS, tp_index % cores])

        groups_of = [[gate_weight[0]], [up_weight[0]], [down_weight[0]]]
        for group in groups_of:
            group.append(lax.ppermute(group[0], "tp", neighbour))

        outgoing, places = pack_rows(
            place_index, moe_input, moe_gain.reshape(1, -1), routes, capacity, ep_count
        )
        arrived = lax.all_to_all(outgoing, "ep", 0, 0, tiled=True)

        for group in groups_of:
            for weight in group[:2]:
                group.append(lax.ppermute(weight, "tp", partner))
        gates, ups, downs = groups_of

        positions = (ep_index * row_count + jnp.arange(row_count, dtype=jnp.int32)).astype(
            jnp.float32
        )
        half = ROPE // 2
        frequency = ROPE_BASE_VALUE ** (-jnp.arange(half, dtype=jnp.float32) * 2.0 / ROPE)
        angles = positions[:, None] * frequency
        cosine, sine = jnp.cos(angles), jnp.sin(angles)

        def rotated(values):
            first, second = values[:, :half], values[:, half:]
            return jnp.concatenate(
                [first * cosine - second * sine, second * cosine + first * sine], axis=1
            ).astype(jnp.bfloat16)

        query = jnp.concatenate(
            [
                queries[:, :PLAIN_HEAD_DIM],
                rotated(queries[:, PLAIN_HEAD_DIM:].astype(jnp.float32)),
                jnp.zeros((row_count, LANES - PLAIN_HEAD_DIM - ROPE), jnp.bfloat16),
            ],
            axis=1,
        )
        latent_normed = rms_scale(compressed_key_value, latent_norm_gain).astype(jnp.bfloat16)
        own_keys = lax.dot_general(
            latent_to_key_value,
            latent_normed,
            (((0,), (1,)), ((), ())),
            preferred_element_type=jnp.float32,
        ).astype(jnp.bfloat16)
        own_rope = rotated(rope_key.astype(jnp.float32)).T
        own_pack = jnp.concatenate(
            [own_keys[:PLAIN_HEAD_DIM], own_rope, own_keys[PLAIN_HEAD_DIM:]], axis=0
        )
        key_value = to_everyone(sequenced(own_pack, arrived), "ep", z_groups, z_count)
        hidden = hidden_units(arrived, gates, ups)
        query_all = to_everyone(sequenced(query, key_value, hidden), "ep", x_groups, x_count)

        partial_out = project_down(hidden, downs, y_count, query_all)
        groups = lax.all_to_all(
            partial_out, "tp", 0, 0, tiled=True, axis_index_groups=y_groups
        )

        partial_all = attend(
            (ep_index % x_count).reshape(1),
            query_all,
            key_value,
            (PLAIN_HEAD_DIM + ROPE) ** (-0.5),
            partial_out,
        )
        partials = [partial_all[0]] + [
            lax.ppermute(
                partial_all[i],
                "ep",
                [
                    (x_count * z + x, x_count * z + (x + i) % x_count)
                    for z in range(z_count)
                    for x in range(x_count)
                ],
            )
            for i in range(1, x_count)
        ]
        attended = merge(partials)
        summed = add_up(groups, ep_count, attended)
        everyone = lax.all_gather(sequenced(attended, summed), "tp", axis=0, tiled=True)
        attention_out = lax.dot_general(
            everyone, out_proj, (((0,), (0,)), ((), ())), preferred_element_type=jnp.float32
        ).astype(jnp.bfloat16)

        returned = lax.all_to_all(summed, "ep", 0, 0, tiled=True)
        own, other = combine(
            place_index, returned.reshape(ep_count * capacity, LANES), places, route_weight
        )
        expert_out = (own + lax.ppermute(other, "tp", partner)).astype(jnp.bfloat16)
        return (attention_out, expert_out)

    return local


def solution(mesh):
    ep_count = mesh.shape["ep"]
    x_count = 4
    local = make_local(ep_count // x_count, x_count, mesh.shape["tp"])

    return jax.shard_map(
        local,
        mesh=mesh,
        in_specs=(
            P("ep", "tp"),
            P("ep", None),
            P("ep", None),
            P(),
            P(None, "tp"),
            P(None, "tp"),
            P("ep", None),
            P(),
            P("ep", None),
            P("ep", None),
            P("ep", None, "tp"),
            P("ep", None, "tp"),
            P("ep", "tp", None),
        ),
        out_specs=(P("ep", "tp"), P("ep", "tp")),
        check_vma=False,
    )
```

```python
import math

import jax
import jax.numpy as jnp
from jax import lax
from jax.experimental import pallas as pl
from jax.experimental.pallas import tpu as pltpu
from jax.sharding import PartitionSpec as P


PLAIN_HEAD_DIM = 64
ROPE = 32
VALUE_HEAD_DIM = 64
LANES = 128

EPSILON = 1e-06
ROPE_BASE_VALUE = 10000.0


VMEM = pl.BlockSpec(memory_space=pltpu.VMEM)
SMEM = pl.BlockSpec(memory_space=pltpu.SMEM)
ANY = pl.BlockSpec(memory_space=pl.ANY)


def kernel_call(body, out_shape, in_specs, out_specs, flops, limit=48):
    return pl.pallas_call(
        body,
        out_shape=out_shape,
        in_specs=in_specs,
        out_specs=out_specs,
        compiler_params=pltpu.CompilerParams(vmem_limit_bytes=limit * 1024 * 1024),
        cost_estimate=pl.CostEstimate(flops=flops, transcendentals=0, bytes_accessed=0),
    )


def rms_scale(values, gain_vector):
    floats = values.astype(jnp.float32)
    return (
        floats
        * lax.rsqrt(jnp.mean(floats * floats, axis=-1, keepdims=True) + EPSILON)
        * gain_vector
    )


def to_everyone(array, axis, groups, count):
    return lax.all_to_all(
        jnp.broadcast_to(array[None], (count, *array.shape)),
        axis,
        0,
        0,
        tiled=True,
        axis_index_groups=groups,
    )


def sequenced(array, *earlier):
    def body(array_ref, *refs):
        refs[-1][...] = array_ref[...]

    return kernel_call(
        body,
        jax.ShapeDtypeStruct(array.shape, array.dtype),
        [VMEM] + [ANY] * len(earlier),
        VMEM,
        array.size,
    )(array, *earlier)


SHARE = 6
PARTS = 4


def message_rows(shape, dim):
    place = lax.broadcasted_iota(jnp.int32, shape, dim)
    source = jnp.floor((place.astype(jnp.float32) + 0.5) * (1.0 / SHARE)).astype(jnp.int32)
    return place + source * (SHARE * (PARTS - 1))


def pack_rows(index, moe_input, gain, routes, capacity, expert_total):
    rows, width = moe_input.shape
    places = expert_total * capacity
    top = routes.shape[1]
    wide = PARTS * LANES

    def body(index_ref, input_ref, gain_ref, routes_ref, out_ref, place_ref):
        floats = input_ref[...].astype(jnp.float32)
        scale = lax.rsqrt(jnp.mean(floats * floats, axis=-1, keepdims=True) + EPSILON)
        normed = (floats * scale * gain_ref[...]).astype(jnp.bfloat16)
        chosen = routes_ref[...]
        expert = lax.broadcasted_iota(jnp.int32, (rows, expert_total), 1)
        named = [chosen[:, k : k + 1] == expert for k in range(top)]
        either = named[0]
        for other in named[1:]:
            either = either | other
        ones = jnp.where(either, 1.0, 0.0).astype(jnp.bfloat16)
        lower = lax.broadcasted_iota(jnp.int32, (rows, rows), 0) > lax.broadcasted_iota(
            jnp.int32, (rows, rows), 1
        )
        lower = jnp.where(lower, 1.0, 0.0).astype(jnp.bfloat16)
        earlier = jnp.dot(lower, ones, preferred_element_type=jnp.float32)
        first_row = expert.astype(jnp.float32) * float(capacity)
        share = float(SHARE)

        def within(part):
            slot = earlier - part.astype(jnp.float32) * share
            return slot, (slot >= 0.0) & (slot < share)

        def pick(k, value, valid):
            chosen_value = jnp.where(named[k] & valid, value + 1.0, 0.0)
            return jnp.sum(chosen_value, axis=1, keepdims=True).astype(jnp.int32) - 1

        slot, valid = within(index_ref[0])
        starts = [pick(k, slot + first_row, valid) for k in range(top)]
        slots = lax.broadcasted_iota(jnp.int32, (rows, places), 1)
        selects = []
        for part in range(PARTS):
            hit = None
            for start in starts:
                target = jnp.where(start < 0, -1, start + part * SHARE)
                here = slots == target
                hit = here if hit is None else hit | here
            selects.append(jnp.where(hit, 1.0, 0.0).astype(jnp.bfloat16))
        for b in range(width // wide):
            total = None
            for part, select in enumerate(selects):
                first = b * wide + part * LANES
                piece = lax.dot_general(
                    select,
                    normed[:, first : first + LANES],
                    (((0,), (0,)), ((), ())),
                    preferred_element_type=jnp.float32,
                )
                total = piece if total is None else total + piece
            out_ref[:, b] = total.reshape(expert_total, capacity, LANES).astype(jnp.bfloat16)

        anywhere = earlier >= 0.0
        for k in range(top):
            place_ref[:, k : k + 1] = pick(k, earlier + first_row, anywhere)

    return kernel_call(
        body,
        (
            jax.ShapeDtypeStruct((expert_total, width // wide, capacity, LANES), jnp.bfloat16),
            jax.ShapeDtypeStruct((rows, top), jnp.int32),
        ),
        [SMEM, VMEM, VMEM, VMEM],
        (VMEM, VMEM),
        2 * rows * places * width,
    )(index, moe_input, gain, routes)


def add_up(parts, blocks, *earlier):
    count, rows, _ = parts.shape
    capacity = SHARE * PARTS

    def body(in_ref, *refs):
        out_ref = refs[-1]
        targets = message_rows((blocks * capacity, rows), 1)
        lines = lax.broadcasted_iota(jnp.int32, (blocks * capacity, rows), 0)
        total = None
        for part in range(PARTS):
            added = in_ref[part].astype(jnp.float32)
            for i in range(part + PARTS, count, PARTS):
                added += in_ref[i].astype(jnp.float32)
            select = jnp.where(lines == targets + part * SHARE, 1.0, 0.0).astype(jnp.bfloat16)
            piece = jnp.dot(
                select, added.astype(jnp.bfloat16), preferred_element_type=jnp.float32
            )
            total = piece if total is None else total + piece
        out_ref[...] = total.reshape(blocks, capacity, LANES).astype(jnp.bfloat16)

    return kernel_call(
        body,
        jax.ShapeDtypeStruct((blocks, capacity, LANES), jnp.bfloat16),
        [VMEM] + [ANY] * len(earlier),
        VMEM,
        1,
    )(parts, *earlier)


def attend(queries, key_value, score_scale, *earlier):
    blocks = len(queries)
    rows = queries[0].shape[0]
    pieces, _, length = key_value.shape
    factor = score_scale * math.log2(math.e)
    first_value = PLAIN_HEAD_DIM + ROPE

    def body(key_ref, *refs):
        for query_ref, out_ref in zip(refs[:blocks], refs[-blocks:]):
            q = query_ref[...]
            scores = [
                jnp.dot(q, key_ref[j, :LANES, :], preferred_element_type=jnp.float32)
                for j in range(pieces)
            ]
            top = scores[0]
            for s in scores[1:]:
                top = jnp.maximum(top, s)
            top = jnp.max(top, axis=1, keepdims=True) * factor
            total = None
            mixed = None
            for j in range(pieces):
                weight = jnp.exp2(scores[j] * factor - top)
                total = weight if total is None else total + weight
                part = lax.dot_general(
                    weight.astype(jnp.bfloat16),
                    key_ref[j, first_value:, :],
                    (((1,), (1,)), ((), ())),
                    preferred_element_type=jnp.float32,
                )
                mixed = part if mixed is None else mixed + part
            total = jnp.sum(total, axis=1, keepdims=True)
            out_ref[:, :VALUE_HEAD_DIM] = (mixed / total).astype(jnp.bfloat16)
            log_total = top + jnp.log2(total)
            high = log_total.astype(jnp.bfloat16).astype(jnp.float32)
            middle = (log_total - high).astype(jnp.bfloat16).astype(jnp.float32)
            low = log_total - high - middle
            lane = lax.broadcasted_iota(jnp.int32, (rows, LANES - VALUE_HEAD_DIM), 1)
            out_ref[:, VALUE_HEAD_DIM:] = jnp.where(
                lane == 0, high, jnp.where(lane == 1, middle, low)
            ).astype(jnp.bfloat16)

    return kernel_call(
        body,
        tuple(jax.ShapeDtypeStruct((rows, LANES), jnp.bfloat16) for _ in range(blocks)),
        [VMEM] * (1 + blocks) + [ANY] * len(earlier),
        (VMEM,) * blocks,
        4 * blocks * rows * pieces * length * 2 * LANES,
    )(key_value, *queries, *earlier)


def merge(partials):
    rows = partials[0].shape[0]

    def body(*refs):
        out_ref = refs[-1]
        values = [r[...].astype(jnp.float32) for r in refs[:-1]]
        first = VALUE_HEAD_DIM
        logs = [
            v[:, first : first + 1] + v[:, first + 1 : first + 2] + v[:, first + 2 : first + 3]
            for v in values
        ]
        top = logs[0]
        for log in logs[1:]:
            top = jnp.maximum(top, log)
        shares = [jnp.exp2(log - top) for log in logs]
        mixed = values[0] * shares[0]
        total = shares[0]
        for value, share in zip(values[1:], shares[1:]):
            mixed += value * share
            total += share
        out_ref[...] = (mixed / total).T[:VALUE_HEAD_DIM].astype(jnp.bfloat16)

    return kernel_call(
        body,
        jax.ShapeDtypeStruct((VALUE_HEAD_DIM, rows), jnp.bfloat16),
        [VMEM] * len(partials),
        VMEM,
        1,
    )(*partials)


def hidden_units(messages, gates, ups):
    sources, blocks, capacity, _ = messages.shape
    rows = sources * SHARE
    units = gates[0].shape[1]
    count = len(gates)
    wide = 2 * LANES

    def body(rows_ref, *refs):
        gate_refs, up_refs, out_ref = refs[:count], refs[count : 2 * count], refs[-1]
        targets = message_rows((rows, sources * capacity), 0)
        lines = lax.broadcasted_iota(jnp.int32, (rows, sources * capacity), 1)
        selects = [
            jnp.where(lines == targets + part * SHARE, 1.0, 0.0).astype(jnp.bfloat16)
            for part in range(PARTS)
        ]
        parts = []
        for b in range(blocks):
            block = rows_ref[:, b].astype(jnp.float32).reshape(sources * capacity, LANES)
            block = block.astype(jnp.bfloat16)
            columns = [
                jnp.dot(select, block, preferred_element_type=jnp.float32).astype(jnp.bfloat16)
                for select in selects
            ]
            for part in range(0, PARTS, 2):
                parts.append(jnp.concatenate(columns[part : part + 2], axis=1))
        for g, (gate_ref, up_ref) in enumerate(zip(gate_refs, up_refs)):
            gate_value = jnp.zeros((rows, units), jnp.float32)
            up_value = jnp.zeros((rows, units), jnp.float32)
            for b, part in enumerate(parts):
                span = slice(b * wide, (b + 1) * wide)
                gate_value += jnp.dot(part, gate_ref[span, :], preferred_element_type=jnp.float32)
                up_value += jnp.dot(part, up_ref[span, :], preferred_element_type=jnp.float32)
            silu = gate_value / (1.0 + jnp.exp(-gate_value))
            out_ref[g] = (silu * up_value).astype(jnp.bfloat16)

    return kernel_call(
        body,
        jax.ShapeDtypeStruct((count, rows, units), jnp.bfloat16),
        [VMEM] * (1 + 2 * count),
        VMEM,
        4 * rows * gates[0].shape[0] * units * count,
    )(messages, *gates, *ups)


def project_down(hidden, downs, *earlier):
    count, rows, units = hidden.shape
    wide = 2 * LANES
    blocks = downs[0].shape[1] // wide

    def body(hidden_ref, *refs):
        out_ref = refs[-1]
        for b in range(blocks):
            span = slice(b * wide, (b + 1) * wide)
            total = None
            for g in range(count):
                part = jnp.dot(
                    hidden_ref[g], refs[g][:, span], preferred_element_type=jnp.float32
                )
                total = part if total is None else total + part
            total = total.astype(jnp.bfloat16)
            for side in range(2):
                out_ref[2 * b + side] = total[:, side * LANES : (side + 1) * LANES]

    return kernel_call(
        body,
        jax.ShapeDtypeStruct((2 * blocks, rows, LANES), jnp.bfloat16),
        [VMEM] * (1 + count) + [ANY] * len(earlier),
        VMEM,
        2 * rows * units * count * wide * blocks,
    )(hidden, *downs, *earlier)


def combine(returned, places, route_weight):
    total, width = returned.shape
    rows, top = route_weight.shape

    def body(rows_ref, place_ref, weight_ref, out_ref):
        slots = lax.broadcasted_iota(jnp.int32, (rows, total), 1)
        result = None
        for k in range(top):
            select = jnp.where(slots == place_ref[:, k : k + 1], 1.0, 0.0).astype(jnp.bfloat16)
            picked = jnp.dot(select, rows_ref[...], preferred_element_type=jnp.float32)
            part = picked * weight_ref[:, k : k + 1]
            result = part if result is None else result + part
        out_ref[...] = result.astype(jnp.bfloat16)

    return kernel_call(
        body,
        jax.ShapeDtypeStruct((rows, width), jnp.bfloat16),
        [VMEM, VMEM, VMEM],
        VMEM,
        2 * rows * total * width * top,
    )(returned, places, route_weight)


def make_local(z_count, x_count, tp_count):
    cores = 2
    ep_count = z_count * x_count
    z_groups = [[x_count * z + x for z in range(z_count)] for x in range(x_count)]
    x_shifts = [
        [
            (x_count * z + x, x_count * z + (x + i) % x_count)
            for z in range(z_count)
            for x in range(x_count)
        ]
        for i in range(x_count)
    ]
    partner = [(i, i ^ 1) for i in range(tp_count)]
    neighbour = [(i, i ^ cores) for i in range(tp_count)]

    def local(
        queries,
        compressed_key_value,
        rope_key,
        latent_norm_gain,
        latent_to_key_value,
        out_proj,
        moe_input,
        moe_gain,
        routes,
        route_weight,
        gate_weight,
        up_weight,
        down_weight,
    ):
        row_count = queries.shape[0]
        capacity = 3 * row_count // ep_count
        tp_index = lax.axis_index("tp").astype(jnp.int32)
        ep_index = lax.axis_index("ep").astype(jnp.int32)
        place_index = (tp_index % PARTS).reshape(1)

        groups_of = [[gate_weight[0]], [up_weight[0]], [down_weight[0]]]
        for group in groups_of:
            group.append(lax.ppermute(group[0], "tp", neighbour))

        outgoing, places = pack_rows(
            place_index, moe_input, moe_gain.reshape(1, -1), routes, capacity, ep_count
        )
        arrived = lax.all_to_all(outgoing, "ep", 0, 0, tiled=True)

        for group in groups_of:
            for weight in group[:2]:
                group.append(lax.ppermute(weight, "tp", partner))
        gates, ups, downs = groups_of

        positions = (ep_index * row_count + jnp.arange(row_count, dtype=jnp.int32)).astype(
            jnp.float32
        )
        half = ROPE // 2
        frequency = ROPE_BASE_VALUE ** (-jnp.arange(half, dtype=jnp.float32) * 2.0 / ROPE)
        angles = positions[:, None] * frequency
        cosine, sine = jnp.cos(angles), jnp.sin(angles)

        def rotated(values):
            first, second = values[:, :half], values[:, half:]
            return jnp.concatenate(
                [first * cosine - second * sine, second * cosine + first * sine], axis=1
            ).astype(jnp.bfloat16)

        query = jnp.concatenate(
            [
                queries[:, :PLAIN_HEAD_DIM],
                rotated(queries[:, PLAIN_HEAD_DIM:].astype(jnp.float32)),
                jnp.zeros((row_count, LANES - PLAIN_HEAD_DIM - ROPE), jnp.bfloat16),
            ],
            axis=1,
        )
        latent_normed = rms_scale(compressed_key_value, latent_norm_gain).astype(jnp.bfloat16)
        own_keys = lax.dot_general(
            latent_to_key_value,
            latent_normed,
            (((0,), (1,)), ((), ())),
            preferred_element_type=jnp.float32,
        ).astype(jnp.bfloat16)
        own_rope = rotated(rope_key.astype(jnp.float32)).T
        own_pack = jnp.concatenate(
            [own_keys[:PLAIN_HEAD_DIM], own_rope, own_keys[PLAIN_HEAD_DIM:]], axis=0
        )
        query_all = [query]
        for i in range(1, x_count):
            query_all.append(lax.ppermute(query, "ep", x_shifts[x_count - i]))
        key_value = to_everyone(sequenced(own_pack, arrived, *query_all), "ep", z_groups, z_count)
        hidden = hidden_units(arrived, gates, ups)

        partial_out = project_down(hidden, downs, key_value)
        groups = lax.all_to_all(partial_out, "tp", 0, 0, tiled=True)

        partial_all = attend(
            query_all, key_value, (PLAIN_HEAD_DIM + ROPE) ** (-0.5), partial_out
        )
        partials = [partial_all[0]] + [
            lax.ppermute(partial_all[i], "ep", x_shifts[i]) for i in range(1, x_count)
        ]
        attended = merge(partials)
        summed = add_up(groups, ep_count, attended)
        everyone = lax.all_gather(sequenced(attended, summed), "tp", axis=0, tiled=True)
        attention_out = lax.dot_general(
            everyone, out_proj, (((0,), (0,)), ((), ())), preferred_element_type=jnp.float32
        ).astype(jnp.bfloat16)

        returned = lax.all_to_all(summed, "ep", 0, 0, tiled=True)
        expert_out = combine(
            returned.reshape(ep_count * capacity, LANES), places, route_weight
        )
        return (attention_out, expert_out)

    return local


def solution(mesh):
    ep_count = mesh.shape["ep"]
    x_count = 4
    local = make_local(ep_count // x_count, x_count, mesh.shape["tp"])

    return jax.shard_map(
        local,
        mesh=mesh,
        in_specs=(
            P("ep", "tp"),
            P("ep", None),
            P("ep", None),
            P(),
            P(None, "tp"),
            P(None, "tp"),
            P("ep", None),
            P(),
            P("ep", None),
            P("ep", None),
            P("ep", None, "tp"),
            P("ep", None, "tp"),
            P("ep", "tp", None),
        ),
        out_specs=(P("ep", "tp"), P("ep", "tp")),
        check_vma=False,
    )
```

```python
import math

import jax
import jax.numpy as jnp
from jax import lax
from jax.experimental import pallas as pl
from jax.experimental.pallas import tpu as pltpu
from jax.sharding import PartitionSpec as P


PLAIN_HEAD_DIM = 64
ROPE = 32
VALUE_HEAD_DIM = 64
LANES = 128

EPSILON = 1e-06
ROPE_BASE_VALUE = 10000.0


VMEM = pl.BlockSpec(memory_space=pltpu.VMEM)
SMEM = pl.BlockSpec(memory_space=pltpu.SMEM)
ANY = pl.BlockSpec(memory_space=pl.ANY)
HBM = pl.BlockSpec(memory_space=pltpu.HBM)


def kernel_call(body, out_shape, in_specs, out_specs, flops, limit=16):
    return pl.pallas_call(
        body,
        out_shape=out_shape,
        in_specs=in_specs,
        out_specs=out_specs,
        compiler_params=pltpu.CompilerParams(vmem_limit_bytes=limit * 1024 * 1024),
        cost_estimate=pl.CostEstimate(flops=flops, transcendentals=0, bytes_accessed=0),
    )


def rms_scale(values, gain_vector):
    floats = values.astype(jnp.float32)
    return (
        floats
        * lax.rsqrt(jnp.mean(floats * floats, axis=-1, keepdims=True) + EPSILON)
        * gain_vector
    )


def to_everyone(array, axis, groups, count):
    return lax.all_to_all(
        jnp.broadcast_to(array[None], (count, *array.shape)),
        axis,
        0,
        0,
        tiled=True,
        axis_index_groups=groups,
    )


def sequenced(array, *earlier):
    def body(array_ref, *refs):
        refs[-1][...] = array_ref[...]

    return kernel_call(
        body,
        jax.ShapeDtypeStruct(array.shape, array.dtype),
        [VMEM] + [ANY] * len(earlier),
        VMEM,
        array.size,
    )(array, *earlier)


SHARE = 6
PARTS = 4


def message_rows(shape, dim):
    place = lax.broadcasted_iota(jnp.int32, shape, dim)
    source = jnp.floor((place.astype(jnp.float32) + 0.5) * (1.0 / SHARE)).astype(jnp.int32)
    return place + source * (SHARE * (PARTS - 1))


def pack_rows(index, moe_input, gain, routes, capacity, expert_total):
    rows, width = moe_input.shape
    places = expert_total * capacity
    top = routes.shape[1]
    wide = PARTS * LANES

    def body(index_ref, input_ref, gain_ref, routes_ref, out_ref, place_ref):
        floats = input_ref[...].astype(jnp.float32)
        scale = lax.rsqrt(jnp.mean(floats * floats, axis=-1, keepdims=True) + EPSILON)
        normed = (floats * scale * gain_ref[...]).astype(jnp.bfloat16)
        chosen = routes_ref[...]
        expert = lax.broadcasted_iota(jnp.int32, (rows, expert_total), 1)
        named = [chosen[:, k : k + 1] == expert for k in range(top)]
        either = named[0]
        for other in named[1:]:
            either = either | other
        ones = jnp.where(either, 1.0, 0.0).astype(jnp.bfloat16)
        lower = lax.broadcasted_iota(jnp.int32, (rows, rows), 0) > lax.broadcasted_iota(
            jnp.int32, (rows, rows), 1
        )
        lower = jnp.where(lower, 1.0, 0.0).astype(jnp.bfloat16)
        earlier = jnp.dot(lower, ones, preferred_element_type=jnp.float32)
        first_row = expert.astype(jnp.float32) * float(capacity)
        share = float(SHARE)

        def within(part):
            slot = earlier - part.astype(jnp.float32) * share
            return slot, (slot >= 0.0) & (slot < share)

        def pick(k, value, valid):
            chosen_value = jnp.where(named[k] & valid, value + 1.0, 0.0)
            return jnp.sum(chosen_value, axis=1, keepdims=True).astype(jnp.int32) - 1

        slot, valid = within(index_ref[0])
        starts = [pick(k, slot + first_row, valid) for k in range(top)]
        slots = lax.broadcasted_iota(jnp.int32, (rows, places), 1)
        selects = []
        for part in range(PARTS):
            hit = None
            for start in starts:
                target = jnp.where(start < 0, -1, start + part * SHARE)
                here = slots == target
                hit = here if hit is None else hit | here
            selects.append(jnp.where(hit, 1.0, 0.0).astype(jnp.bfloat16))
        for b in range(width // wide):
            total = None
            for part, select in enumerate(selects):
                first = b * wide + part * LANES
                piece = lax.dot_general(
                    select,
                    normed[:, first : first + LANES],
                    (((0,), (0,)), ((), ())),
                    preferred_element_type=jnp.float32,
                )
                total = piece if total is None else total + piece
            out_ref[:, b] = total.reshape(expert_total, capacity, LANES).astype(jnp.bfloat16)

        anywhere = earlier >= 0.0
        for k in range(top):
            place_ref[:, k : k + 1] = pick(k, earlier + first_row, anywhere)

    return kernel_call(
        body,
        (
            jax.ShapeDtypeStruct((expert_total, width // wide, capacity, LANES), jnp.bfloat16),
            jax.ShapeDtypeStruct((rows, top), jnp.int32),
        ),
        [SMEM, VMEM, VMEM, VMEM],
        (VMEM, VMEM),
        2 * rows * places * width,
    )(index, moe_input, gain, routes)


def add_up(parts, blocks, *earlier):
    count, rows, _ = parts.shape
    capacity = SHARE * PARTS

    def body(in_ref, *refs):
        out_ref = refs[-1]
        targets = message_rows((blocks * capacity, rows), 1)
        lines = lax.broadcasted_iota(jnp.int32, (blocks * capacity, rows), 0)
        total = None
        for part in range(PARTS):
            added = in_ref[part].astype(jnp.float32)
            for i in range(part + PARTS, count, PARTS):
                added += in_ref[i].astype(jnp.float32)
            select = jnp.where(lines == targets + part * SHARE, 1.0, 0.0).astype(jnp.bfloat16)
            piece = jnp.dot(
                select, added.astype(jnp.bfloat16), preferred_element_type=jnp.float32
            )
            total = piece if total is None else total + piece
        out_ref[...] = total.reshape(blocks, capacity, LANES).astype(jnp.bfloat16)

    return kernel_call(
        body,
        jax.ShapeDtypeStruct((blocks, capacity, LANES), jnp.bfloat16),
        [VMEM] + [ANY] * len(earlier),
        VMEM,
        1,
    )(parts, *earlier)


def attend(queries, key_value, score_scale, *earlier):
    blocks = len(queries)
    rows = queries[0].shape[0]
    pieces, _, length = key_value.shape
    factor = score_scale * math.log2(math.e)
    first_value = PLAIN_HEAD_DIM + ROPE

    def body(key_ref, *refs):
        for query_ref, out_ref in zip(refs[:blocks], refs[-blocks:]):
            q = query_ref[...]
            scores = [
                jnp.dot(q, key_ref[j, :LANES, :], preferred_element_type=jnp.float32)
                for j in range(pieces)
            ]
            top = scores[0]
            for s in scores[1:]:
                top = jnp.maximum(top, s)
            top = jnp.max(top, axis=1, keepdims=True) * factor
            total = None
            mixed = None
            for j in range(pieces):
                weight = jnp.exp2(scores[j] * factor - top)
                total = weight if total is None else total + weight
                part = lax.dot_general(
                    weight.astype(jnp.bfloat16),
                    key_ref[j, first_value:, :],
                    (((1,), (1,)), ((), ())),
                    preferred_element_type=jnp.float32,
                )
                mixed = part if mixed is None else mixed + part
            total = jnp.sum(total, axis=1, keepdims=True)
            out_ref[:, :VALUE_HEAD_DIM] = (mixed / total).astype(jnp.bfloat16)
            log_total = top + jnp.log2(total)
            high = log_total.astype(jnp.bfloat16).astype(jnp.float32)
            middle = (log_total - high).astype(jnp.bfloat16).astype(jnp.float32)
            low = log_total - high - middle
            lane = lax.broadcasted_iota(jnp.int32, (rows, LANES - VALUE_HEAD_DIM), 1)
            out_ref[:, VALUE_HEAD_DIM:] = jnp.where(
                lane == 0, high, jnp.where(lane == 1, middle, low)
            ).astype(jnp.bfloat16)

    return kernel_call(
        body,
        tuple(jax.ShapeDtypeStruct((rows, LANES), jnp.bfloat16) for _ in range(blocks)),
        [VMEM] * (1 + blocks) + [ANY] * len(earlier),
        (VMEM,) * blocks,
        4 * blocks * rows * pieces * length * 2 * LANES,
    )(key_value, *queries, *earlier)


def merge(partials):
    rows = partials[0].shape[0]

    def body(*refs):
        out_ref = refs[-1]
        values = [r[...].astype(jnp.float32) for r in refs[:-1]]
        first = VALUE_HEAD_DIM
        logs = [
            v[:, first : first + 1] + v[:, first + 1 : first + 2] + v[:, first + 2 : first + 3]
            for v in values
        ]
        top = logs[0]
        for log in logs[1:]:
            top = jnp.maximum(top, log)
        shares = [jnp.exp2(log - top) for log in logs]
        mixed = values[0] * shares[0]
        total = shares[0]
        for value, share in zip(values[1:], shares[1:]):
            mixed += value * share
            total += share
        out_ref[...] = (mixed / total).T[:VALUE_HEAD_DIM].astype(jnp.bfloat16)

    return kernel_call(
        body,
        jax.ShapeDtypeStruct((VALUE_HEAD_DIM, rows), jnp.bfloat16),
        [VMEM] * len(partials),
        VMEM,
        1,
    )(*partials)


def experts(messages, gate_ups, downs, *earlier):
    sources, blocks, capacity, _ = messages.shape
    rows = sources * SHARE
    _, width, units = gate_ups[0].shape
    count = len(gate_ups)
    wide = 2 * LANES

    def body(rows_ref, *refs):
        gate_up_in, down_in = refs[:count], refs[count : 2 * count]
        out_ref, gate_up_ref, down_ref, sems = refs[-4:]
        gate_up_copies = [
            pltpu.make_async_copy(gate_up_in[g], gate_up_ref.at[g], sems.at[g])
            for g in range(count)
        ]
        down_copies = [
            pltpu.make_async_copy(down_in[g], down_ref.at[g], sems.at[count + g])
            for g in range(count)
        ]
        for copy in gate_up_copies + down_copies:
            copy.start()
        targets = message_rows((rows, sources * capacity), 0)
        lines = lax.broadcasted_iota(jnp.int32, (rows, sources * capacity), 1)
        selects = [
            jnp.where(lines == targets + part * SHARE, 1.0, 0.0).astype(jnp.bfloat16)
            for part in range(PARTS)
        ]
        parts = []
        for b in range(blocks):
            block = rows_ref[:, b].astype(jnp.float32).reshape(sources * capacity, LANES)
            block = block.astype(jnp.bfloat16)
            columns = [
                jnp.dot(select, block, preferred_element_type=jnp.float32).astype(jnp.bfloat16)
                for select in selects
            ]
            for part in range(0, PARTS, 2):
                parts.append(jnp.concatenate(columns[part : part + 2], axis=1))
        hidden = []
        for g in range(count):
            gate_up_copies[g].wait()
            gate_value = jnp.zeros((rows, units), jnp.float32)
            up_value = jnp.zeros((rows, units), jnp.float32)
            for b, part in enumerate(parts):
                span = slice(b * wide, (b + 1) * wide)
                gate_value += jnp.dot(
                    part, gate_up_ref[g, 0, span, :], preferred_element_type=jnp.float32
                )
                up_value += jnp.dot(
                    part, gate_up_ref[g, 1, span, :], preferred_element_type=jnp.float32
                )
            silu = gate_value / (1.0 + jnp.exp(-gate_value))
            hidden.append((silu * up_value).astype(jnp.bfloat16))
        for copy in down_copies:
            copy.wait()
        for b in range(width // wide):
            span = slice(b * wide, (b + 1) * wide)
            total = None
            for g in range(count):
                part = jnp.dot(
                    hidden[g], down_ref[g, :, span], preferred_element_type=jnp.float32
                )
                total = part if total is None else total + part
            total = total.astype(jnp.bfloat16)
            for side in range(2):
                out_ref[2 * b + side] = total[:, side * LANES : (side + 1) * LANES]

    return pl.pallas_call(
        body,
        out_shape=jax.ShapeDtypeStruct((width // LANES, rows, LANES), jnp.bfloat16),
        in_specs=[VMEM] + [HBM] * (2 * count) + [ANY] * len(earlier),
        out_specs=VMEM,
        scratch_shapes=[
            pltpu.VMEM((count, 2, width, units), jnp.bfloat16),
            pltpu.VMEM((count, units, width), jnp.bfloat16),
            pltpu.SemaphoreType.DMA((2 * count,)),
        ],
        compiler_params=pltpu.CompilerParams(vmem_limit_bytes=36 * 1024 * 1024),
        cost_estimate=pl.CostEstimate(
            flops=6 * rows * width * units * count, transcendentals=0, bytes_accessed=0
        ),
    )(messages, *gate_ups, *downs, *earlier)


def combine(returned, places, route_weight):
    total, width = returned.shape
    rows, top = route_weight.shape

    def body(rows_ref, place_ref, weight_ref, out_ref):
        slots = lax.broadcasted_iota(jnp.int32, (rows, total), 1)
        result = None
        for k in range(top):
            select = jnp.where(slots == place_ref[:, k : k + 1], 1.0, 0.0).astype(jnp.bfloat16)
            picked = jnp.dot(select, rows_ref[...], preferred_element_type=jnp.float32)
            part = picked * weight_ref[:, k : k + 1]
            result = part if result is None else result + part
        out_ref[...] = result.astype(jnp.bfloat16)

    return kernel_call(
        body,
        jax.ShapeDtypeStruct((rows, width), jnp.bfloat16),
        [VMEM, VMEM, VMEM],
        VMEM,
        2 * rows * total * width * top,
    )(returned, places, route_weight)


def make_local(z_count, x_count, tp_count):
    cores = 2
    ep_count = z_count * x_count
    z_groups = [[x_count * z + x for z in range(z_count)] for x in range(x_count)]
    x_shifts = [
        [
            (x_count * z + x, x_count * z + (x + i) % x_count)
            for z in range(z_count)
            for x in range(x_count)
        ]
        for i in range(x_count)
    ]
    partner = [(i, i ^ 1) for i in range(tp_count)]
    y_count = tp_count // cores
    neighbour = [
        (cores * y + c, cores * ((y + (1 if (y + c) % 2 == 0 else -1)) % y_count) + c)
        for y in range(y_count)
        for c in range(cores)
    ]

    def local(
        queries,
        compressed_key_value,
        rope_key,
        latent_norm_gain,
        latent_to_key_value,
        out_proj,
        moe_input,
        moe_gain,
        routes,
        route_weight,
        gate_weight,
        up_weight,
        down_weight,
    ):
        row_count = queries.shape[0]
        capacity = 3 * row_count // ep_count
        tp_index = lax.axis_index("tp").astype(jnp.int32)
        ep_index = lax.axis_index("ep").astype(jnp.int32)
        place_index = (tp_index % PARTS).reshape(1)

        groups_of = [[jnp.stack([gate_weight[0], up_weight[0]])], [down_weight[0]]]
        for group in groups_of:
            group.append(lax.ppermute(group[0], "tp", neighbour))

        outgoing, places = pack_rows(
            place_index, moe_input, moe_gain.reshape(1, -1), routes, capacity, ep_count
        )
        arrived = lax.all_to_all(outgoing, "ep", 0, 0, tiled=True)

        for group in groups_of:
            for weight in group[:2]:
                group.append(lax.ppermute(weight, "tp", partner))
        gate_ups, downs = groups_of

        positions = (ep_index * row_count + jnp.arange(row_count, dtype=jnp.int32)).astype(
            jnp.float32
        )
        half = ROPE // 2
        frequency = ROPE_BASE_VALUE ** (-jnp.arange(half, dtype=jnp.float32) * 2.0 / ROPE)
        angles = positions[:, None] * frequency
        cosine, sine = jnp.cos(angles), jnp.sin(angles)

        def rotated(values):
            first, second = values[:, :half], values[:, half:]
            return jnp.concatenate(
                [first * cosine - second * sine, second * cosine + first * sine], axis=1
            ).astype(jnp.bfloat16)

        query = jnp.concatenate(
            [
                queries[:, :PLAIN_HEAD_DIM],
                rotated(queries[:, PLAIN_HEAD_DIM:].astype(jnp.float32)),
                jnp.zeros((row_count, LANES - PLAIN_HEAD_DIM - ROPE), jnp.bfloat16),
            ],
            axis=1,
        )
        latent_normed = rms_scale(compressed_key_value, latent_norm_gain).astype(jnp.bfloat16)
        own_keys = lax.dot_general(
            latent_to_key_value,
            latent_normed,
            (((0,), (1,)), ((), ())),
            preferred_element_type=jnp.float32,
        ).astype(jnp.bfloat16)
        own_rope = rotated(rope_key.astype(jnp.float32)).T
        own_pack = jnp.concatenate(
            [own_keys[:PLAIN_HEAD_DIM], own_rope, own_keys[PLAIN_HEAD_DIM:]], axis=0
        )
        query_all = [query]
        for i in range(1, x_count):
            query_all.append(lax.ppermute(query, "ep", x_shifts[x_count - i]))
        key_value = to_everyone(sequenced(own_pack, arrived, *query_all), "ep", z_groups, z_count)

        partial_out = experts(arrived, gate_ups, downs)
        groups = lax.all_to_all(partial_out, "tp", 0, 0, tiled=True)

        partial_all = attend(
            query_all, key_value, (PLAIN_HEAD_DIM + ROPE) ** (-0.5), partial_out
        )
        partials = [partial_all[0]] + [
            lax.ppermute(partial_all[i], "ep", x_shifts[i]) for i in range(1, x_count)
        ]
        attended = merge(partials)
        summed = add_up(groups, ep_count, attended)
        everyone = lax.all_gather(sequenced(attended, summed), "tp", axis=0, tiled=True)
        attention_out = lax.dot_general(
            everyone, out_proj, (((0,), (0,)), ((), ())), preferred_element_type=jnp.float32
        ).astype(jnp.bfloat16)

        returned = lax.all_to_all(summed, "ep", 0, 0, tiled=True)
        expert_out = combine(
            returned.reshape(ep_count * capacity, LANES), places, route_weight
        )
        return (attention_out, expert_out)

    return local


def solution(mesh):
    ep_count = mesh.shape["ep"]
    x_count = 4
    local = make_local(ep_count // x_count, x_count, mesh.shape["tp"])

    return jax.shard_map(
        local,
        mesh=mesh,
        in_specs=(
            P("ep", "tp"),
            P("ep", None),
            P("ep", None),
            P(),
            P(None, "tp"),
            P(None, "tp"),
            P("ep", None),
            P(),
            P("ep", None),
            P("ep", None),
            P("ep", None, "tp"),
            P("ep", None, "tp"),
            P("ep", "tp", None),
        ),
        out_specs=(P("ep", "tp"), P("ep", "tp")),
        check_vma=False,
    )
```

```python
import math

import jax
import jax.numpy as jnp
import numpy as np
from jax import lax
from jax.experimental import pallas as pl
from jax.experimental.pallas import tpu as pltpu
from jax.sharding import PartitionSpec as P


PLAIN_HEAD_DIM = 64
ROPE = 32
VALUE_HEAD_DIM = 64
LANES = 128

EPSILON = 1e-06
ROPE_BASE_VALUE = 10000.0


VMEM = pl.BlockSpec(memory_space=pltpu.VMEM)
SMEM = pl.BlockSpec(memory_space=pltpu.SMEM)
ANY = pl.BlockSpec(memory_space=pl.ANY)
HBM = pl.BlockSpec(memory_space=pltpu.HBM)


def kernel_call(body, out_shape, in_specs, out_specs, flops, limit=16):
    return pl.pallas_call(
        body,
        out_shape=out_shape,
        in_specs=in_specs,
        out_specs=out_specs,
        compiler_params=pltpu.CompilerParams(vmem_limit_bytes=limit * 1024 * 1024),
        cost_estimate=pl.CostEstimate(flops=flops, transcendentals=0, bytes_accessed=0),
    )


def angle_tables(blocks, rows):
    half = ROPE // 2
    frequency = ROPE_BASE_VALUE ** (-np.arange(half) * 2.0 / ROPE)
    tables = []
    for positions in (np.arange(blocks) * rows, np.arange(rows)):
        angles = np.zeros((len(positions), LANES))
        angles[:, PLAIN_HEAD_DIM : PLAIN_HEAD_DIM + ROPE] = np.tile(
            positions[:, None] * frequency, (1, 2)
        )
        tables += [np.cos(angles).astype(np.float32), np.sin(angles).astype(np.float32)]
    return tables


def prepare(index, queries, latents, rope_key, gain, weight, tables, copies):
    rows = queries.shape[0]
    first, last = PLAIN_HEAD_DIM, PLAIN_HEAD_DIM + ROPE
    half = ROPE // 2

    def body(index_ref, query_ref, latent_ref, rope_ref, gain_ref, weight_ref, *refs):
        block_cos, block_sin, place_cos, place_sin = refs[:4]
        query_out, key_out, padded_ref = refs[4:]
        base_cos = block_cos[pl.ds(index_ref[0], 1), :]
        base_sin = block_sin[pl.ds(index_ref[0], 1), :]
        cosine = base_cos * place_cos[...] - base_sin * place_sin[...]
        sine = base_sin * place_cos[...] + base_cos * place_sin[...]
        lane = lax.broadcasted_iota(jnp.int32, (rows, LANES), 1)
        early = lane < first + half
        sine = jnp.where(early, -sine, sine)

        def rotated(values):
            other = jnp.where(
                early, pltpu.roll(values, LANES - half, 1), pltpu.roll(values, half, 1)
            )
            return values * cosine + other * sine

        padded_ref[...] = jnp.zeros((rows, LANES), jnp.float32)
        padded_ref[:, :last] = query_ref[...].astype(jnp.float32)
        query_out[...] = rotated(padded_ref[...]).astype(jnp.bfloat16)
        padded_ref[:, first:last] = rope_ref[...].astype(jnp.float32)
        turned = rotated(padded_ref[...]).T[first:last].astype(jnp.bfloat16)
        floats = latent_ref[...].astype(jnp.float32)
        scale = lax.rsqrt(jnp.mean(floats * floats, axis=-1, keepdims=True) + EPSILON)
        normed = (floats * scale * gain_ref[...]).astype(jnp.bfloat16)
        expanded = jnp.dot(normed, weight_ref[...], preferred_element_type=jnp.float32).T
        expanded = expanded.astype(jnp.bfloat16)
        for i in range(copies):
            key_out[i, :first, :] = expanded[:first]
            key_out[i, first:last, :] = turned
            key_out[i, last:, :] = expanded[first:]

    return pl.pallas_call(
        body,
        out_shape=(
            jax.ShapeDtypeStruct((rows, LANES), jnp.bfloat16),
            jax.ShapeDtypeStruct((copies, LANES + ROPE, rows), jnp.bfloat16),
        ),
        in_specs=[SMEM] + [VMEM] * 9,
        out_specs=(VMEM, VMEM),
        scratch_shapes=[pltpu.VMEM((rows, LANES), jnp.float32)],
        compiler_params=pltpu.CompilerParams(vmem_limit_bytes=16 * 1024 * 1024),
        cost_estimate=pl.CostEstimate(
            flops=2 * latents.size * weight.shape[1], transcendentals=0, bytes_accessed=0
        ),
    )(index, queries, latents, rope_key, gain, weight, *tables)


def sequenced(array, *earlier):
    def body(array_ref, *refs):
        refs[-1][...] = array_ref[...]

    return kernel_call(
        body,
        jax.ShapeDtypeStruct(array.shape, array.dtype),
        [VMEM] + [ANY] * len(earlier),
        VMEM,
        array.size,
    )(array, *earlier)


SHARE = 6
PARTS = 4


def message_rows(shape, dim):
    place = lax.broadcasted_iota(jnp.int32, shape, dim)
    source = jnp.floor((place.astype(jnp.float32) + 0.5) * (1.0 / SHARE)).astype(jnp.int32)
    return place + source * (SHARE * (PARTS - 1))


def pack_rows(index, moe_input, gain, routes, capacity, expert_total):
    rows, width = moe_input.shape
    places = expert_total * capacity
    top = routes.shape[1]
    wide = PARTS * LANES

    def body(index_ref, input_ref, gain_ref, routes_ref, out_ref, place_ref):
        floats = input_ref[...].astype(jnp.float32)
        scale = lax.rsqrt(jnp.mean(floats * floats, axis=-1, keepdims=True) + EPSILON)
        normed = (floats * scale * gain_ref[...]).astype(jnp.bfloat16)
        chosen = routes_ref[...]
        expert = lax.broadcasted_iota(jnp.int32, (rows, expert_total), 1)
        named = [chosen[:, k : k + 1] == expert for k in range(top)]
        either = named[0]
        for other in named[1:]:
            either = either | other
        ones = jnp.where(either, 1.0, 0.0).astype(jnp.bfloat16)
        lower = lax.broadcasted_iota(jnp.int32, (rows, rows), 0) > lax.broadcasted_iota(
            jnp.int32, (rows, rows), 1
        )
        lower = jnp.where(lower, 1.0, 0.0).astype(jnp.bfloat16)
        earlier = jnp.dot(lower, ones, preferred_element_type=jnp.float32)
        first_row = expert.astype(jnp.float32) * float(capacity)
        share = float(SHARE)

        def within(part):
            slot = earlier - part.astype(jnp.float32) * share
            return slot, (slot >= 0.0) & (slot < share)

        def pick(k, value, valid):
            chosen_value = jnp.where(named[k] & valid, value + 1.0, 0.0)
            return jnp.sum(chosen_value, axis=1, keepdims=True).astype(jnp.int32) - 1

        slot, valid = within(index_ref[0])
        starts = [pick(k, slot + first_row, valid) for k in range(top)]
        slots = lax.broadcasted_iota(jnp.int32, (rows, places), 1)
        selects = []
        for part in range(PARTS):
            hit = None
            for start in starts:
                target = jnp.where(start < 0, -1, start + part * SHARE)
                here = slots == target
                hit = here if hit is None else hit | here
            selects.append(jnp.where(hit, 1.0, 0.0).astype(jnp.bfloat16))
        for b in range(width // wide):
            total = None
            for part, select in enumerate(selects):
                first = b * wide + part * LANES
                piece = lax.dot_general(
                    select,
                    normed[:, first : first + LANES],
                    (((0,), (0,)), ((), ())),
                    preferred_element_type=jnp.float32,
                )
                total = piece if total is None else total + piece
            out_ref[:, b] = total.reshape(expert_total, capacity, LANES).astype(jnp.bfloat16)

        anywhere = earlier >= 0.0
        for k in range(top):
            place_ref[:, k : k + 1] = pick(k, earlier + first_row, anywhere)

    return kernel_call(
        body,
        (
            jax.ShapeDtypeStruct((expert_total, width // wide, capacity, LANES), jnp.bfloat16),
            jax.ShapeDtypeStruct((rows, top), jnp.int32),
        ),
        [SMEM, VMEM, VMEM, VMEM],
        (VMEM, VMEM),
        2 * rows * places * width,
    )(index, moe_input, gain, routes)


def add_up(parts, blocks, *earlier):
    count, rows, _ = parts.shape
    capacity = SHARE * PARTS

    def body(in_ref, *refs):
        out_ref = refs[-1]
        targets = message_rows((blocks * capacity, rows), 1)
        lines = lax.broadcasted_iota(jnp.int32, (blocks * capacity, rows), 0)
        total = None
        for part in range(PARTS):
            added = in_ref[part].astype(jnp.float32)
            for i in range(part + PARTS, count, PARTS):
                added += in_ref[i].astype(jnp.float32)
            select = jnp.where(lines == targets + part * SHARE, 1.0, 0.0).astype(jnp.bfloat16)
            piece = jnp.dot(
                select, added.astype(jnp.bfloat16), preferred_element_type=jnp.float32
            )
            total = piece if total is None else total + piece
        out_ref[...] = total.reshape(blocks, capacity, LANES).astype(jnp.bfloat16)

    return kernel_call(
        body,
        jax.ShapeDtypeStruct((blocks, capacity, LANES), jnp.bfloat16),
        [VMEM] + [ANY] * len(earlier),
        VMEM,
        1,
    )(parts, *earlier)


def attend(queries, key_value, score_scale, *earlier):
    blocks = len(queries)
    rows = queries[0].shape[0]
    pieces, _, length = key_value.shape
    factor = score_scale * math.log2(math.e)
    first_value = PLAIN_HEAD_DIM + ROPE

    def body(key_ref, *refs):
        for query_ref, out_ref in zip(refs[:blocks], refs[-blocks:]):
            q = query_ref[...]
            scores = [
                jnp.dot(q, key_ref[j, :LANES, :], preferred_element_type=jnp.float32)
                for j in range(pieces)
            ]
            top = scores[0]
            for s in scores[1:]:
                top = jnp.maximum(top, s)
            top = jnp.max(top, axis=1, keepdims=True) * factor
            total = None
            mixed = None
            for j in range(pieces):
                weight = jnp.exp2(scores[j] * factor - top)
                total = weight if total is None else total + weight
                part = lax.dot_general(
                    weight.astype(jnp.bfloat16),
                    key_ref[j, first_value:, :],
                    (((1,), (1,)), ((), ())),
                    preferred_element_type=jnp.float32,
                )
                mixed = part if mixed is None else mixed + part
            total = jnp.sum(total, axis=1, keepdims=True)
            out_ref[:, :VALUE_HEAD_DIM] = (mixed / total).astype(jnp.bfloat16)
            log_total = top + jnp.log2(total)
            high = log_total.astype(jnp.bfloat16).astype(jnp.float32)
            middle = (log_total - high).astype(jnp.bfloat16).astype(jnp.float32)
            low = log_total - high - middle
            lane = lax.broadcasted_iota(jnp.int32, (rows, LANES - VALUE_HEAD_DIM), 1)
            out_ref[:, VALUE_HEAD_DIM:] = jnp.where(
                lane == 0, high, jnp.where(lane == 1, middle, low)
            ).astype(jnp.bfloat16)

    return kernel_call(
        body,
        tuple(jax.ShapeDtypeStruct((rows, LANES), jnp.bfloat16) for _ in range(blocks)),
        [VMEM] * (1 + blocks) + [ANY] * len(earlier),
        (VMEM,) * blocks,
        4 * blocks * rows * pieces * length * 2 * LANES,
    )(key_value, *queries, *earlier)


def merge(partials):
    rows = partials[0].shape[0]

    def body(*refs):
        out_ref = refs[-1]
        values = [r[...].astype(jnp.float32) for r in refs[:-1]]
        first = VALUE_HEAD_DIM
        logs = [
            v[:, first : first + 1] + v[:, first + 1 : first + 2] + v[:, first + 2 : first + 3]
            for v in values
        ]
        top = logs[0]
        for log in logs[1:]:
            top = jnp.maximum(top, log)
        shares = [jnp.exp2(log - top) for log in logs]
        mixed = values[0] * shares[0]
        total = shares[0]
        for value, share in zip(values[1:], shares[1:]):
            mixed += value * share
            total += share
        out_ref[...] = (mixed / total).T[:VALUE_HEAD_DIM].astype(jnp.bfloat16)

    return kernel_call(
        body,
        jax.ShapeDtypeStruct((VALUE_HEAD_DIM, rows), jnp.bfloat16),
        [VMEM] * len(partials),
        VMEM,
        1,
    )(*partials)


def experts(messages, gate_ups, downs, *earlier):
    sources, blocks, capacity, _ = messages.shape
    rows = sources * SHARE
    _, width, units = gate_ups[0].shape
    count = len(gate_ups)
    wide = 2 * LANES

    def body(rows_ref, *refs):
        gate_up_in, down_in = refs[:count], refs[count : 2 * count]
        out_ref, gate_up_ref, down_ref, sems = refs[-4:]
        gate_up_copies = [
            pltpu.make_async_copy(gate_up_in[g], gate_up_ref.at[g], sems.at[g])
            for g in range(count)
        ]
        down_copies = [
            pltpu.make_async_copy(down_in[g], down_ref.at[g], sems.at[count + g])
            for g in range(count)
        ]
        for copy in gate_up_copies + down_copies:
            copy.start()
        targets = message_rows((rows, sources * capacity), 0)
        lines = lax.broadcasted_iota(jnp.int32, (rows, sources * capacity), 1)
        selects = [
            jnp.where(lines == targets + part * SHARE, 1.0, 0.0).astype(jnp.bfloat16)
            for part in range(PARTS)
        ]
        parts = []
        for b in range(blocks):
            block = rows_ref[:, b].astype(jnp.float32).reshape(sources * capacity, LANES)
            block = block.astype(jnp.bfloat16)
            columns = [
                jnp.dot(select, block, preferred_element_type=jnp.float32).astype(jnp.bfloat16)
                for select in selects
            ]
            for part in range(0, PARTS, 2):
                parts.append(jnp.concatenate(columns[part : part + 2], axis=1))
        hidden = []
        for g in range(count):
            gate_up_copies[g].wait()
            gate_value = jnp.zeros((rows, units), jnp.float32)
            up_value = jnp.zeros((rows, units), jnp.float32)
            for b, part in enumerate(parts):
                span = slice(b * wide, (b + 1) * wide)
                gate_value += jnp.dot(
                    part, gate_up_ref[g, 0, span, :], preferred_element_type=jnp.float32
                )
                up_value += jnp.dot(
                    part, gate_up_ref[g, 1, span, :], preferred_element_type=jnp.float32
                )
            silu = gate_value / (1.0 + jnp.exp(-gate_value))
            hidden.append((silu * up_value).astype(jnp.bfloat16))
        for copy in down_copies:
            copy.wait()
        for b in range(width // wide):
            span = slice(b * wide, (b + 1) * wide)
            total = None
            for g in range(count):
                part = jnp.dot(
                    hidden[g], down_ref[g, :, span], preferred_element_type=jnp.float32
                )
                total = part if total is None else total + part
            total = total.astype(jnp.bfloat16)
            for side in range(2):
                out_ref[2 * b + side] = total[:, side * LANES : (side + 1) * LANES]

    return pl.pallas_call(
        body,
        out_shape=jax.ShapeDtypeStruct((width // LANES, rows, LANES), jnp.bfloat16),
        in_specs=[VMEM] + [HBM] * (2 * count) + [ANY] * len(earlier),
        out_specs=VMEM,
        scratch_shapes=[
            pltpu.VMEM((count, 2, width, units), jnp.bfloat16),
            pltpu.VMEM((count, units, width), jnp.bfloat16),
            pltpu.SemaphoreType.DMA((2 * count,)),
        ],
        compiler_params=pltpu.CompilerParams(vmem_limit_bytes=36 * 1024 * 1024),
        cost_estimate=pl.CostEstimate(
            flops=6 * rows * width * units * count, transcendentals=0, bytes_accessed=0
        ),
    )(messages, *gate_ups, *downs, *earlier)


def combine(returned, places, route_weight):
    total, width = returned.shape
    rows, top = route_weight.shape

    def body(rows_ref, place_ref, weight_ref, out_ref):
        slots = lax.broadcasted_iota(jnp.int32, (rows, total), 1)
        result = None
        for k in range(top):
            select = jnp.where(slots == place_ref[:, k : k + 1], 1.0, 0.0).astype(jnp.bfloat16)
            picked = jnp.dot(select, rows_ref[...], preferred_element_type=jnp.float32)
            part = picked * weight_ref[:, k : k + 1]
            result = part if result is None else result + part
        out_ref[...] = result.astype(jnp.bfloat16)

    return kernel_call(
        body,
        jax.ShapeDtypeStruct((rows, width), jnp.bfloat16),
        [VMEM, VMEM, VMEM],
        VMEM,
        2 * rows * total * width * top,
    )(returned, places, route_weight)


def make_local(z_count, x_count, tp_count):
    cores = 2
    ep_count = z_count * x_count
    z_groups = [[x_count * z + x for z in range(z_count)] for x in range(x_count)]
    x_shifts = [
        [
            (x_count * z + x, x_count * z + (x + i) % x_count)
            for z in range(z_count)
            for x in range(x_count)
        ]
        for i in range(x_count)
    ]
    partner = [(i, i ^ 1) for i in range(tp_count)]
    y_count = tp_count // cores
    neighbour = [
        (cores * y + c, cores * ((y + (1 if (y + c) % 2 == 0 else -1)) % y_count) + c)
        for y in range(y_count)
        for c in range(cores)
    ]

    def local(
        queries,
        compressed_key_value,
        rope_key,
        latent_norm_gain,
        latent_to_key_value,
        out_proj,
        moe_input,
        moe_gain,
        routes,
        route_weight,
        gate_weight,
        up_weight,
        down_weight,
    ):
        row_count = queries.shape[0]
        capacity = 3 * row_count // ep_count
        tp_index = lax.axis_index("tp").astype(jnp.int32)
        ep_index = lax.axis_index("ep").astype(jnp.int32)
        place_index = (tp_index % PARTS).reshape(1)

        groups_of = [[jnp.stack([gate_weight[0], up_weight[0]])], [down_weight[0]]]
        for group in groups_of:
            group.append(lax.ppermute(group[0], "tp", neighbour))

        outgoing, places = pack_rows(
            place_index, moe_input, moe_gain.reshape(1, -1), routes, capacity, ep_count
        )
        arrived = lax.all_to_all(outgoing, "ep", 0, 0, tiled=True)

        for group in groups_of:
            for weight in group[:2]:
                group.append(lax.ppermute(weight, "tp", partner))
        gate_ups, downs = groups_of

        query, own_keys = prepare(
            ep_index.reshape(1),
            queries,
            compressed_key_value,
            rope_key,
            latent_norm_gain.reshape(1, -1),
            latent_to_key_value,
            angle_tables(ep_count, row_count),
            z_count,
        )
        query_all = [query]
        for i in range(1, x_count):
            query_all.append(lax.ppermute(query, "ep", x_shifts[x_count - i]))
        key_value = lax.all_to_all(
            own_keys, "ep", 0, 0, tiled=True, axis_index_groups=z_groups
        )

        partial_out = experts(arrived, gate_ups, downs)
        groups = lax.all_to_all(partial_out, "tp", 0, 0, tiled=True)

        partial_all = attend(query_all, key_value, (PLAIN_HEAD_DIM + ROPE) ** (-0.5))
        partials = [partial_all[0]] + [
            lax.ppermute(partial_all[i], "ep", x_shifts[i]) for i in range(1, x_count)
        ]
        attended = merge(partials)
        summed = add_up(groups, ep_count, attended)
        everyone = lax.all_gather(sequenced(attended, summed), "tp", axis=0, tiled=True)
        attention_out = lax.dot_general(
            everyone, out_proj, (((0,), (0,)), ((), ())), preferred_element_type=jnp.float32
        ).astype(jnp.bfloat16)

        returned = lax.all_to_all(summed, "ep", 0, 0, tiled=True)
        expert_out = combine(
            returned.reshape(ep_count * capacity, LANES), places, route_weight
        )
        return (attention_out, expert_out)

    return local


def solution(mesh):
    ep_count = mesh.shape["ep"]
    x_count = 4
    local = make_local(ep_count // x_count, x_count, mesh.shape["tp"])

    return jax.shard_map(
        local,
        mesh=mesh,
        in_specs=(
            P("ep", "tp"),
            P("ep", None),
            P("ep", None),
            P(),
            P(None, "tp"),
            P(None, "tp"),
            P("ep", None),
            P(),
            P("ep", None),
            P("ep", None),
            P("ep", None, "tp"),
            P("ep", None, "tp"),
            P("ep", "tp", None),
        ),
        out_specs=(P("ep", "tp"), P("ep", "tp")),
        check_vma=False,
    )
```

```python
import math

import jax
import jax.numpy as jnp
import numpy as np
from jax import lax
from jax.experimental import pallas as pl
from jax.experimental.pallas import tpu as pltpu
from jax.sharding import PartitionSpec as P


PLAIN_HEAD_DIM = 64
ROPE = 32
VALUE_HEAD_DIM = 64
LANES = 128

EPSILON = 1e-06
ROPE_BASE_VALUE = 10000.0


VMEM = pl.BlockSpec(memory_space=pltpu.VMEM)
SMEM = pl.BlockSpec(memory_space=pltpu.SMEM)
ANY = pl.BlockSpec(memory_space=pl.ANY)
HBM = pl.BlockSpec(memory_space=pltpu.HBM)


def kernel_call(body, out_shape, in_specs, out_specs, flops, limit=16):
    return pl.pallas_call(
        body,
        out_shape=out_shape,
        in_specs=in_specs,
        out_specs=out_specs,
        compiler_params=pltpu.CompilerParams(vmem_limit_bytes=limit * 1024 * 1024),
        cost_estimate=pl.CostEstimate(flops=flops, transcendentals=0, bytes_accessed=0),
    )


def angle_tables(blocks, rows):
    half = ROPE // 2
    frequency = ROPE_BASE_VALUE ** (-np.arange(half) * 2.0 / ROPE)
    tables = []
    for positions in (np.arange(blocks) * rows, np.arange(rows)):
        angles = np.zeros((len(positions), LANES))
        angles[:, PLAIN_HEAD_DIM : PLAIN_HEAD_DIM + ROPE] = np.tile(
            positions[:, None] * frequency, (1, 2)
        )
        tables += [np.cos(angles).astype(np.float32), np.sin(angles).astype(np.float32)]
    return np.concatenate(tables)


def prepare(index, queries, latents, rope_key, gain, weight, tables, copies):
    rows = queries.shape[0]
    blocks = tables.shape[0] // 2 - rows
    first, last = PLAIN_HEAD_DIM, PLAIN_HEAD_DIM + ROPE
    half = ROPE // 2

    def body(index_ref, query_ref, latent_ref, rope_ref, gain_ref, weight_ref, *refs):
        table_ref, query_out, key_out, padded_ref = refs
        base_cos = table_ref[pl.ds(index_ref[0], 1), :]
        base_sin = table_ref[pl.ds(index_ref[0] + blocks, 1), :]
        place_cos = table_ref[2 * blocks : 2 * blocks + rows, :]
        place_sin = table_ref[2 * blocks + rows :, :]
        cosine = base_cos * place_cos - base_sin * place_sin
        sine = base_sin * place_cos + base_cos * place_sin
        lane = lax.broadcasted_iota(jnp.int32, (rows, LANES), 1)
        early = lane < first + half
        sine = jnp.where(early, -sine, sine)

        def rotated(values):
            other = jnp.where(
                early, pltpu.roll(values, LANES - half, 1), pltpu.roll(values, half, 1)
            )
            return values * cosine + other * sine

        padded_ref[...] = jnp.zeros((rows, LANES), jnp.float32)
        padded_ref[:, :last] = query_ref[...].astype(jnp.float32)
        query_out[...] = rotated(padded_ref[...]).astype(jnp.bfloat16)
        padded_ref[:, first:last] = rope_ref[...].astype(jnp.float32)
        turned = rotated(padded_ref[...]).T[first:last].astype(jnp.bfloat16)
        floats = latent_ref[...].astype(jnp.float32)
        scale = lax.rsqrt(jnp.mean(floats * floats, axis=-1, keepdims=True) + EPSILON)
        normed = (floats * scale * gain_ref[...]).astype(jnp.bfloat16)
        expanded = jnp.dot(normed, weight_ref[...], preferred_element_type=jnp.float32).T
        expanded = expanded.astype(jnp.bfloat16)
        for i in range(copies):
            key_out[i, :first, :] = expanded[:first]
            key_out[i, first:last, :] = turned
            key_out[i, last:, :] = expanded[first:]

    return pl.pallas_call(
        body,
        out_shape=(
            jax.ShapeDtypeStruct((rows, LANES), jnp.bfloat16),
            jax.ShapeDtypeStruct((copies, LANES + ROPE, rows), jnp.bfloat16),
        ),
        in_specs=[SMEM] + [VMEM] * 6,
        out_specs=(VMEM, VMEM),
        scratch_shapes=[pltpu.VMEM((rows, LANES), jnp.float32)],
        compiler_params=pltpu.CompilerParams(vmem_limit_bytes=60 * 1024 * 1024),
        cost_estimate=pl.CostEstimate(
            flops=2 * latents.size * weight.shape[1], transcendentals=0, bytes_accessed=0
        ),
    )(index, queries, latents, rope_key, gain, weight, tables)


def sequenced(array, *earlier):
    def body(array_ref, *refs):
        refs[-1][...] = array_ref[...]

    return kernel_call(
        body,
        jax.ShapeDtypeStruct(array.shape, array.dtype),
        [VMEM] + [ANY] * len(earlier),
        VMEM,
        array.size,
    )(array, *earlier)


SHARE = 6
PARTS = 4


def message_rows(shape, dim):
    place = lax.broadcasted_iota(jnp.int32, shape, dim)
    source = jnp.floor((place.astype(jnp.float32) + 0.5) * (1.0 / SHARE)).astype(jnp.int32)
    return place + source * (SHARE * (PARTS - 1))


def pack_rows(index, moe_input, gain, routes, capacity, expert_total):
    rows, width = moe_input.shape
    places = expert_total * capacity
    top = routes.shape[1]
    wide = PARTS * LANES

    def body(index_ref, input_ref, gain_ref, routes_ref, out_ref, place_ref):
        floats = input_ref[...].astype(jnp.float32)
        scale = lax.rsqrt(jnp.mean(floats * floats, axis=-1, keepdims=True) + EPSILON)
        normed = (floats * scale * gain_ref[...]).astype(jnp.bfloat16)
        chosen = routes_ref[...]
        expert = lax.broadcasted_iota(jnp.int32, (rows, expert_total), 1)
        named = [chosen[:, k : k + 1] == expert for k in range(top)]
        either = named[0]
        for other in named[1:]:
            either = either | other
        ones = jnp.where(either, 1.0, 0.0).astype(jnp.bfloat16)
        lower = lax.broadcasted_iota(jnp.int32, (rows, rows), 0) > lax.broadcasted_iota(
            jnp.int32, (rows, rows), 1
        )
        lower = jnp.where(lower, 1.0, 0.0).astype(jnp.bfloat16)
        earlier = jnp.dot(lower, ones, preferred_element_type=jnp.float32)
        first_row = expert.astype(jnp.float32) * float(capacity)
        share = float(SHARE)

        def within(part):
            slot = earlier - part.astype(jnp.float32) * share
            return slot, (slot >= 0.0) & (slot < share)

        def pick(k, value, valid):
            chosen_value = jnp.where(named[k] & valid, value + 1.0, 0.0)
            return jnp.sum(chosen_value, axis=1, keepdims=True).astype(jnp.int32) - 1

        slot, valid = within(index_ref[0])
        starts = [pick(k, slot + first_row, valid) for k in range(top)]
        slots = lax.broadcasted_iota(jnp.int32, (rows, places), 1)
        selects = []
        for part in range(PARTS):
            hit = None
            for start in starts:
                target = jnp.where(start < 0, -1, start + part * SHARE)
                here = slots == target
                hit = here if hit is None else hit | here
            selects.append(jnp.where(hit, 1.0, 0.0).astype(jnp.bfloat16))
        for b in range(width // wide):
            total = None
            for part, select in enumerate(selects):
                first = b * wide + part * LANES
                piece = lax.dot_general(
                    select,
                    normed[:, first : first + LANES],
                    (((0,), (0,)), ((), ())),
                    preferred_element_type=jnp.float32,
                )
                total = piece if total is None else total + piece
            out_ref[:, b] = total.reshape(expert_total, capacity, LANES).astype(jnp.bfloat16)

        anywhere = earlier >= 0.0
        for k in range(top):
            place_ref[:, k : k + 1] = pick(k, earlier + first_row, anywhere)

    return kernel_call(
        body,
        (
            jax.ShapeDtypeStruct((expert_total, width // wide, capacity, LANES), jnp.bfloat16),
            jax.ShapeDtypeStruct((rows, top), jnp.int32),
        ),
        [SMEM, VMEM, VMEM, VMEM],
        (VMEM, VMEM),
        2 * rows * places * width,
    )(index, moe_input, gain, routes)


def add_up(parts, blocks, *earlier):
    count, rows, _ = parts.shape
    capacity = SHARE * PARTS

    def body(in_ref, *refs):
        out_ref = refs[-1]
        targets = message_rows((blocks * capacity, rows), 1)
        lines = lax.broadcasted_iota(jnp.int32, (blocks * capacity, rows), 0)
        total = None
        for part in range(PARTS):
            added = in_ref[part].astype(jnp.float32)
            for i in range(part + PARTS, count, PARTS):
                added += in_ref[i].astype(jnp.float32)
            select = jnp.where(lines == targets + part * SHARE, 1.0, 0.0).astype(jnp.bfloat16)
            piece = jnp.dot(
                select, added.astype(jnp.bfloat16), preferred_element_type=jnp.float32
            )
            total = piece if total is None else total + piece
        out_ref[...] = total.reshape(blocks, capacity, LANES).astype(jnp.bfloat16)

    return kernel_call(
        body,
        jax.ShapeDtypeStruct((blocks, capacity, LANES), jnp.bfloat16),
        [VMEM] + [ANY] * len(earlier),
        VMEM,
        1,
    )(parts, *earlier)


def attend(queries, key_value, score_scale, *earlier):
    blocks = len(queries)
    rows = queries[0].shape[0]
    pieces, _, length = key_value.shape
    factor = score_scale * math.log2(math.e)
    first_value = PLAIN_HEAD_DIM + ROPE

    def body(key_ref, *refs):
        for query_ref, out_ref in zip(refs[:blocks], refs[-blocks:]):
            q = query_ref[...]
            scores = [
                jnp.dot(q, key_ref[j, :LANES, :], preferred_element_type=jnp.float32)
                for j in range(pieces)
            ]
            top = scores[0]
            for s in scores[1:]:
                top = jnp.maximum(top, s)
            top = jnp.max(top, axis=1, keepdims=True) * factor
            total = None
            mixed = None
            for j in range(pieces):
                weight = jnp.exp2(scores[j] * factor - top)
                total = weight if total is None else total + weight
                part = lax.dot_general(
                    weight.astype(jnp.bfloat16),
                    key_ref[j, first_value:, :],
                    (((1,), (1,)), ((), ())),
                    preferred_element_type=jnp.float32,
                )
                mixed = part if mixed is None else mixed + part
            total = jnp.sum(total, axis=1, keepdims=True)
            out_ref[:, :VALUE_HEAD_DIM] = (mixed / total).astype(jnp.bfloat16)
            log_total = top + jnp.log2(total)
            high = log_total.astype(jnp.bfloat16).astype(jnp.float32)
            middle = (log_total - high).astype(jnp.bfloat16).astype(jnp.float32)
            low = log_total - high - middle
            lane = lax.broadcasted_iota(jnp.int32, (rows, LANES - VALUE_HEAD_DIM), 1)
            out_ref[:, VALUE_HEAD_DIM:] = jnp.where(
                lane == 0, high, jnp.where(lane == 1, middle, low)
            ).astype(jnp.bfloat16)

    return kernel_call(
        body,
        tuple(jax.ShapeDtypeStruct((rows, LANES), jnp.bfloat16) for _ in range(blocks)),
        [VMEM] * (1 + blocks) + [ANY] * len(earlier),
        (VMEM,) * blocks,
        4 * blocks * rows * pieces * length * 2 * LANES,
    )(key_value, *queries, *earlier)


def merge(partials):
    rows = partials[0].shape[0]

    def body(*refs):
        out_ref = refs[-1]
        values = [r[...].astype(jnp.float32) for r in refs[:-1]]
        first = VALUE_HEAD_DIM
        logs = [
            v[:, first : first + 1] + v[:, first + 1 : first + 2] + v[:, first + 2 : first + 3]
            for v in values
        ]
        top = logs[0]
        for log in logs[1:]:
            top = jnp.maximum(top, log)
        shares = [jnp.exp2(log - top) for log in logs]
        mixed = values[0] * shares[0]
        total = shares[0]
        for value, share in zip(values[1:], shares[1:]):
            mixed += value * share
            total += share
        out_ref[...] = (mixed / total).T[:VALUE_HEAD_DIM].astype(jnp.bfloat16)

    return kernel_call(
        body,
        jax.ShapeDtypeStruct((VALUE_HEAD_DIM, rows), jnp.bfloat16),
        [VMEM] * len(partials),
        VMEM,
        1,
    )(*partials)


def experts(messages, gate_ups, downs, *earlier):
    sources, blocks, capacity, _ = messages.shape
    rows = sources * SHARE
    _, width, units = gate_ups[0].shape
    count = len(gate_ups)
    wide = 2 * LANES

    def body(rows_ref, *refs):
        gate_up_in, down_in = refs[:count], refs[count : 2 * count]
        out_ref, gate_up_ref, down_ref, sems = refs[-4:]
        gate_up_copies = [
            pltpu.make_async_copy(gate_up_in[g], gate_up_ref.at[g], sems.at[g])
            for g in range(count)
        ]
        down_copies = [
            pltpu.make_async_copy(down_in[g], down_ref.at[g], sems.at[count + g])
            for g in range(count)
        ]
        for copy in gate_up_copies + down_copies:
            copy.start()
        targets = message_rows((rows, sources * capacity), 0)
        lines = lax.broadcasted_iota(jnp.int32, (rows, sources * capacity), 1)
        selects = [
            jnp.where(lines == targets + part * SHARE, 1.0, 0.0).astype(jnp.bfloat16)
            for part in range(PARTS)
        ]
        parts = []
        for b in range(blocks):
            block = rows_ref[:, b].astype(jnp.float32).reshape(sources * capacity, LANES)
            block = block.astype(jnp.bfloat16)
            columns = [
                jnp.dot(select, block, preferred_element_type=jnp.float32).astype(jnp.bfloat16)
                for select in selects
            ]
            for part in range(0, PARTS, 2):
                parts.append(jnp.concatenate(columns[part : part + 2], axis=1))
        hidden = []
        for g in range(count):
            gate_up_copies[g].wait()
            gate_value = jnp.zeros((rows, units), jnp.float32)
            up_value = jnp.zeros((rows, units), jnp.float32)
            for b, part in enumerate(parts):
                span = slice(b * wide, (b + 1) * wide)
                gate_value += jnp.dot(
                    part, gate_up_ref[g, 0, span, :], preferred_element_type=jnp.float32
                )
                up_value += jnp.dot(
                    part, gate_up_ref[g, 1, span, :], preferred_element_type=jnp.float32
                )
            silu = gate_value / (1.0 + jnp.exp(-gate_value))
            hidden.append((silu * up_value).astype(jnp.bfloat16))
        for copy in down_copies:
            copy.wait()
        for b in range(width // wide):
            span = slice(b * wide, (b + 1) * wide)
            total = None
            for g in range(count):
                part = jnp.dot(
                    hidden[g], down_ref[g, :, span], preferred_element_type=jnp.float32
                )
                total = part if total is None else total + part
            total = total.astype(jnp.bfloat16)
            for side in range(2):
                out_ref[2 * b + side] = total[:, side * LANES : (side + 1) * LANES]

    return pl.pallas_call(
        body,
        out_shape=jax.ShapeDtypeStruct((width // LANES, rows, LANES), jnp.bfloat16),
        in_specs=[VMEM] + [HBM] * (2 * count) + [ANY] * len(earlier),
        out_specs=VMEM,
        scratch_shapes=[
            pltpu.VMEM((count, 2, width, units), jnp.bfloat16),
            pltpu.VMEM((count, units, width), jnp.bfloat16),
            pltpu.SemaphoreType.DMA((2 * count,)),
        ],
        compiler_params=pltpu.CompilerParams(vmem_limit_bytes=36 * 1024 * 1024),
        cost_estimate=pl.CostEstimate(
            flops=6 * rows * width * units * count, transcendentals=0, bytes_accessed=0
        ),
    )(messages, *gate_ups, *downs, *earlier)


def combine(returned, places, route_weight):
    total, width = returned.shape
    rows, top = route_weight.shape

    def body(rows_ref, place_ref, weight_ref, out_ref):
        slots = lax.broadcasted_iota(jnp.int32, (rows, total), 1)
        result = None
        for k in range(top):
            select = jnp.where(slots == place_ref[:, k : k + 1], 1.0, 0.0).astype(jnp.bfloat16)
            picked = jnp.dot(select, rows_ref[...], preferred_element_type=jnp.float32)
            part = picked * weight_ref[:, k : k + 1]
            result = part if result is None else result + part
        out_ref[...] = result.astype(jnp.bfloat16)

    return kernel_call(
        body,
        jax.ShapeDtypeStruct((rows, width), jnp.bfloat16),
        [VMEM, VMEM, VMEM],
        VMEM,
        2 * rows * total * width * top,
    )(returned, places, route_weight)


def make_local(z_count, x_count, tp_count):
    cores = 2
    ep_count = z_count * x_count
    z_groups = [[x_count * z + x for z in range(z_count)] for x in range(x_count)]
    x_shifts = [
        [
            (x_count * z + x, x_count * z + (x + i) % x_count)
            for z in range(z_count)
            for x in range(x_count)
        ]
        for i in range(x_count)
    ]
    partner = [(i, i ^ 1) for i in range(tp_count)]
    y_count = tp_count // cores
    neighbour = [
        (cores * y + c, cores * ((y + (1 if (y + c) % 2 == 0 else -1)) % y_count) + c)
        for y in range(y_count)
        for c in range(cores)
    ]

    def local(
        queries,
        compressed_key_value,
        rope_key,
        latent_norm_gain,
        latent_to_key_value,
        out_proj,
        moe_input,
        moe_gain,
        routes,
        route_weight,
        gate_weight,
        up_weight,
        down_weight,
    ):
        row_count = queries.shape[0]
        capacity = 3 * row_count // ep_count
        tp_index = lax.axis_index("tp").astype(jnp.int32)
        ep_index = lax.axis_index("ep").astype(jnp.int32)
        place_index = (tp_index % PARTS).reshape(1)

        groups_of = [[jnp.stack([gate_weight[0], up_weight[0]])], [down_weight[0]]]
        for group in groups_of:
            group.append(lax.ppermute(group[0], "tp", neighbour))

        outgoing, places = pack_rows(
            place_index, moe_input, moe_gain.reshape(1, -1), routes, capacity, ep_count
        )
        arrived = lax.all_to_all(outgoing, "ep", 0, 0, tiled=True)

        for group in groups_of:
            for weight in group[:2]:
                group.append(lax.ppermute(weight, "tp", partner))
        gate_ups, downs = groups_of

        query, own_keys = prepare(
            ep_index.reshape(1),
            queries,
            compressed_key_value,
            rope_key,
            latent_norm_gain.reshape(1, -1),
            latent_to_key_value,
            angle_tables(ep_count, row_count),
            z_count,
        )
        query_all = [query]
        for i in range(1, x_count):
            query_all.append(lax.ppermute(query, "ep", x_shifts[x_count - i]))
        key_value = lax.all_to_all(
            own_keys, "ep", 0, 0, tiled=True, axis_index_groups=z_groups
        )

        partial_out = experts(arrived, gate_ups, downs)
        groups = lax.all_to_all(partial_out, "tp", 0, 0, tiled=True)

        partial_all = attend(query_all, key_value, (PLAIN_HEAD_DIM + ROPE) ** (-0.5))
        partials = [partial_all[0]] + [
            lax.ppermute(partial_all[i], "ep", x_shifts[i]) for i in range(1, x_count)
        ]
        attended = merge(partials)
        summed = add_up(groups, ep_count, attended)
        everyone = lax.all_gather(sequenced(attended, summed), "tp", axis=0, tiled=True)
        attention_out = lax.dot_general(
            everyone, out_proj, (((0,), (0,)), ((), ())), preferred_element_type=jnp.float32
        ).astype(jnp.bfloat16)

        returned = lax.all_to_all(summed, "ep", 0, 0, tiled=True)
        expert_out = combine(
            returned.reshape(ep_count * capacity, LANES), places, route_weight
        )
        return (attention_out, expert_out)

    return local


def solution(mesh):
    ep_count = mesh.shape["ep"]
    x_count = 4
    local = make_local(ep_count // x_count, x_count, mesh.shape["tp"])

    return jax.shard_map(
        local,
        mesh=mesh,
        in_specs=(
            P("ep", "tp"),
            P("ep", None),
            P("ep", None),
            P(),
            P(None, "tp"),
            P(None, "tp"),
            P("ep", None),
            P(),
            P("ep", None),
            P("ep", None),
            P("ep", None, "tp"),
            P("ep", None, "tp"),
            P("ep", "tp", None),
        ),
        out_specs=(P("ep", "tp"), P("ep", "tp")),
        check_vma=False,
    )
```

```python
import math

import jax
import jax.numpy as jnp
import numpy as np
from jax import lax
from jax.experimental import pallas as pl
from jax.experimental.pallas import tpu as pltpu
from jax.sharding import PartitionSpec as P


PLAIN_HEAD_DIM = 64
ROPE = 32
VALUE_HEAD_DIM = 64
LANES = 128

EPSILON = 1e-06
ROPE_BASE_VALUE = 10000.0


VMEM = pl.BlockSpec(memory_space=pltpu.VMEM)
SMEM = pl.BlockSpec(memory_space=pltpu.SMEM)
ANY = pl.BlockSpec(memory_space=pl.ANY)
HBM = pl.BlockSpec(memory_space=pltpu.HBM)


def kernel_call(body, out_shape, in_specs, out_specs, flops, limit=16):
    return pl.pallas_call(
        body,
        out_shape=out_shape,
        in_specs=in_specs,
        out_specs=out_specs,
        compiler_params=pltpu.CompilerParams(vmem_limit_bytes=limit * 1024 * 1024),
        cost_estimate=pl.CostEstimate(flops=flops, transcendentals=0, bytes_accessed=0),
    )


def angle_tables(blocks, rows):
    half = ROPE // 2
    frequency = ROPE_BASE_VALUE ** (-np.arange(half) * 2.0 / ROPE)
    tables = []
    for positions in (np.arange(blocks) * rows, np.arange(rows)):
        angles = np.zeros((len(positions), LANES))
        angles[:, PLAIN_HEAD_DIM : PLAIN_HEAD_DIM + ROPE] = np.tile(
            positions[:, None] * frequency, (1, 2)
        )
        tables += [np.cos(angles).astype(np.float32), np.sin(angles).astype(np.float32)]
    return np.concatenate(tables)


def prepare(index, queries, latents, rope_key, gain, weight, tables, copies):
    rows = queries.shape[0]
    blocks = tables.shape[0] // 2 - rows
    first, last = PLAIN_HEAD_DIM, PLAIN_HEAD_DIM + ROPE
    half = ROPE // 2

    def body(index_ref, query_ref, latent_ref, rope_ref, gain_ref, weight_ref, *refs):
        table_ref, query_out, key_out, padded_ref = refs
        base_cos = table_ref[pl.ds(index_ref[0], 1), :]
        base_sin = table_ref[pl.ds(index_ref[0] + blocks, 1), :]
        place_cos = table_ref[2 * blocks : 2 * blocks + rows, :]
        place_sin = table_ref[2 * blocks + rows :, :]
        cosine = base_cos * place_cos - base_sin * place_sin
        sine = base_sin * place_cos + base_cos * place_sin
        lane = lax.broadcasted_iota(jnp.int32, (rows, LANES), 1)
        early = lane < first + half
        sine = jnp.where(early, -sine, sine)

        def rotated(values):
            other = jnp.where(
                early, pltpu.roll(values, LANES - half, 1), pltpu.roll(values, half, 1)
            )
            return values * cosine + other * sine

        padded_ref[...] = jnp.zeros((rows, LANES), jnp.float32)
        padded_ref[:, :last] = query_ref[...].astype(jnp.float32)
        query_out[...] = rotated(padded_ref[...]).astype(jnp.bfloat16)
        padded_ref[:, first:last] = rope_ref[...].astype(jnp.float32)
        turned = rotated(padded_ref[...]).T[first:last].astype(jnp.bfloat16)
        floats = latent_ref[...].astype(jnp.float32)
        scale = lax.rsqrt(jnp.mean(floats * floats, axis=-1, keepdims=True) + EPSILON)
        normed = (floats * scale * gain_ref[...]).astype(jnp.bfloat16)
        expanded = jnp.dot(normed, weight_ref[...], preferred_element_type=jnp.float32).T
        expanded = expanded.astype(jnp.bfloat16)
        for i in range(copies):
            key_out[i, :first, :] = expanded[:first]
            key_out[i, first:last, :] = turned
            key_out[i, last:, :] = expanded[first:]

    return pl.pallas_call(
        body,
        out_shape=(
            jax.ShapeDtypeStruct((rows, LANES), jnp.bfloat16),
            jax.ShapeDtypeStruct((copies, LANES + ROPE, rows), jnp.bfloat16),
        ),
        in_specs=[SMEM] + [VMEM] * 6,
        out_specs=(VMEM, VMEM),
        scratch_shapes=[pltpu.VMEM((rows, LANES), jnp.float32)],
        compiler_params=pltpu.CompilerParams(vmem_limit_bytes=60 * 1024 * 1024),
        cost_estimate=pl.CostEstimate(
            flops=2 * latents.size * weight.shape[1], transcendentals=0, bytes_accessed=0
        ),
    )(index, queries, latents, rope_key, gain, weight, tables)


def sequenced(array, *earlier):
    def body(array_ref, *refs):
        refs[-1][...] = array_ref[...]

    return kernel_call(
        body,
        jax.ShapeDtypeStruct(array.shape, array.dtype),
        [VMEM] + [ANY] * len(earlier),
        VMEM,
        array.size,
    )(array, *earlier)


SHARE = 6
PARTS = 4


def message_rows(shape, dim):
    place = lax.broadcasted_iota(jnp.int32, shape, dim)
    source = jnp.floor((place.astype(jnp.float32) + 0.5) * (1.0 / SHARE)).astype(jnp.int32)
    return place + source * (SHARE * (PARTS - 1))


def pack_rows(index, moe_input, gain, routes, capacity, expert_total, *earlier):
    rows, width = moe_input.shape
    places = expert_total * capacity
    top = routes.shape[1]
    wide = PARTS * LANES

    def body(index_ref, input_ref, gain_ref, routes_ref, *refs):
        out_ref, place_ref = refs[-2:]
        floats = input_ref[...].astype(jnp.float32)
        scale = lax.rsqrt(jnp.mean(floats * floats, axis=-1, keepdims=True) + EPSILON)
        normed = (floats * scale * gain_ref[...]).astype(jnp.bfloat16)
        chosen = routes_ref[...]
        expert = lax.broadcasted_iota(jnp.int32, (rows, expert_total), 1)
        named = [chosen[:, k : k + 1] == expert for k in range(top)]
        either = named[0]
        for other in named[1:]:
            either = either | other
        ones = jnp.where(either, 1.0, 0.0).astype(jnp.bfloat16)
        lower = lax.broadcasted_iota(jnp.int32, (rows, rows), 0) > lax.broadcasted_iota(
            jnp.int32, (rows, rows), 1
        )
        lower = jnp.where(lower, 1.0, 0.0).astype(jnp.bfloat16)
        earlier = jnp.dot(lower, ones, preferred_element_type=jnp.float32)
        first_row = expert.astype(jnp.float32) * float(capacity)
        share = float(SHARE)

        def within(part):
            slot = earlier - part.astype(jnp.float32) * share
            return slot, (slot >= 0.0) & (slot < share)

        def pick(k, value, valid):
            chosen_value = jnp.where(named[k] & valid, value + 1.0, 0.0)
            return jnp.sum(chosen_value, axis=1, keepdims=True).astype(jnp.int32) - 1

        slot, valid = within(index_ref[0])
        starts = [pick(k, slot + first_row, valid) for k in range(top)]
        slots = lax.broadcasted_iota(jnp.int32, (rows, places), 1)
        selects = []
        for part in range(PARTS):
            hit = None
            for start in starts:
                target = jnp.where(start < 0, -1, start + part * SHARE)
                here = slots == target
                hit = here if hit is None else hit | here
            selects.append(jnp.where(hit, 1.0, 0.0).astype(jnp.bfloat16))
        for b in range(width // wide):
            total = None
            for part, select in enumerate(selects):
                first = b * wide + part * LANES
                piece = lax.dot_general(
                    select,
                    normed[:, first : first + LANES],
                    (((0,), (0,)), ((), ())),
                    preferred_element_type=jnp.float32,
                )
                total = piece if total is None else total + piece
            out_ref[:, b] = total.reshape(expert_total, capacity, LANES).astype(jnp.bfloat16)

        anywhere = earlier >= 0.0
        for k in range(top):
            place_ref[:, k : k + 1] = pick(k, earlier + first_row, anywhere)

    return kernel_call(
        body,
        (
            jax.ShapeDtypeStruct((expert_total, width // wide, capacity, LANES), jnp.bfloat16),
            jax.ShapeDtypeStruct((rows, top), jnp.int32),
        ),
        [SMEM, VMEM, VMEM, VMEM] + [ANY] * len(earlier),
        (VMEM, VMEM),
        2 * rows * places * width,
        limit=60,
    )(index, moe_input, gain, routes, *earlier)


def add_up(parts, blocks, *earlier):
    count, rows, _ = parts.shape
    capacity = SHARE * PARTS

    def body(in_ref, *refs):
        out_ref = refs[-1]
        targets = message_rows((blocks * capacity, rows), 1)
        lines = lax.broadcasted_iota(jnp.int32, (blocks * capacity, rows), 0)
        total = None
        for part in range(PARTS):
            added = in_ref[part].astype(jnp.float32)
            for i in range(part + PARTS, count, PARTS):
                added += in_ref[i].astype(jnp.float32)
            select = jnp.where(lines == targets + part * SHARE, 1.0, 0.0).astype(jnp.bfloat16)
            piece = jnp.dot(
                select, added.astype(jnp.bfloat16), preferred_element_type=jnp.float32
            )
            total = piece if total is None else total + piece
        out_ref[...] = total.reshape(blocks, capacity, LANES).astype(jnp.bfloat16)

    return kernel_call(
        body,
        jax.ShapeDtypeStruct((blocks, capacity, LANES), jnp.bfloat16),
        [VMEM] + [ANY] * len(earlier),
        VMEM,
        1,
    )(parts, *earlier)


def attend(queries, key_value, score_scale, *earlier):
    blocks = len(queries)
    rows = queries[0].shape[0]
    pieces, _, length = key_value.shape
    factor = score_scale * math.log2(math.e)
    first_value = PLAIN_HEAD_DIM + ROPE

    def body(key_ref, *refs):
        for query_ref, out_ref in zip(refs[:blocks], refs[-blocks:]):
            q = query_ref[...]
            scores = [
                jnp.dot(q, key_ref[j, :LANES, :], preferred_element_type=jnp.float32)
                for j in range(pieces)
            ]
            top = scores[0]
            for s in scores[1:]:
                top = jnp.maximum(top, s)
            top = jnp.max(top, axis=1, keepdims=True) * factor
            total = None
            mixed = None
            for j in range(pieces):
                weight = jnp.exp2(scores[j] * factor - top)
                total = weight if total is None else total + weight
                part = lax.dot_general(
                    weight.astype(jnp.bfloat16),
                    key_ref[j, first_value:, :],
                    (((1,), (1,)), ((), ())),
                    preferred_element_type=jnp.float32,
                )
                mixed = part if mixed is None else mixed + part
            total = jnp.sum(total, axis=1, keepdims=True)
            out_ref[:, :VALUE_HEAD_DIM] = (mixed / total).astype(jnp.bfloat16)
            log_total = top + jnp.log2(total)
            high = log_total.astype(jnp.bfloat16).astype(jnp.float32)
            middle = (log_total - high).astype(jnp.bfloat16).astype(jnp.float32)
            low = log_total - high - middle
            lane = lax.broadcasted_iota(jnp.int32, (rows, LANES - VALUE_HEAD_DIM), 1)
            out_ref[:, VALUE_HEAD_DIM:] = jnp.where(
                lane == 0, high, jnp.where(lane == 1, middle, low)
            ).astype(jnp.bfloat16)

    return kernel_call(
        body,
        tuple(jax.ShapeDtypeStruct((rows, LANES), jnp.bfloat16) for _ in range(blocks)),
        [VMEM] * (1 + blocks) + [ANY] * len(earlier),
        (VMEM,) * blocks,
        4 * blocks * rows * pieces * length * 2 * LANES,
    )(key_value, *queries, *earlier)


def merge(partials):
    rows = partials[0].shape[0]

    def body(*refs):
        out_ref = refs[-1]
        values = [r[...].astype(jnp.float32) for r in refs[:-1]]
        first = VALUE_HEAD_DIM
        logs = [
            v[:, first : first + 1] + v[:, first + 1 : first + 2] + v[:, first + 2 : first + 3]
            for v in values
        ]
        top = logs[0]
        for log in logs[1:]:
            top = jnp.maximum(top, log)
        shares = [jnp.exp2(log - top) for log in logs]
        mixed = values[0] * shares[0]
        total = shares[0]
        for value, share in zip(values[1:], shares[1:]):
            mixed += value * share
            total += share
        out_ref[...] = (mixed / total).T[:VALUE_HEAD_DIM].astype(jnp.bfloat16)

    return kernel_call(
        body,
        jax.ShapeDtypeStruct((VALUE_HEAD_DIM, rows), jnp.bfloat16),
        [VMEM] * len(partials),
        VMEM,
        1,
    )(*partials)


def experts(messages, gate_ups, downs, *earlier):
    sources, blocks, capacity, _ = messages.shape
    rows = sources * SHARE
    _, width, units = gate_ups[0].shape
    count = len(gate_ups)
    wide = 2 * LANES

    def body(rows_ref, *refs):
        gate_up_in, down_in = refs[:count], refs[count : 2 * count]
        out_ref, gate_up_ref, down_ref, sems = refs[-4:]
        gate_up_copies = [
            pltpu.make_async_copy(gate_up_in[g], gate_up_ref.at[g], sems.at[g])
            for g in range(count)
        ]
        down_copies = [
            pltpu.make_async_copy(down_in[g], down_ref.at[g], sems.at[count + g])
            for g in range(count)
        ]
        for copy in gate_up_copies + down_copies:
            copy.start()
        targets = message_rows((rows, sources * capacity), 0)
        lines = lax.broadcasted_iota(jnp.int32, (rows, sources * capacity), 1)
        selects = [
            jnp.where(lines == targets + part * SHARE, 1.0, 0.0).astype(jnp.bfloat16)
            for part in range(PARTS)
        ]
        parts = []
        for b in range(blocks):
            block = rows_ref[:, b].astype(jnp.float32).reshape(sources * capacity, LANES)
            block = block.astype(jnp.bfloat16)
            columns = [
                jnp.dot(select, block, preferred_element_type=jnp.float32).astype(jnp.bfloat16)
                for select in selects
            ]
            for part in range(0, PARTS, 2):
                parts.append(jnp.concatenate(columns[part : part + 2], axis=1))
        hidden = []
        for g in range(count):
            gate_up_copies[g].wait()
            gate_value = jnp.zeros((rows, units), jnp.float32)
            up_value = jnp.zeros((rows, units), jnp.float32)
            for b, part in enumerate(parts):
                span = slice(b * wide, (b + 1) * wide)
                gate_value += jnp.dot(
                    part, gate_up_ref[g, 0, span, :], preferred_element_type=jnp.float32
                )
                up_value += jnp.dot(
                    part, gate_up_ref[g, 1, span, :], preferred_element_type=jnp.float32
                )
            silu = gate_value / (1.0 + jnp.exp(-gate_value))
            hidden.append((silu * up_value).astype(jnp.bfloat16))
        for copy in down_copies:
            copy.wait()
        for b in range(width // wide):
            span = slice(b * wide, (b + 1) * wide)
            total = None
            for g in range(count):
                part = jnp.dot(
                    hidden[g], down_ref[g, :, span], preferred_element_type=jnp.float32
                )
                total = part if total is None else total + part
            total = total.astype(jnp.bfloat16)
            for side in range(2):
                out_ref[2 * b + side] = total[:, side * LANES : (side + 1) * LANES]

    return pl.pallas_call(
        body,
        out_shape=jax.ShapeDtypeStruct((width // LANES, rows, LANES), jnp.bfloat16),
        in_specs=[VMEM] + [HBM] * (2 * count) + [ANY] * len(earlier),
        out_specs=VMEM,
        scratch_shapes=[
            pltpu.VMEM((count, 2, width, units), jnp.bfloat16),
            pltpu.VMEM((count, units, width), jnp.bfloat16),
            pltpu.SemaphoreType.DMA((2 * count,)),
        ],
        compiler_params=pltpu.CompilerParams(vmem_limit_bytes=36 * 1024 * 1024),
        cost_estimate=pl.CostEstimate(
            flops=6 * rows * width * units * count, transcendentals=0, bytes_accessed=0
        ),
    )(messages, *gate_ups, *downs, *earlier)


def combine(returned, places, route_weight):
    total, width = returned.shape
    rows, top = route_weight.shape

    def body(rows_ref, place_ref, weight_ref, out_ref):
        slots = lax.broadcasted_iota(jnp.int32, (rows, total), 1)
        result = None
        for k in range(top):
            select = jnp.where(slots == place_ref[:, k : k + 1], 1.0, 0.0).astype(jnp.bfloat16)
            picked = jnp.dot(select, rows_ref[...], preferred_element_type=jnp.float32)
            part = picked * weight_ref[:, k : k + 1]
            result = part if result is None else result + part
        out_ref[...] = result.astype(jnp.bfloat16)

    return kernel_call(
        body,
        jax.ShapeDtypeStruct((rows, width), jnp.bfloat16),
        [VMEM, VMEM, VMEM],
        VMEM,
        2 * rows * total * width * top,
    )(returned, places, route_weight)


def make_local(z_count, x_count, tp_count):
    cores = 2
    ep_count = z_count * x_count
    z_groups = [[x_count * z + x for z in range(z_count)] for x in range(x_count)]
    x_shifts = [
        [
            (x_count * z + x, x_count * z + (x + i) % x_count)
            for z in range(z_count)
            for x in range(x_count)
        ]
        for i in range(x_count)
    ]
    partner = [(i, i ^ 1) for i in range(tp_count)]
    y_count = tp_count // cores
    neighbour = [
        (cores * y + c, cores * ((y + (1 if (y + c) % 2 == 0 else -1)) % y_count) + c)
        for y in range(y_count)
        for c in range(cores)
    ]

    def local(
        queries,
        compressed_key_value,
        rope_key,
        latent_norm_gain,
        latent_to_key_value,
        out_proj,
        moe_input,
        moe_gain,
        routes,
        route_weight,
        gate_weight,
        up_weight,
        down_weight,
    ):
        row_count = queries.shape[0]
        capacity = 3 * row_count // ep_count
        tp_index = lax.axis_index("tp").astype(jnp.int32)
        ep_index = lax.axis_index("ep").astype(jnp.int32)
        place_index = (tp_index % PARTS).reshape(1)

        groups_of = [[jnp.stack([gate_weight[0], up_weight[0]])], [down_weight[0]]]
        for group in groups_of:
            group.append(lax.ppermute(group[0], "tp", neighbour))

        outgoing, places = pack_rows(
            place_index, moe_input, moe_gain.reshape(1, -1), routes, capacity, ep_count, groups_of[0][0]
        )
        arrived = lax.all_to_all(outgoing, "ep", 0, 0, tiled=True)

        for group in groups_of:
            for weight in group[:2]:
                group.append(lax.ppermute(weight, "tp", partner))
        gate_ups, downs = groups_of

        query, own_keys = prepare(
            ep_index.reshape(1),
            queries,
            compressed_key_value,
            rope_key,
            latent_norm_gain.reshape(1, -1),
            latent_to_key_value,
            angle_tables(ep_count, row_count),
            z_count,
        )
        query_all = [query]
        for i in range(1, x_count):
            query_all.append(lax.ppermute(query, "ep", x_shifts[x_count - i]))
        key_value = lax.all_to_all(
            own_keys, "ep", 0, 0, tiled=True, axis_index_groups=z_groups
        )

        partial_out = experts(arrived, gate_ups, downs)
        groups = lax.all_to_all(partial_out, "tp", 0, 0, tiled=True)

        partial_all = attend(query_all, key_value, (PLAIN_HEAD_DIM + ROPE) ** (-0.5))
        partials = [partial_all[0]] + [
            lax.ppermute(partial_all[i], "ep", x_shifts[i]) for i in range(1, x_count)
        ]
        attended = merge(partials)
        summed = add_up(groups, ep_count, attended)
        everyone = lax.all_gather(sequenced(attended, summed), "tp", axis=0, tiled=True)
        attention_out = lax.dot_general(
            everyone, out_proj, (((0,), (0,)), ((), ())), preferred_element_type=jnp.float32
        ).astype(jnp.bfloat16)

        returned = lax.all_to_all(summed, "ep", 0, 0, tiled=True)
        expert_out = combine(
            returned.reshape(ep_count * capacity, LANES), places, route_weight
        )
        return (attention_out, expert_out)

    return local


def solution(mesh):
    ep_count = mesh.shape["ep"]
    x_count = 4
    local = make_local(ep_count // x_count, x_count, mesh.shape["tp"])

    return jax.shard_map(
        local,
        mesh=mesh,
        in_specs=(
            P("ep", "tp"),
            P("ep", None),
            P("ep", None),
            P(),
            P(None, "tp"),
            P(None, "tp"),
            P("ep", None),
            P(),
            P("ep", None),
            P("ep", None),
            P("ep", None, "tp"),
            P("ep", None, "tp"),
            P("ep", "tp", None),
        ),
        out_specs=(P("ep", "tp"), P("ep", "tp")),
        check_vma=False,
    )
```
